32 devices in a mesh: grp: 2 (over x), ep: 4 (over y, core), tp: 4 (over z).
Axes of the slice: x: 2, y: 2, z: 4, core: 2. Of those that a mesh axis runs over, the one named last changes fastest.
Arguments:
- mixer_in: bfloat16 [4096, 2048], P(('grp', 'ep', 'tp')), parts along dimension 0, may hold values from -600 to 600
- mixer_gain: float32 [2048], replicated, may hold values from 0.1 to 1.9
- w_query: bfloat16 [2048, 1024], P(None, 'tp'), may hold values from -6 to 6
- w_key: bfloat16 [2048, 512], P(None, 'tp'), may hold values from -0.1875 to 0.1875
- w_value: bfloat16 [2048, 512], P(None, 'tp'), may hold values from -0.25 to 0.25
- sink_logit: float32 [16], P('tp'), may hold values from 3 to 9
- moe_in: bfloat16 [4096, 2048], P(('grp', 'ep', 'tp')), parts along dimension 0, may hold values from -600 to 600
- moe_gain: float32 [2048], replicated, may hold values from 0.1 to 1.9
- router: bfloat16 [2048, 16], replicated, may hold values from -0.25 to 0.25
- routes: int32 [4096, 4], P(('grp', 'ep', 'tp')), parts along dimension 0, may hold values from 0 to 15, all different within a row; in each aligned block of 128 rows (0 to 127, 128 to 255, ...) at most 48 rows name the same one
- expert_gate: bfloat16 [16, 2048, 512], P(('ep', 'tp')), may hold values from -0.125 to 0.125
- expert_up: bfloat16 [16, 2048, 512], P(('ep', 'tp')), may hold values from -0.125 to 0.125
- expert_down: bfloat16 [16, 512, 2048], P(('ep', 'tp')), may hold values from -0.25 to 0.25
- shared_gate: bfloat16 [2048, 512], P(None, 'tp'), may hold values from -0.125 to 0.125
- shared_up: bfloat16 [2048, 512], P(None, 'tp'), may hold values from -0.125 to 0.125
- shared_down: bfloat16 [512, 2048], P('tp'), may hold values from -0.25 to 0.25
Outputs:
- mixed: bfloat16 [4096, 1024], P(('grp', 'ep'), 'tp'), parts along dimension 0
- moe_out: bfloat16 [4096, 2048], P(('grp', 'ep', 'tp')), parts along dimension 0
The draws below stay inside these ranges and needn't reach their ends.
There are 2 independent parts, one for each index of `grp`. The reference program is written for one: setup_inputs(seed, part) draws one part's arguments, and reference() takes and returns one part's arrays. A program takes and returns all parts, laid end to end along the dimension named above; an argument that names none is the same for every part. Nothing has to cross between parts.
Inputs may be any that keep to these rules, and one draw needn't show every extreme that they name: `routes`: each row names 4 different experts. Within the rows of one device (aligned blocks of 128 rows) no expert is named by more than 48 rows, a bound that some block reaches.
All inputs are finite; a program needn't handle non-finite values.
Results may differ from the reference program's by a relative error of at most 0.012.
Values may be sent and summed in bfloat16 or wider, within the bound.
A program may use at most 128 MiB of HBM per device.

```python
import math
import jax
import jax.numpy as jnp
import numpy as np
from jax import lax

D = 2048
HEADS = 16
KV_HEADS = 8
HEAD_DIM = 64
WINDOW = 128
EFF = 512
SFF = 512
TOP_K = 4
ROWS = 128
TOKENS = 2048
EXPERTS = 16
CAP = 48


def draw_mixer_in(key, part):
    values = jnp.clip(jax.random.normal(jax.random.fold_in(key, 1), (TOKENS, D), jnp.float32), -6.0, 6.0)
    return values.astype(jnp.bfloat16)


def draw_moe_in(key, part):
    values = jnp.clip(jax.random.normal(jax.random.fold_in(key, 4), (TOKENS, D), jnp.float32), -6.0, 6.0)
    return values.astype(jnp.bfloat16)


def attention_weights(key):
    key_part, query_part = jax.random.split(jax.random.fold_in(key, 7), 2)
    spread = (2.0 / D) ** 0.5
    keys_weight = jnp.clip(jax.random.normal(key_part, (D, KV_HEADS, HEAD_DIM), jnp.float32), -6.0, 6.0) * spread
    query_weight = jnp.clip(jax.random.normal(query_part, (D, HEADS, HEAD_DIM), jnp.float32), -6.0, 6.0) * spread
    return (query_weight.reshape(D, HEADS * HEAD_DIM), keys_weight.reshape(D, KV_HEADS * HEAD_DIM))


def draw_w_query(key, part):
    return attention_weights(key)[0].astype(jnp.bfloat16)


def draw_w_key(key, part):
    return attention_weights(key)[1].astype(jnp.bfloat16)


def shard_levels(key, extent, pieces, low, high):
    gain, own = 1.0, jax.random.fold_in(key, 6)
    for axis_at, parts in pieces:
        steps = jnp.exp(jax.random.uniform(jax.random.fold_in(own, axis_at), (parts,), jnp.float32, low / len(pieces), high / len(pieces)))
        gain = gain * jnp.repeat(steps, extent[axis_at] // parts).reshape([-1 if axis == axis_at else 1 for axis in range(len(extent))])
    return gain


def shared_out(stream_key, own, number, rows, amount, top, bound, skew):
    order = jax.random.permutation(stream_key, amount)
    heavy_load, usual = shares(amount, rows * top, bound, skew, True), shares(amount, rows * top, bound, skew, False)
    places = jnp.arange(amount)

    def named(lengths, offset_by):
        used = int((lengths > 0).sum())
        fixed = max(1, used // 4)
        shifted = fixed + (places - fixed + offset_by * (used - fixed)) % max(1, amount - fixed)
        return jnp.zeros((amount,), jnp.int32).at[order[jnp.where(places < fixed, places, shifted)]].set(jnp.asarray(lengths, jnp.int32))

    lengths = jnp.where(number % 4 == 0, named(heavy_load, number // 4), named(usual, number - number // 4 - 1))
    mixed = jax.random.permutation(jax.random.fold_in(own, 3), amount)
    giver, taker = mixed[0:amount // 2 * 2:2], mixed[1:amount // 2 * 2:2]
    margin = jnp.minimum(lengths[giver] - 1, bound - lengths[taker]) // 2
    margin = jnp.where((giver == order[0]) | (taker == order[0]) | (lengths[taker] == 0), 0, jnp.maximum(margin, 0))
    shifted = jax.random.randint(jax.random.fold_in(own, 4), (amount // 2,), 0, 1 << 20) % (margin + 1)
    lengths = lengths.at[giver].add(-shifted).at[taker].add(shifted)
    members = jnp.searchsorted(jnp.cumsum(lengths), jnp.arange(rows * top), side="right").astype(jnp.int32)
    listing = members.reshape(top, rows).T
    listing = listing[jax.random.permutation(jax.random.fold_in(own, 1), rows)]
    offset_by = jax.random.randint(jax.random.fold_in(own, 2), (rows, 1), 0, top)
    return jnp.take_along_axis(listing, (jnp.arange(top)[None, :] + offset_by) % top, axis=1)


def shares(amount, total, bound, skew, full):
    weights = [(1 << 20) // math.isqrt(grade ** skew) + 1 for grade in range(1, amount + 1)]
    largest = bound if full else min(bound, max(-(-total // amount), total * weights[0] // sum(weights)))
    least = 1 if total - largest >= amount - 1 else 0
    given, surplus = [largest] + [least] * (amount - 1), total - largest - least * (amount - 1)
    while surplus > 0:
        movable = [i for i in range(1, amount) if given[i] < largest] or [i for i in range(1, amount) if given[i] < bound]
        pool, remaining = sum([weights[i] for i in movable]), surplus
        for i in movable:
            extra = min(bound - given[i], max(1, remaining * weights[i] // pool), surplus)
            given[i] = given[i] + extra
            surplus = surplus - extra
    return np.array(given)


def bell_draw(key, shape, scale, limit, cuts=(), kind=jnp.bfloat16):
    array = jax.random.normal(key, shape, jnp.float32) * scale
    if len(cuts) > 0:
        array = shard_levels(key, shape, cuts, -0.22, 0.18) * array
    return jnp.clip(array, min=-limit, max=limit).astype(kind)


def setup_inputs(seed: int = 0, part: int = 0) -> dict:
    key_list = jax.random.split(jax.random.key(seed), 17)
    own_keys = jax.random.split(jax.random.fold_in(key_list[16], part), 17)
    mixer_in = draw_mixer_in(jax.random.fold_in(jax.random.fold_in(key_list[16], part), 71), part)
    mixer_gain = jnp.clip(1.0 + 0.18 * jax.random.normal(key_list[1], (D,), jnp.float32), 0.1, 1.9)
    w_query = draw_w_query(jax.random.fold_in(key_list[16], 71), part)
    w_key = draw_w_key(jax.random.fold_in(key_list[16], 71), part)
    w_value = bell_draw(key_list[4], (D, KV_HEADS * HEAD_DIM), (D // 4) ** -0.5, 0.25, ((1, 4),))
    sink_logit = jnp.clip(3.0 + 6.0 * jax.random.uniform(key_list[5], (HEADS,), jnp.float32) ** shard_levels(key_list[5], (HEADS,), ((0, 4),), -0.2, 0.2), 3.0, 9.0)
    moe_in = draw_moe_in(jax.random.fold_in(jax.random.fold_in(key_list[16], part), 71), part)
    moe_gain = jnp.clip(1.0 + 0.18 * jax.random.normal(key_list[7], (D,), jnp.float32), 0.1, 1.9)
    router = bell_draw(key_list[8], (D, EXPERTS), (D // 4) ** -0.5, 0.25)
    routes_keys = jax.random.split(jax.random.fold_in(own_keys[9], 1), TOKENS // ROWS)
    routes_turns = jax.random.permutation(jax.random.fold_in(own_keys[9], 3), TOKENS // ROWS)
    routes = jax.vmap(lambda own, number: shared_out(jax.random.fold_in(own_keys[9], 2), own, number, ROWS, EXPERTS, TOP_K, CAP, 2))(routes_keys, routes_turns).reshape((TOKENS, TOP_K))
    expert_gate = bell_draw(key_list[10], (EXPERTS, D, EFF), D ** -0.5, 0.125, ((0, 16),))
    expert_up = bell_draw(key_list[11], (EXPERTS, D, EFF), D ** -0.5, 0.125, ((0, 16),))
    expert_down = bell_draw(key_list[12], (EXPERTS, EFF, D), EFF ** -0.5, 0.25, ((0, 16),))
    shared_gate = bell_draw(key_list[13], (D, SFF), D ** -0.5, 0.125, ((1, 4),))
    shared_up = bell_draw(key_list[14], (D, SFF), D ** -0.5, 0.125, ((1, 4),))
    shared_down = bell_draw(key_list[15], (SFF, D), SFF ** -0.5, 0.25, ((0, 4),))
    return dict(mixer_in=mixer_in, mixer_gain=mixer_gain, w_query=w_query, w_key=w_key, w_value=w_value, sink_logit=sink_logit, moe_in=moe_in, moe_gain=moe_gain, router=router, routes=routes, expert_gate=expert_gate, expert_up=expert_up, expert_down=expert_down, shared_gate=shared_gate, shared_up=shared_up, shared_down=shared_down)


EPS = 1e-06
THETA = 10000.0
ROUTED_SCALE = 2.5

def rms_rows(row_block, gain_vector):
    values = row_block.astype(jnp.float32)
    factor = lax.rsqrt(lax.optimization_barrier(jnp.mean(values * values, axis=-1, keepdims=True)) + EPS)
    return (values * factor * gain_vector.astype(jnp.float32)).astype(jnp.bfloat16)

def rotate(head_rows, positions):
    half_width = head_rows.shape[-1] // 2
    inverse = THETA ** (-(jnp.arange(half_width, dtype=jnp.float32) * 2.0) / head_rows.shape[-1])
    angles = positions.astype(jnp.float32)[:, None] * inverse[None, :]
    cosine_table = jnp.cos(angles)[:, None, :]
    sine_table = jnp.sin(angles)[:, None, :]
    first_half = head_rows[..., :half_width]
    second_half = head_rows[..., half_width:]
    return jnp.concatenate([first_half * cosine_table - second_half * sine_table, second_half * cosine_table + first_half * sine_table], axis=-1)

def window_attention(query_rows, key_rows, value_rows, sink_logit):
    length = query_rows.shape[0]
    head_count = query_rows.shape[1]
    kv_count = key_rows.shape[1]
    group_size = head_count // kv_count
    head_width = query_rows.shape[2]
    block_rows = min(512, length)
    padding = ((WINDOW, WINDOW), (0, 0), (0, 0))
    key_table = jnp.pad(key_rows, padding)
    value_table = jnp.pad(value_rows, padding)
    grouped = query_rows.reshape(length, kv_count, group_size, head_width)
    row_ids = jnp.arange(block_rows, dtype=jnp.int32)[:, None]
    col_ids = jnp.arange(block_rows + 2 * WINDOW, dtype=jnp.int32)[None, :]
    sink_table = sink_logit.astype(jnp.float32).reshape(kv_count, group_size)[:, :, None, None]

    def one_block(block_index):
        block_start = block_index * block_rows
        query_block = lax.dynamic_slice_in_dim(grouped, block_start, block_rows, 0).astype(jnp.float32)
        key_block = lax.dynamic_slice_in_dim(key_table, block_start, block_rows + 2 * WINDOW, 0).astype(jnp.float32)
        value_block = lax.dynamic_slice_in_dim(value_table, block_start, block_rows + 2 * WINDOW, 0).astype(jnp.float32)
        scores = jnp.einsum('qkgd,ckd->kgqc', query_block, key_block) * head_width ** (-0.5)
        key_pos = block_start - WINDOW + col_ids
        query_pos = block_start + row_ids
        in_window = (jnp.abs(key_pos - query_pos) <= WINDOW) & (key_pos >= 0) & (key_pos < length)
        scores = jnp.where(in_window[None, None], scores, -jnp.inf)
        row_max = jnp.maximum(lax.optimization_barrier(jnp.max(scores, axis=-1, keepdims=True)), sink_table)
        weights = jnp.exp(scores - row_max)
        denominator = lax.optimization_barrier(jnp.sum(weights, axis=-1, keepdims=True)) + jnp.exp(sink_table - row_max)
        probability = (weights / denominator).astype(jnp.bfloat16)
        output = jnp.einsum('kgqc,ckd->qkgd', probability.astype(jnp.float32), value_block)
        return output.reshape(block_rows, head_count * head_width).astype(jnp.bfloat16)
    blocks_out = lax.map(one_block, jnp.arange(length // block_rows, dtype=jnp.int32))
    return blocks_out.reshape(length, head_count * head_width)

def reference(mixer_in, mixer_gain, w_query, w_key, w_value, sink_logit, moe_in, moe_gain, router, routes, expert_gate, expert_up, expert_down, shared_gate, shared_up, shared_down):
    normed_first = rms_rows(mixer_in, mixer_gain)
    positions = jnp.arange(normed_first.shape[0], dtype=jnp.int32)
    query_rows = rotate(jnp.dot(normed_first, w_query, preferred_element_type=jnp.float32).reshape(-1, HEADS, HEAD_DIM), positions).astype(jnp.bfloat16)
    key_rows = rotate(jnp.dot(normed_first, w_key, preferred_element_type=jnp.float32).reshape(-1, KV_HEADS, HEAD_DIM), positions).astype(jnp.bfloat16)
    value_rows = jnp.dot(normed_first, w_value, preferred_element_type=jnp.float32).astype(jnp.bfloat16)
    value_rows = value_rows.reshape(-1, KV_HEADS, HEAD_DIM)
    mixed = window_attention(query_rows, key_rows, value_rows, sink_logit)
    normed_second = rms_rows(moe_in, moe_gain)
    affinity = jax.nn.sigmoid(jnp.dot(normed_second, router, preferred_element_type=jnp.float32))
    chosen = jnp.take_along_axis(affinity, routes, axis=1)
    route_weight = ROUTED_SCALE * chosen / lax.optimization_barrier(jnp.sum(chosen, axis=-1, keepdims=True))
    shared_hidden = (jax.nn.silu(jnp.dot(normed_second, shared_gate, preferred_element_type=jnp.float32)) * jnp.dot(normed_second, shared_up, preferred_element_type=jnp.float32)).astype(jnp.bfloat16)
    shared = jnp.dot(shared_hidden, shared_down, preferred_element_type=jnp.float32)
    token_count = routes.shape[0]
    sources = token_count // ROWS
    per_source = routes.reshape(sources, ROWS * TOP_K)
    one_hot = (per_source[:, :, None] == jnp.arange(EXPERTS, dtype=jnp.int32)[None, None, :]).astype(jnp.int32)
    slot_index = lax.optimization_barrier(jnp.sum((jnp.cumsum(one_hot, axis=1) - 1) * one_hot, axis=-1))
    source_ids = jnp.arange(sources, dtype=jnp.int32)[:, None]
    column = (source_ids * CAP + slot_index).reshape(-1).astype(jnp.int32)
    token_ids = jnp.arange(token_count * TOP_K, dtype=jnp.int32) // TOP_K
    flat_routes = routes.reshape(-1)
    row_table = jnp.full((EXPERTS, sources * CAP), token_count, jnp.int32).at[flat_routes, column].set(token_ids)
    weight_table = jnp.zeros((EXPERTS, sources * CAP), jnp.float32).at[flat_routes, column].set(route_weight.reshape(-1))
    padded_rows = jnp.concatenate([normed_second, jnp.zeros((1, normed_second.shape[1]), jnp.bfloat16)], axis=0)

    def one_expert(totals, inputs):
        row_ids, scales, gate_weight, up_weight, down_weight = inputs
        gathered = padded_rows[row_ids]
        hidden = (jax.nn.silu(jnp.dot(gathered, gate_weight, preferred_element_type=jnp.float32)) * jnp.dot(gathered, up_weight, preferred_element_type=jnp.float32)).astype(jnp.bfloat16)
        result = jnp.dot(hidden, down_weight, preferred_element_type=jnp.float32).astype(jnp.bfloat16)
        return (totals.at[row_ids].add(result.astype(jnp.float32) * scales[:, None]), None)
    totals, _ = lax.scan(one_expert, jnp.zeros((token_count + 1, normed_second.shape[1]), jnp.float32), (row_table, weight_table, expert_gate, expert_up, expert_down))
    moe_out = (totals[:token_count] + shared).astype(jnp.bfloat16)
    return (mixed, moe_out)
```

```python
import functools

import jax
import jax.numpy as jnp
from jax import lax
from jax.experimental import pallas as pl
from jax.experimental.pallas import tpu as pltpu
from jax.sharding import PartitionSpec as P

HEAD_DIM = 64
WINDOW = 128
EPS = 1e-06
THETA = 10000.0
ROUTED_SCALE = 2.5
LANES = 128
CHUNK = 512
MESH = pl.DeviceIdType.MESH
VMEM_LIMIT = 63 * 2**20


def remote(src, dst, send_sem, recv_sem, device):
    return pltpu.make_async_remote_copy(
        src_ref=src,
        dst_ref=dst,
        send_sem=send_sem,
        recv_sem=recv_sem,
        device_id=device,
        device_id_type=MESH,
    )


def greet(grp, ep, tp, ep_count, tp_count):
    barrier = pltpu.get_barrier_semaphore()

    @pl.when(tp > 0)
    def _():
        pl.semaphore_signal(barrier, inc=1, device_id=(grp, ep, tp - 1), device_id_type=MESH)

    @pl.when(tp < tp_count - 1)
    def _():
        pl.semaphore_signal(barrier, inc=1, device_id=(grp, ep, tp + 1), device_id_type=MESH)

    for d in range(1, ep_count):
        pl.semaphore_signal(
            barrier, inc=1, device_id=(grp, lax.rem(ep + d, ep_count), tp), device_id_type=MESH
        )
    return barrier


def layer_kernel(
    ep_count, tp_count, slots,
    second_in, gain_second, gain_first, router, routes, inverse, sink,
    first_hbm, gate_hbm, up_hbm, down_hbm, sgate_hbm, sup_hbm, sdown_hbm, wq_hbm, wk_hbm, wv_hbm,
    out, mixed,
    gath2, gath1, first_in, metag, sbuf, disp, back, sides, psend,
    gate, up, down, sgate, sup, sdown, wq, wk, wv,
    hidden, hexp, cosine, sine, qbuf, kvbuf,
    l_sem, s2, r2, sm, rm, s1, r1, sd, rd, sb, rb, sp, rs, hs, hr,
):
    grp, ep, tp = lax.axis_index("grp"), lax.axis_index("ep"), lax.axis_index("tp")
    rows, width = second_in.shape
    experts = metag.shape[1] // 2
    total = ep_count * slots
    parts = width // CHUNK
    f32, bf16 = jnp.float32, jnp.bfloat16
    away = pl.ds(slots, total - slots)

    local = [
        pltpu.make_async_copy(src, dst, l_sem.at[i])
        for i, (src, dst) in enumerate(
            [
                (first_hbm, first_in),
                (sgate_hbm, sgate),
                (sup_hbm, sup),
                (gate_hbm.at[0], gate),
                (up_hbm.at[0], up),
                (down_hbm.at[0], down),
                (wq_hbm, wq),
                (wk_hbm, wk),
                (wv_hbm, wv),
                (sdown_hbm, sdown),
            ]
        )
    ]
    for copy in local:
        copy.start()
    barrier = greet(grp, ep, tp, ep_count, tp_count)

    def toward(side):
        return (grp, ep, tp + (1 if side == 0 else -1))

    def exists(side):
        return tp < tp_count - 1 if side == 0 else tp > 0

    def peer(d):
        return (grp, lax.rem(ep + d, ep_count), tp)

    def part_span(part, size=CHUNK):
        return pl.ds(pl.multiple_of(part * size, size), size)

    def each_part(body, count=parts):
        def step(part, carry):
            body(part)
            return carry

        lax.fori_loop(0, count, step, 0)

    def at(side, distance):
        block = tp - distance if side == 0 else tp + distance
        return block, (block >= 0 if side == 0 else block < tp_count)

    def send_second(side, block, part):
        ref = gath2.at[block, :, part_span(part)]
        return remote(ref, ref, s2.at[side, block], r2.at[block, part], toward(side))

    def send_meta(side, block):
        return remote(metag.at[block], metag.at[block], sm.at[side, block], rm.at[block], toward(side))

    def send_first(side, block):
        return remote(gath1.at[block], gath1.at[block], s1.at[side, block], r1.at[block], toward(side))

    def dispatch_copy(block, d, span):
        mine = pl.ds(d * slots, slots)
        return remote(sbuf.at[block, mine, span], disp.at[block, mine, span], sd.at[block], rd.at[block], peer(d))

    def dispatch_all(block):
        return remote(sbuf.at[block, away], disp.at[block, away], sd.at[block], rd.at[block], peer(1))

    def return_copy(block, d, part):
        mine, span = pl.ds(d * slots, slots), part_span(part)
        return remote(
            sbuf.at[block, mine, span], back.at[block, mine, span],
            sb.at[block], rb.at[block, part], peer(ep_count - d),
        )

    def return_part(block, part):
        span = part_span(part)
        return remote(
            sbuf.at[block, away, span], back.at[block, away, span], sb.at[block], rb.at[block, part], peer(1)
        )

    def return_all(block):
        return remote(sbuf.at[block, away], back.at[block, away], sb.at[block], rb.at[block, 0], peer(1))

    def pass_on(side, block, part):
        span = part_span(part)
        return remote(
            psend.at[block, :, span], sides.at[side, block, :, span],
            sp.at[block, part], rs.at[side, block, part], toward(side),
        )

    def halo(side):
        source = tp_count * rows if side == 0 else rows
        target = 0 if side == 0 else (tp_count + 1) * rows
        return remote(
            kvbuf.at[pl.ds(source, rows)], kvbuf.at[pl.ds(target, rows)],
            hs.at[side], hr.at[side], (grp, ep + (1 if side == 0 else -1), tp),
        )

    def normalize(source, gain, target):
        def squares(part, carry):
            values = source[:, part_span(part)].astype(f32)
            return carry + jnp.sum(values * values, axis=1, keepdims=True)

        summed = lax.fori_loop(0, parts, squares, jnp.zeros((rows, 1), f32))
        factor = lax.rsqrt(summed / width + EPS)

        def scale(part):
            span = part_span(part)
            target[:, span] = (source[:, span].astype(f32) * factor * gain[:, span]).astype(bf16)

        each_part(scale)

    def places_of(block, d):
        expert = lax.rem(ep + d, ep_count) * tp_count + tp
        slot_ids = lax.broadcasted_iota(jnp.int32, (slots, rows), 0).astype(f32)
        return slot_ids == metag[block, pl.ds(expert, 1), :], expert

    def pick_part(block, part):
        span = part_span(part)
        picks = [jnp.where(places_of(block, d)[0], 1.0, 0.0) for d in range(ep_count)]
        pick = jnp.concatenate(picks, axis=0).astype(bf16)
        picked = jnp.dot(pick, gath2[block, :, span], preferred_element_type=f32).astype(bf16)
        disp[block, 0:slots, span] = picked[0:slots]
        sbuf[block, slots:total, span] = picked[slots:total]
        for d in range(1, ep_count):
            dispatch_copy(block, d, span).start()

    def shared_hidden(block):
        values = gath2[block]
        gated = jnp.dot(values, sgate[...], preferred_element_type=f32)
        lifted = jnp.dot(values, sup[...], preferred_element_type=f32)
        hidden[block] = (jax.nn.silu(gated) * lifted).astype(bf16)

    def expert(block):
        dispatch_all(block).wait()

        def units(part):
            span = part_span(part, 256)
            values = disp[block]
            gated = jnp.dot(values, gate[:, span], preferred_element_type=f32)
            lifted = jnp.dot(values, up[:, span], preferred_element_type=f32)
            hexp[:, span] = (jax.nn.silu(gated) * lifted).astype(bf16)

        each_part(units, gate.shape[1] // 256)

        def columns(part):
            span = part_span(part)
            result = jnp.dot(hexp[...], down[:, span], preferred_element_type=f32).astype(bf16)
            back[block, 0:slots, span] = result[0:slots]
            sbuf[block, slots:total, span] = result[slots:total]

            @pl.when(block != tp)
            def _():
                for d in range(1, ep_count):
                    return_copy(block, d, part).start()

        each_part(columns)

    def experts_at(distance):
        def one(side, carry):
            block = tp + (2 * side - 1) * distance

            @pl.when((block >= 0) & (block < tp_count) & ((distance > 0) | (side == 0)))
            def _():
                expert(block)

            return carry

        lax.fori_loop(0, 2, one, 0)

    def start_own_first(side, step):
        last = tp if side == 0 else tp_count - 1 - tp

        @pl.when(exists(side) & (step == last))
        def _():
            send_first(side, tp).start()

    def rotated(values, cos_rows, sin_rows):
        pieces = []
        half = HEAD_DIM // 2
        size = LANES if values.shape[1] % LANES == 0 else HEAD_DIM
        for start in range(0, values.shape[1], size):
            piece = values[:, start : start + size]
            if size == LANES:
                lane = lax.broadcasted_iota(jnp.int32, piece.shape, 1)
                swapped = jnp.where(
                    lax.rem(lane, HEAD_DIM) < half,
                    pltpu.roll(piece, LANES - half, 1),
                    pltpu.roll(piece, half, 1),
                )
            else:
                swapped = jnp.concatenate([piece[:, half:], piece[:, :half]], axis=1)
            pieces.append(piece * cos_rows[:, :size] + swapped * sin_rows[:, :size])
        return pieces[0] if len(pieces) == 1 else jnp.concatenate(pieces, axis=1)

    def project(block):
        base = pl.multiple_of(block * rows, rows)
        values = gath1[block]
        cos_rows, sin_rows = cosine[pl.ds(base, rows), :], sine[pl.ds(base, rows), :]
        query = jnp.dot(values, wq[...], preferred_element_type=f32)
        key = jnp.dot(values, wk[...], preferred_element_type=f32)
        value = jnp.dot(values, wv[...], preferred_element_type=f32)
        qbuf[pl.ds(base, rows), :] = rotated(query, cos_rows, sin_rows).astype(bf16)
        kvbuf[pl.ds(pl.multiple_of(base + rows, rows), rows), :] = jnp.concatenate(
            [rotated(key, cos_rows, sin_rows), value], axis=1
        ).astype(bf16)

    def tables():
        def one(block):
            start = pl.multiple_of(block * rows, rows)
            shape = (rows, LANES)
            place = ep * (tp_count * rows) + start + lax.broadcasted_iota(jnp.int32, shape, 0)
            angle = place.astype(f32) * inverse[...]
            lane = lax.broadcasted_iota(jnp.int32, shape, 1)
            turn = jnp.sin(angle)
            cosine[pl.ds(start, rows), :] = jnp.cos(angle)
            sine[pl.ds(start, rows), :] = jnp.where(lax.rem(lane, HEAD_DIM) < HEAD_DIM // 2, -turn, turn)

        each_part(one, tp_count)

    kv_heads = wk.shape[1] // HEAD_DIM
    group = wq.shape[1] // wk.shape[1]

    def attend(block):
        base = pl.multiple_of(block * rows, rows)
        window = kvbuf[pl.ds(base, 3 * rows), :]
        query = qbuf[pl.ds(base, rows), :]
        shape = (rows, 3 * rows)
        row = lax.broadcasted_iota(jnp.int32, shape, 0)
        col = lax.broadcasted_iota(jnp.int32, shape, 1)
        gap = col - row - rows
        low = jnp.where((ep == 0) & (block == 0), rows, 0)
        high = jnp.where((ep == ep_count - 1) & (block == tp_count - 1), 2 * rows, 3 * rows)
        near = (gap <= WINDOW) & (gap >= -WINDOW) & (col >= low) & (col < high)
        pieces = []
        for g in range(kv_heads):
            keys = window[:, g * HEAD_DIM : (g + 1) * HEAD_DIM]
            start = (kv_heads + g) * HEAD_DIM
            values = window[:, start : start + HEAD_DIM]
            for h in range(g * group, (g + 1) * group):
                scores = lax.dot_general(
                    query[:, h * HEAD_DIM : (h + 1) * HEAD_DIM], keys, (((1,), (1,)), ((), ())),
                    preferred_element_type=f32,
                ) * HEAD_DIM ** (-0.5)
                scores = jnp.where(near, scores, -jnp.inf)
                bound = sink[0, h]
                top = jnp.maximum(jnp.max(scores, axis=1, keepdims=True), bound)
                weights = jnp.exp(scores - top)
                summed = jnp.sum(weights, axis=1, keepdims=True) + jnp.exp(bound - top)
                share = (weights * (1.0 / summed)).astype(bf16)
                pieces.append(jnp.dot(share, values, preferred_element_type=f32))
        mixed[pl.ds(base, rows), :] = jnp.concatenate(pieces, axis=1).astype(bf16)

    normalize(second_in, gain_second, gath2.at[tp])
    ids = lax.broadcasted_iota(jnp.int32, (experts, rows), 0)
    hit = ids == routes[0:1, :]
    for j in range(1, routes.shape[0]):
        hit = hit | (ids == routes[j : j + 1, :])
    earlier = (
        lax.broadcasted_iota(jnp.int32, (rows, rows), 0) < lax.broadcasted_iota(jnp.int32, (rows, rows), 1)
    )
    before = jnp.dot(
        jnp.where(hit, 1.0, 0.0).astype(bf16), jnp.where(earlier, 1.0, 0.0).astype(bf16),
        preferred_element_type=f32,
    )
    metag[tp, 0:experts, :] = jnp.where(hit, before, -1.0)
    pl.semaphore_wait(barrier, ep_count + jnp.where((tp > 0) & (tp < tp_count - 1), 1, 0))
    def send_own(part):
        for side in range(2):

            @pl.when(exists(side))
            def _():
                send_second(side, tp, part).start()

    send_own(0)
    affinity = lax.dot_general(
        router[...], gath2[tp], (((1,), (1,)), ((), ())), preferred_element_type=f32
    )
    chosen = jnp.where(hit, jax.nn.sigmoid(affinity), 0.0)
    metag[tp, experts : 2 * experts, :] = ROUTED_SCALE * chosen / jnp.sum(chosen, axis=0, keepdims=True)
    pick_part(tp, 0)
    for side in range(2):

        @pl.when(exists(side))
        def _():
            send_meta(side, tp).start()

    for part in range(1, parts):
        send_own(part)

    def pick_rest(part, carry):
        pick_part(tp, part)
        return carry

    lax.fori_loop(1, parts, pick_rest, 0)
    local[0].wait()
    normalize(first_in, gain_first, gath1.at[tp])
    for side in range(2):
        start_own_first(side, 0)

    @pl.when(tp == 0)
    def _():
        sides[0] = jnp.zeros(sides.shape[1:], sides.dtype)

    @pl.when(tp == tp_count - 1)
    def _():
        sides[1] = jnp.zeros(sides.shape[1:], sides.dtype)

    @pl.when(ep == 0)
    def _():
        kvbuf[0:rows, :] = jnp.zeros((rows, kvbuf.shape[1]), bf16)

    @pl.when(ep == ep_count - 1)
    def _():
        kvbuf[(tp_count + 1) * rows : (tp_count + 2) * rows, :] = jnp.zeros((rows, kvbuf.shape[1]), bf16)

    for copy in local[1:]:
        copy.wait()
    shared_hidden(tp)

    def weights_of(block):
        pieces = []
        for d in range(ep_count):
            hit_rows, number = places_of(block, d)
            pieces.append(jnp.where(hit_rows, metag[block, pl.ds(experts + number, 1), :], 0.0))
        weights = jnp.concatenate(pieces, axis=0)
        top = weights.astype(bf16)
        return top, (weights - top.astype(f32)).astype(bf16)

    def value_of(block, weights, span):
        turned = (((0,), (0,)), ((), ()))
        picked = back[block, :, span]
        return (
            lax.dot_general(weights[0], picked, turned, preferred_element_type=f32)
            + lax.dot_general(weights[1], picked, turned, preferred_element_type=f32)
            + jnp.dot(hidden[block], sdown[:, span], preferred_element_type=f32)
        )

    def reduce_step(step):
        for side in range(2):
            block = step - tp if side == 0 else 2 * (tp_count - 1) - step - tp
            active = (block > tp) & (block < tp_count) if side == 0 else (block < tp) & (block >= 0)

            @pl.when(active)
            def _():
                weights = weights_of(block)

                def one_part(part):
                    span = part_span(part)
                    return_part(block, part).wait_recv()
                    own = value_of(block, weights, span)

                    @pl.when(tp > 0 if side == 0 else tp < tp_count - 1)
                    def _():
                        pass_on(side, block, part).wait_recv()

                    psend[block, :, span] = (own + sides[side, block, :, span].astype(f32)).astype(bf16)
                    pass_on(side, block, part).start()

                each_part(one_part)

    early = tp_count > 2

    def hop(k, carry):
        def one_part(part):
            for side in range(2):
                block, inside = at(side, k)

                @pl.when(inside)
                def _():
                    send_second(side, block, part).wait_recv()

                    @pl.when(exists(side))
                    def _():
                        send_second(side, block, part).start()

                    @pl.when(part == 0)
                    def _():
                        send_meta(side, block).wait_recv()

                        @pl.when(exists(side))
                        def _():
                            send_meta(side, block).start()

            for side in range(2):
                block, inside = at(side, k)

                @pl.when(inside)
                def _():
                    pick_part(block, part)

        each_part(one_part)
        for side in range(2):
            start_own_first(side, k)
        for side in range(2):
            block, inside = at(side, k)

            @pl.when(inside)
            def _():
                shared_hidden(block)

        if early:

            @pl.when(k == tp_count - 1)
            def _():
                reduce_step(1)

        experts_at(k - 1)

        @pl.when(k == 1)
        def _():
            tables()
            project(tp)

        return carry

    lax.fori_loop(1, tp_count, hop, 0)
    experts_at(tp_count - 1)
    for part in range(parts):
        for d in range(1, ep_count):
            return_copy(tp, d, part).start()

    def start_halo(block):
        @pl.when((block == tp_count - 1) & (ep < ep_count - 1))
        def _():
            halo(0).start()

        @pl.when((block == 0) & (ep > 0))
        def _():
            halo(1).start()

    start_halo(tp)

    def attend_inner(block):
        @pl.when((block > 0) & (block < tp_count - 1))
        def _():
            attend(block)

    def first_hop(k, carry):
        for side in range(2):
            block, inside = at(side, k)

            @pl.when(inside & exists(side))
            def _():
                send_first(side, block).wait_recv()
                send_first(side, block).start()

        reduce_step(jnp.where(k == 1, 2 if early else 1, 2 * k - 1))
        for side in range(2):
            block, inside = at(side, k)

            @pl.when(inside & jnp.logical_not(exists(side)))
            def _():
                send_first(side, block).wait_recv()

        def use(side, carry):
            block = tp + (2 * side - 1) * k

            @pl.when((block >= 0) & (block < tp_count))
            def _():
                project(block)
                start_halo(block)

            return carry

        lax.fori_loop(0, 2, use, 0)

        def settle(side, carry):
            block = tp + (2 * side - 1) * (k - 1)

            @pl.when((block > 0) & (block < tp_count - 1) & ((k > 1) | (side == 0)))
            def _():
                attend(block)

            return carry

        lax.fori_loop(0, 2, settle, 0)

        @pl.when(k == jnp.maximum(tp, tp_count - 1 - tp))
        def _():
            @pl.when(ep < ep_count - 1)
            def _():
                halo(1).wait_recv()

            @pl.when(ep > 0)
            def _():
                halo(0).wait_recv()

            def edge(side, carry):
                attend((tp_count - 1) * (1 - side))
                return carry

            lax.fori_loop(0, 2, edge, 0)

        if early:

            @pl.when(k > 1)
            def _():
                reduce_step(2 * k)

        return carry

    lax.fori_loop(1, tp_count, first_hop, 0)
    own_weights = weights_of(tp)

    def last_part(part):
        span = part_span(part)
        return_part(tp, part).wait_recv()
        own = value_of(tp, own_weights, span)

        @pl.when(tp > 0)
        def _():
            pass_on(0, tp, part).wait_recv()

        @pl.when(tp < tp_count - 1)
        def _():
            pass_on(1, tp, part).wait_recv()

        out[:, span] = (
            own + sides[0, tp, :, span].astype(f32) + sides[1, tp, :, span].astype(f32)
        ).astype(bf16)

    each_part(last_part)

    def finish(block):
        return_all(block).wait_send()
        for side in range(2):
            passed = block <= tp if side == 0 else block >= tp
            summed = block > tp if side == 0 else block < tp

            @pl.when(exists(side) & passed)
            def _():
                ref = gath2.at[block]
                remote(ref, ref, s2.at[side, block], r2.at[block, 0], toward(side)).wait_send()
                send_meta(side, block).wait_send()
                send_first(side, block).wait_send()

            @pl.when(summed)
            def _():
                for part in range(parts):
                    pass_on(side, block, part).wait_send()

    each_part(finish, tp_count)

    @pl.when(ep < ep_count - 1)
    def _():
        halo(0).wait_send()

    @pl.when(ep > 0)
    def _():
        halo(1).wait_send()


def layer(
    second, first, gain_second, gain_first, router, routes, inverse, sink,
    gate, up, down, sgate, sup, sdown, wq, wk, wv, ep_count, tp_count, slots,
):
    rows, width = second.shape
    experts = router.shape[0]
    vmem = pl.BlockSpec(memory_space=pltpu.VMEM)
    smem = pl.BlockSpec(memory_space=pltpu.SMEM)
    hbm = pl.BlockSpec(memory_space=pl.ANY)
    dma = pltpu.SemaphoreType.DMA
    bf16, f32 = jnp.bfloat16, jnp.float32
    total = ep_count * slots
    parts = width // CHUNK
    span = tp_count * rows
    kv_cols = wk.shape[1] + wv.shape[1]
    return pl.pallas_call(
        functools.partial(layer_kernel, ep_count, tp_count, slots),
        out_shape=(
            jax.ShapeDtypeStruct((rows, width), bf16),
            jax.ShapeDtypeStruct((span, wq.shape[1]), bf16),
        ),
        in_specs=[vmem] * 6 + [smem] + [hbm] * 10,
        out_specs=(vmem, vmem),
        scratch_shapes=[
            pltpu.VMEM((tp_count, rows, width), bf16),
            pltpu.VMEM((tp_count, rows, width), bf16),
            pltpu.VMEM((rows, width), bf16),
            pltpu.VMEM((tp_count, 2 * experts, rows), f32),
            pltpu.VMEM((tp_count, total, width), bf16),
            pltpu.VMEM((tp_count, total, width), bf16),
            pltpu.VMEM((tp_count, total, width), bf16),
            pltpu.VMEM((2, tp_count, rows, width), bf16),
            pltpu.VMEM((tp_count, rows, width), bf16),
            pltpu.VMEM(gate.shape[1:], bf16),
            pltpu.VMEM(up.shape[1:], bf16),
            pltpu.VMEM(down.shape[1:], bf16),
            pltpu.VMEM(sgate.shape, bf16),
            pltpu.VMEM(sup.shape, bf16),
            pltpu.VMEM(sdown.shape, bf16),
            pltpu.VMEM(wq.shape, bf16),
            pltpu.VMEM(wk.shape, bf16),
            pltpu.VMEM(wv.shape, bf16),
            pltpu.VMEM((tp_count, rows, sgate.shape[1]), bf16),
            pltpu.VMEM((total, gate.shape[2]), bf16),
            pltpu.VMEM((span, LANES), f32),
            pltpu.VMEM((span, LANES), f32),
            pltpu.VMEM((span, wq.shape[1]), bf16),
            pltpu.VMEM((span + 2 * rows, kv_cols), bf16),
            dma((10,)),
            dma((2, tp_count)),
            dma((tp_count, parts)),
            dma((2, tp_count)),
            dma((tp_count,)),
            dma((2, tp_count)),
            dma((tp_count,)),
            dma((tp_count,)),
            dma((tp_count,)),
            dma((tp_count,)),
            dma((tp_count, parts)),
            dma((tp_count, parts)),
            dma((2, tp_count, parts)),
            dma((2,)),
            dma((2,)),
        ],
        compiler_params=pltpu.CompilerParams(
            collective_id=0, has_side_effects=True, vmem_limit_bytes=VMEM_LIMIT
        ),
        name="layer",
    )(
        second, gain_second, gain_first, router, routes, inverse, sink,
        first, gate, up, down, sgate, sup, sdown, wq, wk, wv,
    )


def body(
    mixer_in,
    mixer_gain,
    w_query,
    w_key,
    w_value,
    sink_logit,
    moe_in,
    moe_gain,
    router,
    routes,
    expert_gate,
    expert_up,
    expert_down,
    shared_gate,
    shared_up,
    shared_down,
):
    tokens = mixer_in.shape[0]
    ep_count, tp_count = lax.axis_size("ep"), lax.axis_size("tp")
    top_count = routes.shape[1]
    experts = router.shape[1]
    capacity = 3 * top_count * tokens // (2 * experts)
    slots = -(-capacity // 16) * 16
    half = HEAD_DIM // 2
    inverse = THETA ** (-(jnp.arange(half, dtype=jnp.float32) * 2.0) / HEAD_DIM)
    moe_out, mixed = layer(
        moe_in, mixer_in, moe_gain[None, :], mixer_gain[None, :], router.T, routes.T,
        jnp.tile(inverse, LANES // half)[None, :], sink_logit[None, :],
        expert_gate, expert_up, expert_down, shared_gate, shared_up, shared_down,
        w_query, w_key, w_value, ep_count, tp_count, slots,
    )
    return (mixed, moe_out)


def solution(mesh):
    return jax.shard_map(
        body,
        mesh=mesh,
        in_specs=(
            P(("grp", "ep", "tp"), None),
            P(),
            P(None, "tp"),
            P(None, "tp"),
            P(None, "tp"),
            P("tp"),
            P(("grp", "ep", "tp"), None),
            P(),
            P(),
            P(("grp", "ep", "tp"), None),
            P(("ep", "tp"), None, None),
            P(("ep", "tp"), None, None),
            P(("ep", "tp"), None, None),
            P(None, "tp"),
            P(None, "tp"),
            P("tp", None),
        ),
        out_specs=(P(("grp", "ep"), "tp"), P(("grp", "ep", "tp"), None)),
        check_vma=False,
    )
```

```python
import functools

import jax
import jax.numpy as jnp
import numpy as np
from jax import lax
from jax.experimental import pallas as pl
from jax.experimental.pallas import tpu as pltpu
from jax.sharding import PartitionSpec as P

HEAD_DIM = 64
WINDOW = 128
EPS = 1e-06
THETA = 10000.0
ROUTED_SCALE = 2.5
LANES = 128
CHUNK = 512
LAG = 2
MESH = pl.DeviceIdType.MESH
VMEM_LIMIT = 63 * 2**20


def remote(src, dst, send_sem, recv_sem, device):
    return pltpu.make_async_remote_copy(
        src_ref=src,
        dst_ref=dst,
        send_sem=send_sem,
        recv_sem=recv_sem,
        device_id=device,
        device_id_type=MESH,
    )


def greet(grp, ep, tp, ep_count, tp_count):
    barrier = pltpu.get_barrier_semaphore()

    @pl.when(tp > 0)
    def _():
        pl.semaphore_signal(barrier, inc=1, device_id=(grp, ep, tp - 1), device_id_type=MESH)

    @pl.when(tp < tp_count - 1)
    def _():
        pl.semaphore_signal(barrier, inc=1, device_id=(grp, ep, tp + 1), device_id_type=MESH)

    for d in range(1, ep_count):
        pl.semaphore_signal(
            barrier, inc=1, device_id=(grp, lax.rem(ep + d, ep_count), tp), device_id_type=MESH
        )
    return barrier


def layer_kernel(
    ep_count, tp_count, slots,
    second_in, gain_second, gain_first, router, routes, inverse, sink,
    first_hbm, gate_hbm, up_hbm, down_hbm, sgate_hbm, sup_hbm, sdown_hbm, wq_hbm, wk_hbm, wv_hbm,
    out, mixed,
    gath2, gath1, first_in, metag, sbuf, disp, back, sides, psend,
    gate, up, down, sgate, sup, sdown, wq, wk, wv,
    hidden, hexp, cosine, sine, qbuf, kvbuf,
    l_sem, s2, r2, sm, rm, s1, r1, sd, rd, sb, rb, sp, rs, hs, hr,
):
    grp, ep, tp = lax.axis_index("grp"), lax.axis_index("ep"), lax.axis_index("tp")
    rows, width = second_in.shape
    experts = metag.shape[1] // 2
    total = ep_count * slots
    parts = width // CHUNK
    f32, bf16 = jnp.float32, jnp.bfloat16
    away = pl.ds(slots, total - slots)

    local = [
        pltpu.make_async_copy(src, dst, l_sem.at[i])
        for i, (src, dst) in enumerate(
            [
                (first_hbm, first_in),
                (sgate_hbm, sgate),
                (sup_hbm, sup),
                (gate_hbm.at[0], gate),
                (up_hbm.at[0], up),
                (down_hbm.at[0], down),
                (wq_hbm, wq),
                (wk_hbm, wk),
                (wv_hbm, wv),
                (sdown_hbm, sdown),
            ]
        )
    ]
    for copy in local:
        copy.start()
    barrier = greet(grp, ep, tp, ep_count, tp_count)

    def toward(side):
        return (grp, ep, tp + 1 - 2 * side)

    def exists(side):
        return (tp + 1 - 2 * side >= 0) & (tp + 1 - 2 * side < tp_count)

    def peer(d):
        return (grp, lax.rem(ep + d, ep_count), tp)

    def part_span(part, size=CHUNK):
        return pl.ds(pl.multiple_of(part * size, size), size)

    def each_part(body, count=parts):
        def step(part, carry):
            body(part)
            return carry

        lax.fori_loop(0, count, step, 0)

    def near(side, distance):
        block = tp + (2 * side - 1) * distance
        return block, (block >= 0) & (block < tp_count)

    swaps = tp_count > 2

    def swapped(side, block, allowed):
        far, second = (tp_count - 1) * side, 1 + (tp_count - 3) * side
        other = jnp.where(block == second, far, jnp.where(block == far, second, block))
        return jnp.where(allowed, other, block)

    def at(side, order):
        block, inside = near(side, order)
        if swaps:
            block = swapped(side, block, jnp.where(side == 0, tp, tp_count - 1 - tp) >= 2)
        return block, inside

    def late(side):
        return (tp == 1 + side * (tp_count - 3)) & swaps

    def send_second(side, block, part):
        ref = gath2.at[block, :, part_span(part)]
        return remote(ref, ref, s2.at[side, block], r2.at[block, part], toward(side))

    def send_meta(side, block):
        return remote(metag.at[block], metag.at[block], sm.at[side, block], rm.at[block], toward(side))

    def send_first(side, block):
        return remote(gath1.at[block], gath1.at[block], s1.at[side, block], r1.at[block], toward(side))

    def dispatch_copy(block, d, span):
        mine = pl.ds(d * slots, slots)
        return remote(sbuf.at[block, mine, span], disp.at[block, mine, span], sd.at[block], rd.at[block], peer(d))

    def dispatch_all(block):
        return remote(sbuf.at[block, away], disp.at[block, away], sd.at[block], rd.at[block], peer(1))

    def return_copy(block, d, part):
        mine, span = pl.ds(d * slots, slots), part_span(part)
        return remote(
            sbuf.at[block, mine, span], back.at[block, mine, span],
            sb.at[block], rb.at[block, part], peer(ep_count - d),
        )

    def return_part(block, part):
        span = part_span(part)
        return remote(
            sbuf.at[block, away, span], back.at[block, away, span], sb.at[block], rb.at[block, part], peer(1)
        )

    def return_all(block):
        return remote(sbuf.at[block, away], back.at[block, away], sb.at[block], rb.at[block, 0], peer(1))

    def pass_on(side, block, part):
        span = part_span(part)
        return remote(
            psend.at[block, :, span], sides.at[side, block, :, span],
            sp.at[block, part], rs.at[side, block, part], toward(side),
        )

    def halo(side):
        source = tp_count * rows if side == 0 else rows
        target = 0 if side == 0 else (tp_count + 1) * rows
        return remote(
            kvbuf.at[pl.ds(source, rows)], kvbuf.at[pl.ds(target, rows)],
            hs.at[side], hr.at[side], (grp, ep + (1 if side == 0 else -1), tp),
        )

    def normalize(source, gain, target):
        def squares(part, carry):
            values = source[:, part_span(part)].astype(f32)
            return carry + jnp.sum(values * values, axis=1, keepdims=True)

        summed = lax.fori_loop(0, parts, squares, jnp.zeros((rows, 1), f32))
        factor = lax.rsqrt(summed / width + EPS)

        def scale(part):
            span = part_span(part)
            target[:, span] = (source[:, span].astype(f32) * factor * gain[:, span]).astype(bf16)

        each_part(scale)

    def places_of(block, d):
        expert = lax.rem(ep + d, ep_count) * tp_count + tp
        slot_ids = lax.broadcasted_iota(jnp.int32, (slots, rows), 0).astype(f32)
        return slot_ids == metag[block, pl.ds(expert, 1), :], expert

    def pick_part(block, part):
        span = part_span(part)
        picks = [jnp.where(places_of(block, d)[0], 1.0, 0.0) for d in range(ep_count)]
        pick = jnp.concatenate(picks, axis=0).astype(bf16)
        picked = jnp.dot(pick, gath2[block, :, span], preferred_element_type=f32).astype(bf16)
        disp[block, 0:slots, span] = picked[0:slots]
        sbuf[block, slots:total, span] = picked[slots:total]
        for d in range(1, ep_count):
            dispatch_copy(block, d, span).start()

    def shared_hidden(block):
        values = gath2[block]
        gated = jnp.dot(values, sgate[...], preferred_element_type=f32)
        lifted = jnp.dot(values, sup[...], preferred_element_type=f32)
        hidden[block] = (jax.nn.silu(gated) * lifted).astype(bf16)

    def expert(block):
        dispatch_all(block).wait()

        def units(part):
            span = part_span(part, 256)
            values = disp[block]
            gated = jnp.dot(values, gate[:, span], preferred_element_type=f32)
            lifted = jnp.dot(values, up[:, span], preferred_element_type=f32)
            hexp[:, span] = (jax.nn.silu(gated) * lifted).astype(bf16)

        each_part(units, gate.shape[1] // 256)

        def columns(part):
            span = part_span(part)
            result = jnp.dot(hexp[...], down[:, span], preferred_element_type=f32).astype(bf16)
            back[block, 0:slots, span] = result[0:slots]
            sbuf[block, slots:total, span] = result[slots:total]

            @pl.when(block != tp)
            def _():
                for d in range(1, ep_count):
                    return_copy(block, d, part).start()

        each_part(columns)

    def experts_at(order):
        def one(side, carry):
            block, inside = at(side, order)

            @pl.when(inside & ((order > 0) | (side == 0)))
            def _():
                expert(block)

            return carry

        lax.fori_loop(0, 2, one, 0)

    def start_own_first(side, step):
        last = tp if side == 0 else tp_count - 1 - tp

        @pl.when(exists(side) & (step == last))
        def _():
            send_first(side, tp).start()

    def rotated(values, cos_rows, sin_rows):
        pieces = []
        half = HEAD_DIM // 2
        size = LANES if values.shape[1] % LANES == 0 else HEAD_DIM
        for start in range(0, values.shape[1], size):
            piece = values[:, start : start + size]
            if size == LANES:
                lane = lax.broadcasted_iota(jnp.int32, piece.shape, 1)
                crossed = jnp.where(
                    lax.rem(lane, HEAD_DIM) < half,
                    pltpu.roll(piece, LANES - half, 1),
                    pltpu.roll(piece, half, 1),
                )
            else:
                crossed = jnp.concatenate([piece[:, half:], piece[:, :half]], axis=1)
            pieces.append(piece * cos_rows[:, :size] + crossed * sin_rows[:, :size])
        return pieces[0] if len(pieces) == 1 else jnp.concatenate(pieces, axis=1)

    def project(block):
        base = pl.multiple_of(block * rows, rows)
        values = gath1[block]
        cos_rows, sin_rows = cosine[pl.ds(base, rows), :], sine[pl.ds(base, rows), :]
        query = jnp.dot(values, wq[...], preferred_element_type=f32)
        key = jnp.dot(values, wk[...], preferred_element_type=f32)
        value = jnp.dot(values, wv[...], preferred_element_type=f32)
        qbuf[pl.ds(base, rows), :] = rotated(query, cos_rows, sin_rows).astype(bf16)
        kvbuf[pl.ds(pl.multiple_of(base + rows, rows), rows), :] = jnp.concatenate(
            [rotated(key, cos_rows, sin_rows), value], axis=1
        ).astype(bf16)

    def tables():
        def one(block):
            start = pl.multiple_of(block * rows, rows)
            shape = (rows, LANES)
            place = ep * (tp_count * rows) + start + lax.broadcasted_iota(jnp.int32, shape, 0)
            angle = place.astype(f32) * inverse[...]
            lane = lax.broadcasted_iota(jnp.int32, shape, 1)
            turn = jnp.sin(angle)
            cosine[pl.ds(start, rows), :] = jnp.cos(angle)
            sine[pl.ds(start, rows), :] = jnp.where(lax.rem(lane, HEAD_DIM) < HEAD_DIM // 2, -turn, turn)

        each_part(one, tp_count)

    kv_heads = wk.shape[1] // HEAD_DIM
    group = wq.shape[1] // wk.shape[1]

    def attend(block):
        base = pl.multiple_of(block * rows, rows)
        window = kvbuf[pl.ds(base, 3 * rows), :]
        query = qbuf[pl.ds(base, rows), :]
        shape = (rows, 3 * rows)
        row = lax.broadcasted_iota(jnp.int32, shape, 0)
        col = lax.broadcasted_iota(jnp.int32, shape, 1)
        gap = col - row - rows
        low = jnp.where((ep == 0) & (block == 0), rows, 0)
        high = jnp.where((ep == ep_count - 1) & (block == tp_count - 1), 2 * rows, 3 * rows)
        near = (gap <= WINDOW) & (gap >= -WINDOW) & (col >= low) & (col < high)
        pieces = []
        for g in range(kv_heads):
            keys = window[:, g * HEAD_DIM : (g + 1) * HEAD_DIM]
            start = (kv_heads + g) * HEAD_DIM
            values = window[:, start : start + HEAD_DIM]
            for h in range(g * group, (g + 1) * group):
                scores = lax.dot_general(
                    query[:, h * HEAD_DIM : (h + 1) * HEAD_DIM], keys, (((1,), (1,)), ((), ())),
                    preferred_element_type=f32,
                ) * HEAD_DIM ** (-0.5)
                scores = jnp.where(near, scores, -jnp.inf)
                bound = sink[0, h]
                top = jnp.maximum(jnp.max(scores, axis=1, keepdims=True), bound)
                weights = jnp.exp(scores - top)
                summed = jnp.sum(weights, axis=1, keepdims=True) + jnp.exp(bound - top)
                share = (weights * (1.0 / summed)).astype(bf16)
                pieces.append(jnp.dot(share, values, preferred_element_type=f32))
        mixed[pl.ds(base, rows), :] = jnp.concatenate(pieces, axis=1).astype(bf16)

    normalize(second_in, gain_second, gath2.at[tp])
    ids = lax.broadcasted_iota(jnp.int32, (experts, rows), 0)
    hit = ids == routes[0:1, :]
    for j in range(1, routes.shape[0]):
        hit = hit | (ids == routes[j : j + 1, :])
    earlier = (
        lax.broadcasted_iota(jnp.int32, (rows, rows), 0) < lax.broadcasted_iota(jnp.int32, (rows, rows), 1)
    )
    before = jnp.dot(
        jnp.where(hit, 1.0, 0.0).astype(bf16), jnp.where(earlier, 1.0, 0.0).astype(bf16),
        preferred_element_type=f32,
    )
    metag[tp, 0:experts, :] = jnp.where(hit, before, -1.0)
    pl.semaphore_wait(barrier, ep_count + jnp.where((tp > 0) & (tp < tp_count - 1), 1, 0))
    def send_own(part):
        for side in range(2):

            @pl.when(exists(side) & jnp.logical_not(late(side)))
            def _():
                send_second(side, tp, part).start()

    send_own(0)
    affinity = lax.dot_general(
        router[...], gath2[tp], (((1,), (1,)), ((), ())), preferred_element_type=f32
    )
    chosen = jnp.where(hit, jax.nn.sigmoid(affinity), 0.0)
    metag[tp, experts : 2 * experts, :] = ROUTED_SCALE * chosen / jnp.sum(chosen, axis=0, keepdims=True)
    pick_part(tp, 0)
    for side in range(2):

        @pl.when(exists(side))
        def _():
            send_meta(side, tp).start()

    for part in range(1, parts):
        send_own(part)

    def pick_rest(part, carry):
        pick_part(tp, part)
        return carry

    lax.fori_loop(1, parts, pick_rest, 0)
    local[0].wait()
    normalize(first_in, gain_first, gath1.at[tp])
    for side in range(2):
        start_own_first(side, 0)

    @pl.when(tp == 0)
    def _():
        sides[0] = jnp.zeros(sides.shape[1:], sides.dtype)

    @pl.when(tp == tp_count - 1)
    def _():
        sides[1] = jnp.zeros(sides.shape[1:], sides.dtype)

    @pl.when(ep == 0)
    def _():
        kvbuf[0:rows, :] = jnp.zeros((rows, kvbuf.shape[1]), bf16)

    @pl.when(ep == ep_count - 1)
    def _():
        kvbuf[(tp_count + 1) * rows : (tp_count + 2) * rows, :] = jnp.zeros((rows, kvbuf.shape[1]), bf16)

    for copy in local[1:]:
        copy.wait()
    shared_hidden(tp)

    def weights_of(block):
        pieces = []
        for d in range(ep_count):
            hit_rows, number = places_of(block, d)
            pieces.append(jnp.where(hit_rows, metag[block, pl.ds(experts + number, 1), :], 0.0))
        weights = jnp.concatenate(pieces, axis=0)
        top = weights.astype(bf16)
        return top, (weights - top.astype(f32)).astype(bf16)

    def value_of(block, weights, span):
        turned = (((0,), (0,)), ((), ()))
        picked = back[block, :, span]
        return (
            lax.dot_general(weights[0], picked, turned, preferred_element_type=f32)
            + lax.dot_general(weights[1], picked, turned, preferred_element_type=f32)
            + jnp.dot(hidden[block], sdown[:, span], preferred_element_type=f32)
        )

    def reduce_step(step):
        def one(turn, carry):
            side = jnp.where(2 * tp < tp_count, 1 - turn, turn)
            block = jnp.where(side == 0, step - tp, 2 * (tp_count - 1) - step - tp)
            active = (block >= 0) & (block < tp_count)
            if swaps:
                block = swapped(1 - side, block, True)
            active = active & ((block - tp) * (1 - 2 * side) > 0)

            @pl.when(active)
            def _():
                weights = weights_of(block)

                def one_part(part):
                    span = part_span(part)
                    return_part(block, part).wait_recv()
                    own = value_of(block, weights, span)

                    @pl.when(exists(1 - side))
                    def _():
                        pass_on(side, block, part).wait_recv()

                    psend[block, :, span] = (own + sides[side, block, :, span].astype(f32)).astype(bf16)
                    pass_on(side, block, part).start()

                each_part(one_part)

            return carry

        lax.fori_loop(0, 2, one, 0)

    early = tp_count > 2
    ends = (tp == 0) | (tp == tp_count - 1)

    def hop(k, carry):
        def one_turn(turn):
            def receive(second, carry):
                part = turn - second * LAG
                side = jnp.where(2 * tp < tp_count, second, 1 - second)
                block, inside = at(side, k)

                @pl.when(inside & (part >= 0) & (part < parts))
                def _():
                    send_second(side, block, part).wait_recv()

                    @pl.when(exists(side))
                    def _():
                        send_second(side, block, part).start()

                    @pl.when(part == 0)
                    def _():
                        send_meta(side, block).wait_recv()

                        @pl.when(exists(side))
                        def _():
                            send_meta(side, block).start()

                    @pl.when(late(side) & (k == 1) & (part == parts - 1))
                    def _():
                        for own in range(parts):
                            send_second(side, tp, own).start()

                    pick_part(block, part)

                return carry

            lax.fori_loop(0, 2, receive, 0)

            @pl.when(k == 1)
            def _():
                @pl.when(turn == 1)
                def _():
                    tables()

                @pl.when(turn == 2)
                def _():
                    project(tp)

            if early:

                @pl.when(ends & (k == tp_count - 1) & (turn == LAG + 1))
                def _():
                    reduce_step(1)

            inner = ends & (k > 1) & (k < tp_count - 1) & (turn == LAG + 1)

            @pl.when(inner | ((k == 1) & (turn == LAG + 2)))
            def _():
                experts_at(k - 1)

        each_part(one_turn, parts + LAG)
        for side in range(2):
            start_own_first(side, k)
        for side in range(2):
            block, inside = at(side, k)

            @pl.when(inside)
            def _():
                shared_hidden(block)

        @pl.when((k > 1) & (jnp.logical_not(ends) | (k == tp_count - 1)))
        def _():
            experts_at(k - 1)

        return carry

    lax.fori_loop(1, tp_count, hop, 0)
    if early:
        reduce_step(2)
    experts_at(tp_count - 1)
    for part in range(parts):
        for d in range(1, ep_count):
            return_copy(tp, d, part).start()

    def start_halo(block):
        @pl.when((block == tp_count - 1) & (ep < ep_count - 1))
        def _():
            halo(0).start()

        @pl.when((block == 0) & (ep > 0))
        def _():
            halo(1).start()

    start_halo(tp)

    def attend_inner(block):
        @pl.when((block > 0) & (block < tp_count - 1))
        def _():
            attend(block)

    def first_hop(k, carry):
        for side in range(2):
            block, inside = near(side, k)

            @pl.when(inside & exists(side))
            def _():
                send_first(side, block).wait_recv()
                send_first(side, block).start()

        if early:

            @pl.when(k > 1)
            def _():
                reduce_step(2 * k - 1)

        else:
            reduce_step(2 * k - 1)
        for side in range(2):
            block, inside = near(side, k)

            @pl.when(inside & jnp.logical_not(exists(side)))
            def _():
                send_first(side, block).wait_recv()

        def use(side, carry):
            block = tp + (2 * side - 1) * k

            @pl.when((block >= 0) & (block < tp_count))
            def _():
                project(block)
                start_halo(block)

            return carry

        lax.fori_loop(0, 2, use, 0)

        def settle(side, carry):
            block = tp + (2 * side - 1) * (k - 1)

            @pl.when((block > 0) & (block < tp_count - 1) & ((k > 1) | (side == 0)))
            def _():
                attend(block)

            return carry

        lax.fori_loop(0, 2, settle, 0)

        @pl.when(k == jnp.maximum(tp, tp_count - 1 - tp))
        def _():
            @pl.when(ep < ep_count - 1)
            def _():
                halo(1).wait_recv()

            @pl.when(ep > 0)
            def _():
                halo(0).wait_recv()

            def edge(side, carry):
                attend((tp_count - 1) * (1 - side))
                return carry

            lax.fori_loop(0, 2, edge, 0)

        if early:

            @pl.when(k > 1)
            def _():
                reduce_step(2 * k)

        return carry

    lax.fori_loop(1, tp_count, first_hop, 0)
    own_weights = weights_of(tp)

    def last_part(part):
        span = part_span(part)
        return_part(tp, part).wait_recv()
        own = value_of(tp, own_weights, span)

        @pl.when(tp > 0)
        def _():
            pass_on(0, tp, part).wait_recv()

        @pl.when(tp < tp_count - 1)
        def _():
            pass_on(1, tp, part).wait_recv()

        out[:, span] = (
            own + sides[0, tp, :, span].astype(f32) + sides[1, tp, :, span].astype(f32)
        ).astype(bf16)

    each_part(last_part)

    def finish(block):
        return_all(block).wait_send()
        for side in range(2):
            passed = block <= tp if side == 0 else block >= tp
            summed = block > tp if side == 0 else block < tp

            @pl.when(exists(side) & passed)
            def _():
                ref = gath2.at[block]
                remote(ref, ref, s2.at[side, block], r2.at[block, 0], toward(side)).wait_send()
                send_meta(side, block).wait_send()
                send_first(side, block).wait_send()

            @pl.when(summed)
            def _():
                for part in range(parts):
                    pass_on(side, block, part).wait_send()

    each_part(finish, tp_count)

    @pl.when(ep < ep_count - 1)
    def _():
        halo(0).wait_send()

    @pl.when(ep > 0)
    def _():
        halo(1).wait_send()


def layer(
    second, first, gain_second, gain_first, router, routes, inverse, sink,
    gate, up, down, sgate, sup, sdown, wq, wk, wv, ep_count, tp_count, slots,
):
    rows, width = second.shape
    experts = router.shape[0]
    vmem = pl.BlockSpec(memory_space=pltpu.VMEM)
    smem = pl.BlockSpec(memory_space=pltpu.SMEM)
    hbm = pl.BlockSpec(memory_space=pl.ANY)
    dma = pltpu.SemaphoreType.DMA
    bf16, f32 = jnp.bfloat16, jnp.float32
    total = ep_count * slots
    parts = width // CHUNK
    span = tp_count * rows
    kv_cols = wk.shape[1] + wv.shape[1]
    return pl.pallas_call(
        functools.partial(layer_kernel, ep_count, tp_count, slots),
        out_shape=(
            jax.ShapeDtypeStruct((rows, width), bf16),
            jax.ShapeDtypeStruct((span, wq.shape[1]), bf16),
        ),
        in_specs=[vmem] * 6 + [smem] + [hbm] * 10,
        out_specs=(vmem, vmem),
        scratch_shapes=[
            pltpu.VMEM((tp_count, rows, width), bf16),
            pltpu.VMEM((tp_count, rows, width), bf16),
            pltpu.VMEM((rows, width), bf16),
            pltpu.VMEM((tp_count, 2 * experts, rows), f32),
            pltpu.VMEM((tp_count, total, width), bf16),
            pltpu.VMEM((tp_count, total, width), bf16),
            pltpu.VMEM((tp_count, total, width), bf16),
            pltpu.VMEM((2, tp_count, rows, width), bf16),
            pltpu.VMEM((tp_count, rows, width), bf16),
            pltpu.VMEM(gate.shape[1:], bf16),
            pltpu.VMEM(up.shape[1:], bf16),
            pltpu.VMEM(down.shape[1:], bf16),
            pltpu.VMEM(sgate.shape, bf16),
            pltpu.VMEM(sup.shape, bf16),
            pltpu.VMEM(sdown.shape, bf16),
            pltpu.VMEM(wq.shape, bf16),
            pltpu.VMEM(wk.shape, bf16),
            pltpu.VMEM(wv.shape, bf16),
            pltpu.VMEM((tp_count, rows, sgate.shape[1]), bf16),
            pltpu.VMEM((total, gate.shape[2]), bf16),
            pltpu.VMEM((span, LANES), f32),
            pltpu.VMEM((span, LANES), f32),
            pltpu.VMEM((span, wq.shape[1]), bf16),
            pltpu.VMEM((span + 2 * rows, kv_cols), bf16),
            dma((10,)),
            dma((2, tp_count)),
            dma((tp_count, parts)),
            dma((2, tp_count)),
            dma((tp_count,)),
            dma((2, tp_count)),
            dma((tp_count,)),
            dma((tp_count,)),
            dma((tp_count,)),
            dma((tp_count,)),
            dma((tp_count, parts)),
            dma((tp_count, parts)),
            dma((2, tp_count, parts)),
            dma((2,)),
            dma((2,)),
        ],
        compiler_params=pltpu.CompilerParams(
            collective_id=0, has_side_effects=True, vmem_limit_bytes=VMEM_LIMIT
        ),
        name="layer",
    )(
        second, gain_second, gain_first, router, routes, inverse, sink,
        first, gate, up, down, sgate, sup, sdown, wq, wk, wv,
    )


def body(
    mixer_in,
    mixer_gain,
    w_query,
    w_key,
    w_value,
    sink_logit,
    moe_in,
    moe_gain,
    router,
    routes,
    expert_gate,
    expert_up,
    expert_down,
    shared_gate,
    shared_up,
    shared_down,
):
    tokens = mixer_in.shape[0]
    ep_count, tp_count = lax.axis_size("ep"), lax.axis_size("tp")
    top_count = routes.shape[1]
    experts = router.shape[1]
    capacity = 3 * top_count * tokens // (2 * experts)
    slots = -(-capacity // 16) * 16
    half = HEAD_DIM // 2
    inverse = np.float32(THETA) ** (-(np.arange(half, dtype=np.float32) * np.float32(2.0)) / np.float32(HEAD_DIM))
    moe_out, mixed = layer(
        moe_in, mixer_in, moe_gain[None, :], mixer_gain[None, :], router.T, routes.T,
        jnp.asarray(np.tile(inverse, LANES // half)[None, :]), sink_logit[None, :],
        expert_gate, expert_up, expert_down, shared_gate, shared_up, shared_down,
        w_query, w_key, w_value, ep_count, tp_count, slots,
    )
    return (mixed, moe_out)


def solution(mesh):
    return jax.shard_map(
        body,
        mesh=mesh,
        in_specs=(
            P(("grp", "ep", "tp"), None),
            P(),
            P(None, "tp"),
            P(None, "tp"),
            P(None, "tp"),
            P("tp"),
            P(("grp", "ep", "tp"), None),
            P(),
            P(),
            P(("grp", "ep", "tp"), None),
            P(("ep", "tp"), None, None),
            P(("ep", "tp"), None, None),
            P(("ep", "tp"), None, None),
            P(None, "tp"),
            P(None, "tp"),
            P("tp", None),
        ),
        out_specs=(P(("grp", "ep"), "tp"), P(("grp", "ep", "tp"), None)),
        check_vma=False,
    )
```

```python
import functools

import jax
import jax.numpy as jnp
import numpy as np
from jax import lax
from jax.experimental import pallas as pl
from jax.experimental.pallas import tpu as pltpu
from jax.sharding import PartitionSpec as P

HEAD_DIM = 64
WINDOW = 128
EPS = 1e-06
THETA = 10000.0
ROUTED_SCALE = 2.5
LANES = 128
CHUNK = 512
LAG = 2
MESH = pl.DeviceIdType.MESH
VMEM_LIMIT = 63 * 2**20


def remote(src, dst, send_sem, recv_sem, device):
    return pltpu.make_async_remote_copy(
        src_ref=src,
        dst_ref=dst,
        send_sem=send_sem,
        recv_sem=recv_sem,
        device_id=device,
        device_id_type=MESH,
    )


def greet(grp, ep, tp, ep_count, tp_count):
    barrier = pltpu.get_barrier_semaphore()

    @pl.when(tp > 0)
    def _():
        pl.semaphore_signal(barrier, inc=1, device_id=(grp, ep, tp - 1), device_id_type=MESH)

    @pl.when(tp < tp_count - 1)
    def _():
        pl.semaphore_signal(barrier, inc=1, device_id=(grp, ep, tp + 1), device_id_type=MESH)

    for d in range(1, ep_count):
        pl.semaphore_signal(
            barrier, inc=1, device_id=(grp, lax.rem(ep + d, ep_count), tp), device_id_type=MESH
        )
    return barrier


def layer_kernel(
    ep_count, tp_count, slots,
    second_in, gain_second, gain_first, router, routes, inverse, sink,
    first_hbm, gate_hbm, up_hbm, down_hbm, sgate_hbm, sup_hbm, sdown_hbm, wq_hbm, wk_hbm, wv_hbm,
    out, mixed_out,
    mixed, gath2, gath1, first_in, metag, sbuf, disp, back, sides, psend,
    gate, up, down, sgate, sup, sdown, wq, wk, wv,
    hidden, hexp, cosine, sine, qbuf, kvbuf,
    l_sem, s2, r2, sm, rm, s1, r1, sd, rd, sb, rb, sp, rs, hs, hr, out_sem, mixed_sem,
):
    grp, ep, tp = lax.axis_index("grp"), lax.axis_index("ep"), lax.axis_index("tp")
    rows, width = second_in.shape
    experts = metag.shape[1] // 2
    total = ep_count * slots
    parts = width // CHUNK
    f32, bf16 = jnp.float32, jnp.bfloat16
    away = pl.ds(slots, total - slots)

    local = [
        pltpu.make_async_copy(src, dst, l_sem.at[i])
        for i, (src, dst) in enumerate(
            [
                (first_hbm, first_in),
                (sgate_hbm, sgate),
                (sup_hbm, sup),
                (gate_hbm.at[0], gate),
                (up_hbm.at[0], up),
                (down_hbm.at[0], down),
                (wq_hbm, wq),
                (wk_hbm, wk),
                (wv_hbm, wv),
                (sdown_hbm, sdown),
            ]
        )
    ]
    for copy in local:
        copy.start()
    barrier = greet(grp, ep, tp, ep_count, tp_count)

    def toward(side):
        return (grp, ep, tp + 1 - 2 * side)

    def exists(side):
        return (tp + 1 - 2 * side >= 0) & (tp + 1 - 2 * side < tp_count)

    def peer(d):
        return (grp, lax.rem(ep + d, ep_count), tp)

    def part_span(part, size=CHUNK):
        return pl.ds(pl.multiple_of(part * size, size), size)

    def each_part(body, count=parts):
        def step(part, carry):
            body(part)
            return carry

        lax.fori_loop(0, count, step, 0)

    def near(side, distance):
        block = tp + (2 * side - 1) * distance
        return block, (block >= 0) & (block < tp_count)

    swaps = tp_count > 2

    def swapped(side, block, allowed):
        far, second = (tp_count - 1) * side, 1 + (tp_count - 3) * side
        other = jnp.where(block == second, far, jnp.where(block == far, second, block))
        return jnp.where(allowed, other, block)

    def at(side, order):
        block, inside = near(side, order)
        if swaps:
            block = swapped(side, block, jnp.where(side == 0, tp, tp_count - 1 - tp) >= 2)
        return block, inside

    def late(side):
        return (tp == 1 + side * (tp_count - 3)) & swaps

    def send_second(side, block, part):
        ref = gath2.at[block, :, part_span(part)]
        return remote(ref, ref, s2.at[side, block], r2.at[block, part], toward(side))

    def send_meta(side, block):
        return remote(metag.at[block], metag.at[block], sm.at[side, block], rm.at[block], toward(side))

    def send_first(side, block):
        return remote(gath1.at[block], gath1.at[block], s1.at[side, block], r1.at[block], toward(side))

    def dispatch_copy(block, d, span):
        mine = pl.ds(d * slots, slots)
        return remote(sbuf.at[block, mine, span], disp.at[block, mine, span], sd.at[block], rd.at[block], peer(d))

    def dispatch_all(block):
        return remote(sbuf.at[block, away], disp.at[block, away], sd.at[block], rd.at[block], peer(1))

    def return_copy(block, d, part):
        mine, span = pl.ds(d * slots, slots), part_span(part)
        return remote(
            sbuf.at[block, mine, span], back.at[block, mine, span],
            sb.at[block], rb.at[block, part], peer(ep_count - d),
        )

    def return_part(block, part):
        span = part_span(part)
        return remote(
            sbuf.at[block, away, span], back.at[block, away, span], sb.at[block], rb.at[block, part], peer(1)
        )

    def return_all(block):
        return remote(sbuf.at[block, away], back.at[block, away], sb.at[block], rb.at[block, 0], peer(1))

    def pass_on(side, block, part):
        span = part_span(part)
        return remote(
            psend.at[block, :, span], sides.at[side, block, :, span],
            sp.at[block, part], rs.at[side, block, part], toward(side),
        )

    def halo(side):
        source = tp_count * rows if side == 0 else rows
        target = 0 if side == 0 else (tp_count + 1) * rows
        return remote(
            kvbuf.at[pl.ds(source, rows)], kvbuf.at[pl.ds(target, rows)],
            hs.at[side], hr.at[side], (grp, ep + (1 if side == 0 else -1), tp),
        )

    def out_copy(part):
        span = part_span(part)
        return pltpu.make_async_copy(psend.at[tp, :, span], out.at[:, span], out_sem.at[part])

    def mixed_copy(block):
        span = part_span(block, rows)
        return pltpu.make_async_copy(mixed.at[span], mixed_out.at[span], mixed_sem.at[block])

    def normalize(source, gain, target):
        def squares(part, carry):
            values = source[:, part_span(part)].astype(f32)
            return carry + jnp.sum(values * values, axis=1, keepdims=True)

        summed = lax.fori_loop(0, parts, squares, jnp.zeros((rows, 1), f32))
        factor = lax.rsqrt(summed / width + EPS)

        def scale(part):
            span = part_span(part)
            target[:, span] = (source[:, span].astype(f32) * factor * gain[:, span]).astype(bf16)

        each_part(scale)

    def places_of(block, d):
        expert = lax.rem(ep + d, ep_count) * tp_count + tp
        slot_ids = lax.broadcasted_iota(jnp.int32, (slots, rows), 0).astype(f32)
        return slot_ids == metag[block, pl.ds(expert, 1), :], expert

    def pick_part(block, part):
        span = part_span(part)
        picks = [jnp.where(places_of(block, d)[0], 1.0, 0.0) for d in range(ep_count)]
        pick = jnp.concatenate(picks, axis=0).astype(bf16)
        picked = jnp.dot(pick, gath2[block, :, span], preferred_element_type=f32).astype(bf16)
        disp[block, 0:slots, span] = picked[0:slots]
        sbuf[block, slots:total, span] = picked[slots:total]
        for d in range(1, ep_count):
            dispatch_copy(block, d, span).start()

    def shared_hidden(block):
        values = gath2[block]
        gated = jnp.dot(values, sgate[...], preferred_element_type=f32)
        lifted = jnp.dot(values, sup[...], preferred_element_type=f32)
        hidden[block] = (jax.nn.silu(gated) * lifted).astype(bf16)

    def expert(block):
        dispatch_all(block).wait()

        def units(part):
            span = part_span(part, 256)
            values = disp[block]
            gated = jnp.dot(values, gate[:, span], preferred_element_type=f32)
            lifted = jnp.dot(values, up[:, span], preferred_element_type=f32)
            hexp[:, span] = (jax.nn.silu(gated) * lifted).astype(bf16)

        each_part(units, gate.shape[1] // 256)

        def columns(part):
            span = part_span(part)
            result = jnp.dot(hexp[...], down[:, span], preferred_element_type=f32).astype(bf16)
            back[block, 0:slots, span] = result[0:slots]
            sbuf[block, slots:total, span] = result[slots:total]

            @pl.when(block != tp)
            def _():
                for d in range(1, ep_count):
                    return_copy(block, d, part).start()

        each_part(columns)

    def experts_at(order):
        def one(side, carry):
            block, inside = at(side, order)

            @pl.when(inside & ((order > 0) | (side == 0)))
            def _():
                expert(block)

            return carry

        lax.fori_loop(0, 2, one, 0)

    def start_own_first(side, step):
        last = tp if side == 0 else tp_count - 1 - tp

        @pl.when(exists(side) & (step == last))
        def _():
            send_first(side, tp).start()

    def rotated(values, cos_rows, sin_rows):
        pieces = []
        half = HEAD_DIM // 2
        size = LANES if values.shape[1] % LANES == 0 else HEAD_DIM
        for start in range(0, values.shape[1], size):
            piece = values[:, start : start + size]
            if size == LANES:
                lane = lax.broadcasted_iota(jnp.int32, piece.shape, 1)
                crossed = jnp.where(
                    lax.rem(lane, HEAD_DIM) < half,
                    pltpu.roll(piece, LANES - half, 1),
                    pltpu.roll(piece, half, 1),
                )
            else:
                crossed = jnp.concatenate([piece[:, half:], piece[:, :half]], axis=1)
            pieces.append(piece * cos_rows[:, :size] + crossed * sin_rows[:, :size])
        return pieces[0] if len(pieces) == 1 else jnp.concatenate(pieces, axis=1)

    def project(block):
        base = pl.multiple_of(block * rows, rows)
        values = gath1[block]
        cos_rows, sin_rows = cosine[pl.ds(base, rows), :], sine[pl.ds(base, rows), :]
        query = jnp.dot(values, wq[...], preferred_element_type=f32)
        key = jnp.dot(values, wk[...], preferred_element_type=f32)
        value = jnp.dot(values, wv[...], preferred_element_type=f32)
        qbuf[pl.ds(base, rows), :] = rotated(query, cos_rows, sin_rows).astype(bf16)
        kvbuf[pl.ds(pl.multiple_of(base + rows, rows), rows), :] = jnp.concatenate(
            [rotated(key, cos_rows, sin_rows), value], axis=1
        ).astype(bf16)

    def start_halo(block):
        @pl.when((block == tp_count - 1) & (ep < ep_count - 1))
        def _():
            halo(0).start()

        @pl.when((block == 0) & (ep > 0))
        def _():
            halo(1).start()

    def tables():
        def one(block):
            start = pl.multiple_of(block * rows, rows)
            shape = (rows, LANES)
            place = ep * (tp_count * rows) + start + lax.broadcasted_iota(jnp.int32, shape, 0)
            angle = place.astype(f32) * inverse[...]
            lane = lax.broadcasted_iota(jnp.int32, shape, 1)
            turn = jnp.sin(angle)
            cosine[pl.ds(start, rows), :] = jnp.cos(angle)
            sine[pl.ds(start, rows), :] = jnp.where(lax.rem(lane, HEAD_DIM) < HEAD_DIM // 2, -turn, turn)

        each_part(one, tp_count)

    kv_heads = wk.shape[1] // HEAD_DIM
    group = wq.shape[1] // wk.shape[1]

    def attend(block):
        base = pl.multiple_of(block * rows, rows)
        window = kvbuf[pl.ds(base, 3 * rows), :]
        query = qbuf[pl.ds(base, rows), :]
        shape = (rows, 3 * rows)
        row = lax.broadcasted_iota(jnp.int32, shape, 0)
        col = lax.broadcasted_iota(jnp.int32, shape, 1)
        gap = col - row - rows
        low = jnp.where((ep == 0) & (block == 0), rows, 0)
        high = jnp.where((ep == ep_count - 1) & (block == tp_count - 1), 2 * rows, 3 * rows)
        near = (gap <= WINDOW) & (gap >= -WINDOW) & (col >= low) & (col < high)
        pieces = []
        for g in range(kv_heads):
            keys = window[:, g * HEAD_DIM : (g + 1) * HEAD_DIM]
            start = (kv_heads + g) * HEAD_DIM
            values = window[:, start : start + HEAD_DIM]
            for h in range(g * group, (g + 1) * group):
                scores = lax.dot_general(
                    query[:, h * HEAD_DIM : (h + 1) * HEAD_DIM], keys, (((1,), (1,)), ((), ())),
                    preferred_element_type=f32,
                ) * HEAD_DIM ** (-0.5)
                scores = jnp.where(near, scores, -jnp.inf)
                bound = sink[0, h]
                top = jnp.maximum(jnp.max(scores, axis=1, keepdims=True), bound)
                weights = jnp.exp(scores - top)
                summed = jnp.sum(weights, axis=1, keepdims=True) + jnp.exp(bound - top)
                share = (weights * (1.0 / summed)).astype(bf16)
                pieces.append(jnp.dot(share, values, preferred_element_type=f32))
        mixed[pl.ds(base, rows), :] = jnp.concatenate(pieces, axis=1).astype(bf16)
        mixed_copy(block).start()

    normalize(second_in, gain_second, gath2.at[tp])
    ids = lax.broadcasted_iota(jnp.int32, (experts, rows), 0)
    hit = ids == routes[0:1, :]
    for j in range(1, routes.shape[0]):
        hit = hit | (ids == routes[j : j + 1, :])
    earlier = (
        lax.broadcasted_iota(jnp.int32, (rows, rows), 0) < lax.broadcasted_iota(jnp.int32, (rows, rows), 1)
    )
    before = jnp.dot(
        jnp.where(hit, 1.0, 0.0).astype(bf16), jnp.where(earlier, 1.0, 0.0).astype(bf16),
        preferred_element_type=f32,
    )
    metag[tp, 0:experts, :] = jnp.where(hit, before, -1.0)
    pl.semaphore_wait(barrier, ep_count + jnp.where((tp > 0) & (tp < tp_count - 1), 1, 0))
    def send_own(part):
        for side in range(2):

            @pl.when(exists(side) & jnp.logical_not(late(side)))
            def _():
                send_second(side, tp, part).start()

    send_own(0)
    affinity = lax.dot_general(
        router[...], gath2[tp], (((1,), (1,)), ((), ())), preferred_element_type=f32
    )
    chosen = jnp.where(hit, jax.nn.sigmoid(affinity), 0.0)
    metag[tp, experts : 2 * experts, :] = ROUTED_SCALE * chosen / jnp.sum(chosen, axis=0, keepdims=True)
    pick_part(tp, 0)
    for side in range(2):

        @pl.when(exists(side))
        def _():
            send_meta(side, tp).start()

    for part in range(1, parts):
        send_own(part)

    def pick_rest(part, carry):
        pick_part(tp, part)
        return carry

    lax.fori_loop(1, parts, pick_rest, 0)
    local[0].wait()
    normalize(first_in, gain_first, gath1.at[tp])
    for side in range(2):
        start_own_first(side, 0)

    @pl.when(tp == 0)
    def _():
        sides[0] = jnp.zeros(sides.shape[1:], sides.dtype)

    @pl.when(tp == tp_count - 1)
    def _():
        sides[1] = jnp.zeros(sides.shape[1:], sides.dtype)

    @pl.when(ep == 0)
    def _():
        kvbuf[0:rows, :] = jnp.zeros((rows, kvbuf.shape[1]), bf16)

    @pl.when(ep == ep_count - 1)
    def _():
        kvbuf[(tp_count + 1) * rows : (tp_count + 2) * rows, :] = jnp.zeros((rows, kvbuf.shape[1]), bf16)

    for copy in local[1:]:
        copy.wait()
    shared_hidden(tp)

    def weights_of(block):
        pieces = []
        for d in range(ep_count):
            hit_rows, number = places_of(block, d)
            pieces.append(jnp.where(hit_rows, metag[block, pl.ds(experts + number, 1), :], 0.0))
        weights = jnp.concatenate(pieces, axis=0)
        top = weights.astype(bf16)
        return top, (weights - top.astype(f32)).astype(bf16)

    def value_of(block, weights, span):
        turned = (((0,), (0,)), ((), ()))
        picked = back[block, :, span]
        return (
            lax.dot_general(weights[0], picked, turned, preferred_element_type=f32)
            + lax.dot_general(weights[1], picked, turned, preferred_element_type=f32)
            + jnp.dot(hidden[block], sdown[:, span], preferred_element_type=f32)
        )

    def reduce_step(step):
        def one(turn, carry):
            side = jnp.where(2 * tp < tp_count, 1 - turn, turn)
            block = jnp.where(side == 0, step - tp, 2 * (tp_count - 1) - step - tp)
            active = (block >= 0) & (block < tp_count)
            if swaps:
                block = swapped(1 - side, block, True)
            active = active & ((block - tp) * (1 - 2 * side) > 0)

            @pl.when(active)
            def _():
                weights = weights_of(block)

                def one_part(part):
                    span = part_span(part)
                    return_part(block, part).wait_recv()
                    own = value_of(block, weights, span)

                    @pl.when(exists(1 - side))
                    def _():
                        pass_on(side, block, part).wait_recv()

                    psend[block, :, span] = (own + sides[side, block, :, span].astype(f32)).astype(bf16)
                    pass_on(side, block, part).start()

                each_part(one_part)

            return carry

        lax.fori_loop(0, 2, one, 0)

    early = tp_count > 2
    ends = (tp == 0) | (tp == tp_count - 1)

    def hop(k, carry):
        def one_turn(turn):
            def receive(second, carry):
                part = turn - second * LAG
                side = jnp.where(2 * tp < tp_count, second, 1 - second)
                block, inside = at(side, k)

                @pl.when(inside & (part >= 0) & (part < parts))
                def _():
                    send_second(side, block, part).wait_recv()

                    @pl.when(exists(side))
                    def _():
                        send_second(side, block, part).start()

                    @pl.when(part == 0)
                    def _():
                        send_meta(side, block).wait_recv()

                        @pl.when(exists(side))
                        def _():
                            send_meta(side, block).start()

                    @pl.when(late(side) & (k == 1) & (part == parts - 1))
                    def _():
                        for own in range(parts):
                            send_second(side, tp, own).start()

                    pick_part(block, part)

                return carry

            lax.fori_loop(0, 2, receive, 0)

            @pl.when(k == 1)
            def _():
                @pl.when(turn == 1)
                def _():
                    tables()

                @pl.when(turn == 2)
                def _():
                    project(tp)
                    start_halo(tp)

            if early:

                @pl.when(ends & (k == tp_count - 1) & (turn == LAG + 1))
                def _():
                    reduce_step(1)

            inner = ends & (k > 1) & (k < tp_count - 1) & (turn == LAG + 1)

            @pl.when(inner | ((k == 1) & (turn == LAG + 2)))
            def _():
                experts_at(k - 1)

        each_part(one_turn, parts + LAG)
        for side in range(2):
            start_own_first(side, k)
        for side in range(2):
            block, inside = at(side, k)

            @pl.when(inside)
            def _():
                shared_hidden(block)

        @pl.when((k > 1) & (jnp.logical_not(ends) | (k == tp_count - 1)))
        def _():
            experts_at(k - 1)

        return carry

    lax.fori_loop(1, tp_count, hop, 0)
    experts_at(tp_count - 1)

    def give_back(low, high):
        for part in range(low, high):
            for d in range(1, ep_count):
                return_copy(tp, d, part).start()

    give_back(0, parts // 2)
    if early:
        reduce_step(2)

    def first_hop(k, carry):
        for side in range(2):
            block, inside = near(side, k)

            @pl.when(inside & exists(side))
            def _():
                send_first(side, block).wait_recv()
                send_first(side, block).start()

        if early:

            @pl.when(k > 1)
            def _():
                reduce_step(2 * k - 1)

        else:
            reduce_step(2 * k - 1)
        for side in range(2):
            block, inside = near(side, k)

            @pl.when(inside & jnp.logical_not(exists(side)))
            def _():
                send_first(side, block).wait_recv()

        def use(side, carry):
            block = tp + (2 * side - 1) * k

            @pl.when((block >= 0) & (block < tp_count))
            def _():
                project(block)
                start_halo(block)

            return carry

        lax.fori_loop(0, 2, use, 0)

        @pl.when(k == jnp.maximum(tp, tp_count - 1 - tp))
        def _():
            give_back(parts // 2, parts)

        def settle(side, carry):
            block = tp + (2 * side - 1) * (k - 1)

            @pl.when((block > 0) & (block < tp_count - 1) & ((k > 1) | (side == 0)))
            def _():
                attend(block)

            return carry

        lax.fori_loop(0, 2, settle, 0)

        if early:

            @pl.when(k > 1)
            def _():
                reduce_step(2 * k)

        return carry

    lax.fori_loop(1, tp_count, first_hop, 0)

    @pl.when(ep < ep_count - 1)
    def _():
        halo(1).wait_recv()

    @pl.when(ep > 0)
    def _():
        halo(0).wait_recv()

    def edge(side, carry):
        attend((tp_count - 1) * (1 - side))
        return carry

    lax.fori_loop(0, 2, edge, 0)
    own_weights = weights_of(tp)

    def last_part(part):
        span = part_span(part)
        return_part(tp, part).wait_recv()
        own = value_of(tp, own_weights, span)

        @pl.when(tp > 0)
        def _():
            pass_on(0, tp, part).wait_recv()

        @pl.when(tp < tp_count - 1)
        def _():
            pass_on(1, tp, part).wait_recv()

        psend[tp, :, span] = (
            own + sides[0, tp, :, span].astype(f32) + sides[1, tp, :, span].astype(f32)
        ).astype(bf16)
        out_copy(part).start()

    each_part(last_part)

    def finish(block):
        return_all(block).wait_send()
        for side in range(2):
            passed = block <= tp if side == 0 else block >= tp
            summed = block > tp if side == 0 else block < tp

            @pl.when(exists(side) & passed)
            def _():
                ref = gath2.at[block]
                remote(ref, ref, s2.at[side, block], r2.at[block, 0], toward(side)).wait_send()
                send_meta(side, block).wait_send()
                send_first(side, block).wait_send()

            @pl.when(summed)
            def _():
                for part in range(parts):
                    pass_on(side, block, part).wait_send()

    each_part(finish, tp_count)
    each_part(lambda part: out_copy(part).wait())
    each_part(lambda block: mixed_copy(block).wait(), tp_count)

    @pl.when(ep < ep_count - 1)
    def _():
        halo(0).wait_send()

    @pl.when(ep > 0)
    def _():
        halo(1).wait_send()


def layer(
    second, first, gain_second, gain_first, router, routes, inverse, sink,
    gate, up, down, sgate, sup, sdown, wq, wk, wv, ep_count, tp_count, slots,
):
    rows, width = second.shape
    experts = router.shape[0]
    vmem = pl.BlockSpec(memory_space=pltpu.VMEM)
    smem = pl.BlockSpec(memory_space=pltpu.SMEM)
    hbm = pl.BlockSpec(memory_space=pl.ANY)
    dma = pltpu.SemaphoreType.DMA
    bf16, f32 = jnp.bfloat16, jnp.float32
    total = ep_count * slots
    parts = width // CHUNK
    span = tp_count * rows
    kv_cols = wk.shape[1] + wv.shape[1]
    return pl.pallas_call(
        functools.partial(layer_kernel, ep_count, tp_count, slots),
        out_shape=(
            jax.ShapeDtypeStruct((rows, width), bf16),
            jax.ShapeDtypeStruct((span, wq.shape[1]), bf16),
        ),
        in_specs=[vmem] * 6 + [smem] + [hbm] * 10,
        out_specs=(hbm, hbm),
        scratch_shapes=[
            pltpu.VMEM((span, wq.shape[1]), bf16),
            pltpu.VMEM((tp_count, rows, width), bf16),
            pltpu.VMEM((tp_count, rows, width), bf16),
            pltpu.VMEM((rows, width), bf16),
            pltpu.VMEM((tp_count, 2 * experts, rows), f32),
            pltpu.VMEM((tp_count, total, width), bf16),
            pltpu.VMEM((tp_count, total, width), bf16),
            pltpu.VMEM((tp_count, total, width), bf16),
            pltpu.VMEM((2, tp_count, rows, width), bf16),
            pltpu.VMEM((tp_count, rows, width), bf16),
            pltpu.VMEM(gate.shape[1:], bf16),
            pltpu.VMEM(up.shape[1:], bf16),
            pltpu.VMEM(down.shape[1:], bf16),
            pltpu.VMEM(sgate.shape, bf16),
            pltpu.VMEM(sup.shape, bf16),
            pltpu.VMEM(sdown.shape, bf16),
            pltpu.VMEM(wq.shape, bf16),
            pltpu.VMEM(wk.shape, bf16),
            pltpu.VMEM(wv.shape, bf16),
            pltpu.VMEM((tp_count, rows, sgate.shape[1]), bf16),
            pltpu.VMEM((total, gate.shape[2]), bf16),
            pltpu.VMEM((span, LANES), f32),
            pltpu.VMEM((span, LANES), f32),
            pltpu.VMEM((span, wq.shape[1]), bf16),
            pltpu.VMEM((span + 2 * rows, kv_cols), bf16),
            dma((10,)),
            dma((2, tp_count)),
            dma((tp_count, parts)),
            dma((2, tp_count)),
            dma((tp_count,)),
            dma((2, tp_count)),
            dma((tp_count,)),
            dma((tp_count,)),
            dma((tp_count,)),
            dma((tp_count,)),
            dma((tp_count, parts)),
            dma((tp_count, parts)),
            dma((2, tp_count, parts)),
            dma((2,)),
            dma((2,)),
            dma((parts,)),
            dma((tp_count,)),
        ],
        compiler_params=pltpu.CompilerParams(
            collective_id=0, has_side_effects=True, vmem_limit_bytes=VMEM_LIMIT
        ),
        name="layer",
    )(
        second, gain_second, gain_first, router, routes, inverse, sink,
        first, gate, up, down, sgate, sup, sdown, wq, wk, wv,
    )


def settle_kernel(first, second, first_out, second_out, first_buf, second_buf, sems):
    arrays = [(first, first_buf, first_out), (second, second_buf, second_out)]
    pieces = []
    for i, (source, buffer, target) in enumerate(arrays):
        half = source.shape[0] // 2
        for j in range(2):
            rows = pl.ds(j * half, half)
            pieces.append(
                (
                    pltpu.make_async_copy(source.at[rows], buffer.at[rows], sems.at[0, i, j]),
                    pltpu.make_async_copy(buffer.at[rows], target.at[rows], sems.at[1, i, j]),
                )
            )
    for load, _ in pieces:
        load.start()
    for load, store in pieces:
        load.wait()
        store.start()
    for _, store in pieces:
        store.wait()


def settle(first, second):
    hbm = pl.BlockSpec(memory_space=pl.ANY)
    return pl.pallas_call(
        settle_kernel,
        out_shape=(jax.ShapeDtypeStruct(first.shape, first.dtype), jax.ShapeDtypeStruct(second.shape, second.dtype)),
        in_specs=[hbm, hbm],
        out_specs=(hbm, hbm),
        scratch_shapes=[
            pltpu.VMEM(first.shape, first.dtype),
            pltpu.VMEM(second.shape, second.dtype),
            pltpu.SemaphoreType.DMA((2, 2, 2)),
        ],
        compiler_params=pltpu.CompilerParams(vmem_limit_bytes=VMEM_LIMIT),
        name="settle",
    )(first, second)


def body(
    mixer_in,
    mixer_gain,
    w_query,
    w_key,
    w_value,
    sink_logit,
    moe_in,
    moe_gain,
    router,
    routes,
    expert_gate,
    expert_up,
    expert_down,
    shared_gate,
    shared_up,
    shared_down,
):
    tokens = mixer_in.shape[0]
    ep_count, tp_count = lax.axis_size("ep"), lax.axis_size("tp")
    top_count = routes.shape[1]
    experts = router.shape[1]
    capacity = 3 * top_count * tokens // (2 * experts)
    slots = -(-capacity // 16) * 16
    half = HEAD_DIM // 2
    inverse = np.float32(THETA) ** (-(np.arange(half, dtype=np.float32) * np.float32(2.0)) / np.float32(HEAD_DIM))
    moe_out, mixed = layer(
        moe_in, mixer_in, moe_gain[None, :], mixer_gain[None, :], router.T, routes.T,
        jnp.asarray(np.tile(inverse, LANES // half)[None, :]), sink_logit[None, :],
        expert_gate, expert_up, expert_down, shared_gate, shared_up, shared_down,
        w_query, w_key, w_value, ep_count, tp_count, slots,
    )
    moe_out, mixed = settle(moe_out, mixed)
    return (mixed, moe_out)


def solution(mesh):
    return jax.shard_map(
        body,
        mesh=mesh,
        in_specs=(
            P(("grp", "ep", "tp"), None),
            P(),
            P(None, "tp"),
            P(None, "tp"),
            P(None, "tp"),
            P("tp"),
            P(("grp", "ep", "tp"), None),
            P(),
            P(),
            P(("grp", "ep", "tp"), None),
            P(("ep", "tp"), None, None),
            P(("ep", "tp"), None, None),
            P(("ep", "tp"), None, None),
            P(None, "tp"),
            P(None, "tp"),
            P("tp", None),
        ),
        out_specs=(P(("grp", "ep"), "tp"), P(("grp", "ep", "tp"), None)),
        check_vma=False,
    )
```

```python
import functools

import jax
import jax.numpy as jnp
import numpy as np
from jax import lax
from jax.experimental import pallas as pl
from jax.experimental.pallas import tpu as pltpu
from jax.sharding import PartitionSpec as P

HEAD_DIM = 64
WINDOW = 128
EPS = 1e-06
THETA = 10000.0
ROUTED_SCALE = 2.5
LANES = 128
CHUNK = 512
LAG = 2
MESH = pl.DeviceIdType.MESH
VMEM_LIMIT = 63 * 2**20


def remote(src, dst, send_sem, recv_sem, device):
    return pltpu.make_async_remote_copy(
        src_ref=src,
        dst_ref=dst,
        send_sem=send_sem,
        recv_sem=recv_sem,
        device_id=device,
        device_id_type=MESH,
    )


def greet(grp, ep, tp, grp_count, ep_count, tp_count):
    barrier = pltpu.get_barrier_semaphore()

    @pl.when(tp > 0)
    def _():
        pl.semaphore_signal(barrier, inc=1, device_id=(grp, ep, tp - 1), device_id_type=MESH)

    @pl.when(tp < tp_count - 1)
    def _():
        pl.semaphore_signal(barrier, inc=1, device_id=(grp, ep, tp + 1), device_id_type=MESH)

    for d in range(1, ep_count):
        pl.semaphore_signal(
            barrier, inc=1, device_id=(grp, lax.rem(ep + d, ep_count), tp), device_id_type=MESH
        )
    for d in range(1, grp_count):
        pl.semaphore_signal(
            barrier, inc=1, device_id=(lax.rem(grp + d, grp_count), ep, tp), device_id_type=MESH
        )
    return barrier


def layer_kernel(
    grp_count, ep_count, tp_count, slots,
    second_in, gain_second, gain_first, router, routes, inverse, sink,
    first_hbm, gate_hbm, up_hbm, down_hbm, sgate_hbm, sup_hbm, sdown_hbm, wq_hbm, wk_hbm, wv_hbm,
    out, mixed_out,
    mixed, gath2, gath1, first_in, metag, sbuf, disp, back, sides, psend,
    gate, up, down, sgate, sup, sdown, wq, wk, wv, far_q, far_k, far_v, lent_q, lent_kv,
    hidden, hexp, cosine, sine, qbuf, kvbuf,
    l_sem, s2, r2, sm, rm, s1, r1, sd, rd, sb, rb, sp, rs, hs, hr, out_sem, mixed_sem, ws, wr, qs, qr,
):
    grp, ep, tp = lax.axis_index("grp"), lax.axis_index("ep"), lax.axis_index("tp")
    rows, width = second_in.shape
    experts = metag.shape[1] // 2
    total = ep_count * slots
    parts = width // CHUNK
    f32, bf16 = jnp.float32, jnp.bfloat16
    away = pl.ds(slots, total - slots)

    local = [
        pltpu.make_async_copy(src, dst, l_sem.at[i])
        for i, (src, dst) in enumerate(
            [
                (first_hbm, first_in),
                (sgate_hbm, sgate),
                (sup_hbm, sup),
                (gate_hbm.at[0], gate),
                (up_hbm.at[0], up),
                (down_hbm.at[0], down),
                (wq_hbm, wq),
                (wk_hbm, wk),
                (wv_hbm, wv),
                (sdown_hbm, sdown),
            ]
        )
    ]
    for copy in local:
        copy.start()
    barrier = greet(grp, ep, tp, grp_count, ep_count, tp_count)

    def toward(side):
        return (grp, ep, tp + 1 - 2 * side)

    def exists(side):
        return (tp + 1 - 2 * side >= 0) & (tp + 1 - 2 * side < tp_count)

    def peer(d):
        return (grp, lax.rem(ep + d, ep_count), tp)

    def part_span(part, size=CHUNK):
        return pl.ds(pl.multiple_of(part * size, size), size)

    def each_part(body, count=parts):
        def step(part, carry):
            body(part)
            return carry

        lax.fori_loop(0, count, step, 0)

    def near(side, distance):
        block = tp + (2 * side - 1) * distance
        return block, (block >= 0) & (block < tp_count)

    swaps = tp_count > 2

    def swapped(side, block, allowed):
        far, second = (tp_count - 1) * side, 1 + (tp_count - 3) * side
        other = jnp.where(block == second, far, jnp.where(block == far, second, block))
        return jnp.where(allowed, other, block)

    def at(side, order):
        block, inside = near(side, order)
        if swaps:
            block = swapped(side, block, jnp.where(side == 0, tp, tp_count - 1 - tp) >= 2)
        return block, inside

    def late(side):
        return (tp == 1 + side * (tp_count - 3)) & swaps

    def send_second(side, block, part):
        ref = gath2.at[block, :, part_span(part)]
        return remote(ref, ref, s2.at[side, block], r2.at[block, part], toward(side))

    def send_meta(side, block):
        return remote(metag.at[block], metag.at[block], sm.at[side, block], rm.at[block], toward(side))

    assist = tp_count >= 4
    ends = (tp == 0) | (tp == tp_count - 1)
    slim = tp_count == 4
    plain = jnp.logical_not(ends) | (not assist)
    helps = ((tp == 1) | (tp == tp_count - 2)) & assist
    outward = jnp.where(tp == 1, 1, 0)
    pair = 2 if ep_count % 2 == 0 else 1
    core = lax.rem(ep, pair)
    piece_rows = width // (grp_count * pair)
    lent = [(wq, far_q), (wk, far_k), (wv, far_v)]

    def carries(side):
        target = tp + 1 - 2 * side
        return exists(side) & (((target > 0) & (target < tp_count - 1)) | (not assist))

    def share_of(group, half):
        return group * pair + half

    def lend(share, to, device, own):
        span = pl.ds(pl.multiple_of(share * piece_rows, piece_rows), piece_rows)
        return [
            remote(
                (near_ref if own else far_ref).at[span], far_ref.at[span],
                ws.at[share, to, i], wr.at[share, i], device,
            )
            for i, (near_ref, far_ref) in enumerate(lent)
        ]

    def lend_out():
        return lend(share_of(grp, core), 0, (grp, ep, jnp.where(tp == 0, 1, tp_count - 2)), True)

    def partner():
        return (grp, ep + 1 - 2 * core, tp)

    def relays():
        mine = share_of(grp, core)
        copies = []
        for d in range(1, grp_count):
            copies.append(lend(mine, d, (lax.rem(grp + d, grp_count), ep, tp), False))
        if pair == 2:
            copies.append(lend(mine, 0, partner(), False))
        return copies

    def relays_across():
        copies = []
        for d in range(1, grp_count):
            copies.append(lend(share_of(lax.rem(grp + d, grp_count), core), 0, partner(), False))
        return copies

    def relay_first():
        for copy in lend(share_of(grp, core), 0, toward(outward), False):
            copy.wait_recv()
        for copies in relays():
            for copy in copies:
                copy.start()

    def relay_second():
        for copies in relays_across():
            for copy in copies:
                copy.wait_recv()
            if pair == 2:
                for copy in copies:
                    copy.start()

    def relay_last():
        if pair == 2:
            for group in range(grp_count):
                for copy in lend(share_of(group, 1 - core), 0, partner(), False):
                    copy.wait_recv()

    def query_copy(block, device):
        return remote(
            lent_q.at[block], qbuf.at[part_span(block, rows)], qs.at[0, block], qr.at[0, block], device
        )

    def kv_copy(block, device):
        return remote(
            lent_kv.at[block], kvbuf.at[part_span(block + 1, rows)], qs.at[1, block], qr.at[1, block], device
        )

    def send_first(side, block):
        return remote(gath1.at[block], gath1.at[block], s1.at[side, block], r1.at[block], toward(side))

    def dispatch_copy(block, d, span):
        mine = pl.ds(d * slots, slots)
        return remote(sbuf.at[block, mine, span], disp.at[block, mine, span], sd.at[block], rd.at[block], peer(d))

    def dispatch_all(block):
        return remote(sbuf.at[block, away], disp.at[block, away], sd.at[block], rd.at[block], peer(1))

    def return_copy(block, d, part):
        mine, span = pl.ds(d * slots, slots), part_span(part)
        return remote(
            sbuf.at[block, mine, span], back.at[block, mine, span],
            sb.at[block], rb.at[block, part], peer(ep_count - d),
        )

    def return_part(block, part):
        span = part_span(part)
        return remote(
            sbuf.at[block, away, span], back.at[block, away, span], sb.at[block], rb.at[block, part], peer(1)
        )

    def return_all(block):
        return remote(sbuf.at[block, away], back.at[block, away], sb.at[block], rb.at[block, 0], peer(1))

    def pass_on(side, block, part):
        span = part_span(part)
        return remote(
            psend.at[block, :, span], sides.at[side, block, :, span],
            sp.at[block, part], rs.at[side, block, part], toward(side),
        )

    def halo(side):
        source = tp_count * rows if side == 0 else rows
        target = 0 if side == 0 else (tp_count + 1) * rows
        return remote(
            kvbuf.at[pl.ds(source, rows)], kvbuf.at[pl.ds(target, rows)],
            hs.at[side], hr.at[side], (grp, ep + (1 if side == 0 else -1), tp),
        )

    def out_copy(part):
        span = part_span(part)
        return pltpu.make_async_copy(psend.at[tp, :, span], out.at[:, span], out_sem.at[part])

    def mixed_copy(block):
        span = part_span(block, rows)
        return pltpu.make_async_copy(mixed.at[span], mixed_out.at[span], mixed_sem.at[block])

    def normalize(source, gain, target):
        def squares(part, carry):
            values = source[:, part_span(part)].astype(f32)
            return carry + jnp.sum(values * values, axis=1, keepdims=True)

        summed = lax.fori_loop(0, parts, squares, jnp.zeros((rows, 1), f32))
        factor = lax.rsqrt(summed / width + EPS)

        def scale(part):
            span = part_span(part)
            target[:, span] = (source[:, span].astype(f32) * factor * gain[:, span]).astype(bf16)

        each_part(scale)

    def places_of(block, d):
        expert = lax.rem(ep + d, ep_count) * tp_count + tp
        slot_ids = lax.broadcasted_iota(jnp.int32, (slots, rows), 0).astype(f32)
        return slot_ids == metag[block, pl.ds(expert, 1), :], expert

    def pick_part(block, part):
        span = part_span(part)
        picks = [jnp.where(places_of(block, d)[0], 1.0, 0.0) for d in range(ep_count)]
        pick = jnp.concatenate(picks, axis=0).astype(bf16)
        picked = jnp.dot(pick, gath2[block, :, span], preferred_element_type=f32).astype(bf16)
        disp[block, 0:slots, span] = picked[0:slots]
        sbuf[block, slots:total, span] = picked[slots:total]
        for d in range(1, ep_count):
            dispatch_copy(block, d, span).start()

    def shared_hidden(block):
        values = gath2[block]
        gated = jnp.dot(values, sgate[...], preferred_element_type=f32)
        lifted = jnp.dot(values, sup[...], preferred_element_type=f32)
        hidden[block] = (jax.nn.silu(gated) * lifted).astype(bf16)

    def expert(block):
        dispatch_all(block).wait()

        def units(part):
            span = part_span(part, 256)
            values = disp[block]
            gated = jnp.dot(values, gate[:, span], preferred_element_type=f32)
            lifted = jnp.dot(values, up[:, span], preferred_element_type=f32)
            hexp[:, span] = (jax.nn.silu(gated) * lifted).astype(bf16)

        each_part(units, gate.shape[1] // 256)

        def columns(part):
            span = part_span(part)
            result = jnp.dot(hexp[...], down[:, span], preferred_element_type=f32).astype(bf16)
            back[block, 0:slots, span] = result[0:slots]
            sbuf[block, slots:total, span] = result[slots:total]

            @pl.when(block != tp)
            def _():
                for d in range(1, ep_count):
                    return_copy(block, d, part).start()

        each_part(columns)

    def experts_at(order):
        def one(side, carry):
            block, inside = at(side, order)

            @pl.when(inside & ((order > 0) | (side == 0)))
            def _():
                expert(block)

            return carry

        lax.fori_loop(0, 2, one, 0)

    def start_own_first(side, step):
        last = tp if side == 0 else tp_count - 1 - tp

        @pl.when(carries(side) & (step == last))
        def _():
            send_first(side, tp).start()

    def rotated(values, cos_rows, sin_rows):
        pieces = []
        half = HEAD_DIM // 2
        size = LANES if values.shape[1] % LANES == 0 else HEAD_DIM
        for start in range(0, values.shape[1], size):
            piece = values[:, start : start + size]
            if size == LANES:
                lane = lax.broadcasted_iota(jnp.int32, piece.shape, 1)
                crossed = jnp.where(
                    lax.rem(lane, HEAD_DIM) < half,
                    pltpu.roll(piece, LANES - half, 1),
                    pltpu.roll(piece, half, 1),
                )
            else:
                crossed = jnp.concatenate([piece[:, half:], piece[:, :half]], axis=1)
            pieces.append(piece * cos_rows[:, :size] + crossed * sin_rows[:, :size])
        return pieces[0] if len(pieces) == 1 else jnp.concatenate(pieces, axis=1)

    def projected(block, query_w, key_w, value_w):
        span = part_span(block, rows)
        values = gath1[block]
        cos_rows, sin_rows = cosine[span, :], sine[span, :]
        query = jnp.dot(values, query_w[...], preferred_element_type=f32)
        key = jnp.dot(values, key_w[...], preferred_element_type=f32)
        value = jnp.dot(values, value_w[...], preferred_element_type=f32)
        joined = jnp.concatenate([rotated(key, cos_rows, sin_rows), value], axis=1).astype(bf16)
        return rotated(query, cos_rows, sin_rows).astype(bf16), joined

    def project(block):
        qbuf[part_span(block, rows), :], kvbuf[part_span(block + 1, rows), :] = projected(block, wq, wk, wv)

    def project_far(block):
        lent_q[block], lent_kv[block] = projected(block, far_q, far_k, far_v)
        query_copy(block, toward(outward)).start()
        kv_copy(block, toward(outward)).start()

    def start_halo(block):
        @pl.when((block == tp_count - 1) & (ep < ep_count - 1))
        def _():
            halo(0).start()

        @pl.when((block == 0) & (ep > 0))
        def _():
            halo(1).start()

    def tables():
        def one(block):
            start = pl.multiple_of(block * rows, rows)
            shape = (rows, LANES)
            place = ep * (tp_count * rows) + start + lax.broadcasted_iota(jnp.int32, shape, 0)
            angle = place.astype(f32) * inverse[...]
            lane = lax.broadcasted_iota(jnp.int32, shape, 1)
            turn = jnp.sin(angle)
            cosine[pl.ds(start, rows), :] = jnp.cos(angle)
            sine[pl.ds(start, rows), :] = jnp.where(lax.rem(lane, HEAD_DIM) < HEAD_DIM // 2, -turn, turn)

        each_part(one, tp_count)

    kv_heads = wk.shape[1] // HEAD_DIM
    group = wq.shape[1] // wk.shape[1]

    def attend(block):
        base = pl.multiple_of(block * rows, rows)
        window = kvbuf[pl.ds(base, 3 * rows), :]
        query = qbuf[pl.ds(base, rows), :]
        shape = (rows, 3 * rows)
        row = lax.broadcasted_iota(jnp.int32, shape, 0)
        col = lax.broadcasted_iota(jnp.int32, shape, 1)
        gap = col - row - rows
        low = jnp.where((ep == 0) & (block == 0), rows, 0)
        high = jnp.where((ep == ep_count - 1) & (block == tp_count - 1), 2 * rows, 3 * rows)
        near = (gap <= WINDOW) & (gap >= -WINDOW) & (col >= low) & (col < high)
        pieces = []
        for g in range(kv_heads):
            keys = window[:, g * HEAD_DIM : (g + 1) * HEAD_DIM]
            start = (kv_heads + g) * HEAD_DIM
            values = window[:, start : start + HEAD_DIM]
            for h in range(g * group, (g + 1) * group):
                scores = lax.dot_general(
                    query[:, h * HEAD_DIM : (h + 1) * HEAD_DIM], keys, (((1,), (1,)), ((), ())),
                    preferred_element_type=f32,
                ) * HEAD_DIM ** (-0.5)
                scores = jnp.where(near, scores, -jnp.inf)
                bound = sink[0, h]
                top = jnp.maximum(jnp.max(scores, axis=1, keepdims=True), bound)
                weights = jnp.exp(scores - top)
                summed = jnp.sum(weights, axis=1, keepdims=True) + jnp.exp(bound - top)
                share = (weights * (1.0 / summed)).astype(bf16)
                pieces.append(jnp.dot(share, values, preferred_element_type=f32))
        mixed[pl.ds(base, rows), :] = jnp.concatenate(pieces, axis=1).astype(bf16)
        mixed_copy(block).start()

    normalize(second_in, gain_second, gath2.at[tp])
    ids = lax.broadcasted_iota(jnp.int32, (experts, rows), 0)
    hit = ids == routes[0:1, :]
    for j in range(1, routes.shape[0]):
        hit = hit | (ids == routes[j : j + 1, :])
    earlier = (
        lax.broadcasted_iota(jnp.int32, (rows, rows), 0) < lax.broadcasted_iota(jnp.int32, (rows, rows), 1)
    )
    before = jnp.dot(
        jnp.where(hit, 1.0, 0.0).astype(bf16), jnp.where(earlier, 1.0, 0.0).astype(bf16),
        preferred_element_type=f32,
    )
    metag[tp, 0:experts, :] = jnp.where(hit, before, -1.0)
    pl.semaphore_wait(barrier, ep_count + grp_count - 1 + jnp.where((tp > 0) & (tp < tp_count - 1), 1, 0))

    def send_own(part):
        for side in range(2):

            @pl.when(exists(side) & jnp.logical_not(late(side)))
            def _():
                send_second(side, tp, part).start()

    send_own(0)
    affinity = lax.dot_general(
        router[...], gath2[tp], (((1,), (1,)), ((), ())), preferred_element_type=f32
    )
    chosen = jnp.where(hit, jax.nn.sigmoid(affinity), 0.0)
    metag[tp, experts : 2 * experts, :] = ROUTED_SCALE * chosen / jnp.sum(chosen, axis=0, keepdims=True)
    pick_part(tp, 0)
    for side in range(2):

        @pl.when(exists(side))
        def _():
            send_meta(side, tp).start()

    for part in range(1, parts):
        send_own(part)

    def pick_rest(part, carry):
        pick_part(tp, part)
        return carry

    lax.fori_loop(1, parts, pick_rest, 0)
    local[0].wait()
    normalize(first_in, gain_first, gath1.at[tp])

    @pl.when(tp == 0)
    def _():
        sides[0] = jnp.zeros(sides.shape[1:], sides.dtype)

    @pl.when(tp == tp_count - 1)
    def _():
        sides[1] = jnp.zeros(sides.shape[1:], sides.dtype)

    @pl.when(ep == 0)
    def _():
        kvbuf[0:rows, :] = jnp.zeros((rows, kvbuf.shape[1]), bf16)

    @pl.when(ep == ep_count - 1)
    def _():
        kvbuf[(tp_count + 1) * rows : (tp_count + 2) * rows, :] = jnp.zeros((rows, kvbuf.shape[1]), bf16)

    for copy in local[1:]:
        copy.wait()
    if assist:

        @pl.when(ends)
        def _():
            for copy in lend_out():
                copy.start()

    for side in range(2):
        start_own_first(side, 0)
    shared_hidden(tp)

    def weights_of(block):
        pieces = []
        for d in range(ep_count):
            hit_rows, number = places_of(block, d)
            pieces.append(jnp.where(hit_rows, metag[block, pl.ds(experts + number, 1), :], 0.0))
        weights = jnp.concatenate(pieces, axis=0)
        top = weights.astype(bf16)
        return top, (weights - top.astype(f32)).astype(bf16)

    def value_of(block, weights, span):
        turned = (((0,), (0,)), ((), ()))
        picked = back[block, :, span]
        return (
            lax.dot_general(weights[0], picked, turned, preferred_element_type=f32)
            + lax.dot_general(weights[1], picked, turned, preferred_element_type=f32)
            + jnp.dot(hidden[block], sdown[:, span], preferred_element_type=f32)
        )

    def reduce_piece(side, block, part, weights):
        span = part_span(part)
        return_part(block, part).wait_recv()
        own = value_of(block, weights, span)

        @pl.when(exists(1 - side))
        def _():
            pass_on(side, block, part).wait_recv()

        psend[block, :, span] = (own + sides[side, block, :, span].astype(f32)).astype(bf16)
        pass_on(side, block, part).start()

    def edge(last):
        @pl.when((last == 1) & (ep < ep_count - 1))
        def _():
            halo(1).wait_recv()

        @pl.when((last == 0) & (ep > 0))
        def _():
            halo(0).wait_recv()

        attend((tp_count - 1) * last)

    def reduce_merged():
        end = (tp_count - 1) * (1 - outward)
        second = 1 + (tp_count - 3) * outward

        def slot(i):
            def stream(j, carry):
                part = i - LAG * j
                side = jnp.where(j == 1, outward, 1 - outward)
                block = jnp.where(j == 0, tp_count - 1 - end, jnp.where(j == 1, end, second))

                @pl.when((part >= 0) & (part < parts))
                def _():
                    reduce_piece(side, block, part, weights_of(block))

                return carry

            lax.fori_loop(0, 3, stream, 0)

            @pl.when(i == 0)
            def _():
                attend(second)

            @pl.when((i == 3) | (i == 5))
            def _():
                edge(jnp.where(i == 3, 1, 0))

        each_part(slot, parts + 2 * LAG)

    def reduce_step(step):
        def one(turn, carry):
            side = jnp.where(2 * tp < tp_count, 1 - turn, turn)
            block = jnp.where(side == 0, step - tp, 2 * (tp_count - 1) - step - tp)
            active = (block >= 0) & (block < tp_count)
            if swaps:
                block = swapped(1 - side, block, True)
            active = active & ((block - tp) * (1 - 2 * side) > 0)

            @pl.when(active)
            def _():
                weights = weights_of(block)
                each_part(lambda part: reduce_piece(side, block, part, weights))

            return carry

        lax.fori_loop(0, 2, one, 0)

    early = tp_count > 2

    def hop(k, carry):
        def one_turn(turn):
            def receive(second, carry):
                part = turn - second * LAG
                side = jnp.where(2 * tp < tp_count, second, 1 - second)
                block, inside = at(side, k)

                @pl.when(inside & (part >= 0) & (part < parts))
                def _():
                    send_second(side, block, part).wait_recv()

                    @pl.when(exists(side))
                    def _():
                        send_second(side, block, part).start()

                    @pl.when(part == 0)
                    def _():
                        send_meta(side, block).wait_recv()

                        @pl.when(exists(side))
                        def _():
                            send_meta(side, block).start()

                    @pl.when(late(side) & (k == 1) & (part == parts - 1))
                    def _():
                        for own in range(parts):
                            send_second(side, tp, own).start()

                    pick_part(block, part)

                return carry

            lax.fori_loop(0, 2, receive, 0)

            @pl.when(k == 1)
            def _():
                @pl.when(turn == 1)
                def _():
                    tables()

                @pl.when(turn == 2)
                def _():
                    project(tp)
                    start_halo(tp)

            if early:

                @pl.when(ends & (k == tp_count - 1) & (turn == LAG + 1))
                def _():
                    reduce_step(1)

            if assist:

                @pl.when(helps & (k == 2) & (turn == LAG + 1))
                def _():
                    relay_first()

            middle = ends & (k > 1) & (k == tp_count - 1) & (turn == LAG)

            @pl.when(middle | ((k == 1) & (turn == LAG + 2)))
            def _():
                experts_at(k - 1)

        each_part(one_turn, parts + LAG)
        for side in range(2):
            start_own_first(side, k)
        for side in range(2):
            block, inside = at(side, k)

            @pl.when(inside)
            def _():
                shared_hidden(block)

        if slim:

            @pl.when(helps & (k == tp_count - 1))
            def _():
                side = 1 - outward
                block, _ = near(side, 1)
                send_first(side, block).wait_recv()
                send_first(side, block).start()
                project(block)
                start_halo(block)

        @pl.when((k > 1) & (jnp.logical_not(ends) | (k < tp_count - 1)))
        def _():
            experts_at(k - 1)

        return carry

    lax.fori_loop(1, tp_count, hop, 0)
    if early:
        reduce_step(2)

    experts_at(tp_count - 1)

    def give_back(low, high):
        for part in range(low, high):
            for d in range(1, ep_count):
                return_copy(tp, d, part).start()

    @pl.when(ends | (not slim))
    def _():
        give_back(0, parts // 2)

    if assist:

        @pl.when(helps)
        def _():
            relay_second()


    def first_hop(k, carry):
        def open_at(side):
            block, inside = near(side, k)
            if slim:
                inside = inside & ((k > 1) | (side == outward))
            return block, inside

        for side in range(2):
            block, inside = open_at(side)

            @pl.when(inside & plain)
            def _():
                send_first(side, block).wait_recv()

                @pl.when(carries(side))
                def _():
                    send_first(side, block).start()

        if assist:

            @pl.when(helps)
            def _():
                @pl.when(k == 1)
                def _():
                    relay_last()

                def one(turn, carry):
                    block, inside = near(outward, k * turn)

                    @pl.when(inside & ((turn == 1) | (k == 1)))
                    def _():
                        project_far(block)

                    return carry

                lax.fori_loop(0, 2, one, 0)

        def use(side, carry):
            block, inside = open_at(side)

            @pl.when(inside & plain)
            def _():
                project(block)
                start_halo(block)

            return carry

        lax.fori_loop(0, 2, use, 0)
        @pl.when((k == jnp.maximum(tp, tp_count - 1 - tp)) & plain)
        def _():
            give_back(0 if slim else parts // 2, parts)

        if slim:

            @pl.when((k == 2) & ends)
            def _():
                reduce_step(3)

            @pl.when((k == 2) & helps)
            def _():
                reduce_merged()

        elif early:

            @pl.when(k > 1)
            def _():
                reduce_step(2 * k - 1)
                reduce_step(2 * k)

        else:
            reduce_step(2 * k - 1)

        def settle(side, carry):
            block, _ = near(side, k - 1)

            inner = (block > 0) & (block < tp_count - 1) & ((k > 1) | (side == 0))
            if slim:
                inner = inner & (k == 1)

            @pl.when(inner & plain)
            def _():
                attend(block)

            return carry

        lax.fori_loop(0, 2, settle, 0)
        return carry

    lax.fori_loop(1, tp_count, first_hop, 0)
    if assist:

        @pl.when(ends)
        def _():
            def arrive(block):
                @pl.when(block != tp)
                def _():
                    query_copy(block, toward(jnp.where(tp == 0, 0, 1))).wait_recv()
                    kv_copy(block, toward(jnp.where(tp == 0, 0, 1))).wait_recv()
                    start_halo(block)

            each_part(arrive, tp_count)
            give_back(parts // 2, parts)
            each_part(lambda block: attend(block + 1), tp_count - 2)

    @pl.when(jnp.logical_not(helps) | (not slim))
    def _():
        each_part(lambda turn: edge(1 - turn), 2)

    own_weights = weights_of(tp)

    def last_part(part):
        span = part_span(part)
        return_part(tp, part).wait_recv()
        own = value_of(tp, own_weights, span)

        @pl.when(tp > 0)
        def _():
            pass_on(0, tp, part).wait_recv()

        @pl.when(tp < tp_count - 1)
        def _():
            pass_on(1, tp, part).wait_recv()

        psend[tp, :, span] = (
            own + sides[0, tp, :, span].astype(f32) + sides[1, tp, :, span].astype(f32)
        ).astype(bf16)
        out_copy(part).start()

    each_part(last_part)

    def finish(block):
        return_all(block).wait_send()
        for side in range(2):
            passed = block <= tp if side == 0 else block >= tp
            summed = block > tp if side == 0 else block < tp

            @pl.when(exists(side) & passed)
            def _():
                ref = gath2.at[block]
                remote(ref, ref, s2.at[side, block], r2.at[block, 0], toward(side)).wait_send()
                send_meta(side, block).wait_send()

            @pl.when(carries(side) & passed)
            def _():
                send_first(side, block).wait_send()

            @pl.when(summed)
            def _():
                for part in range(parts):
                    pass_on(side, block, part).wait_send()

    each_part(finish, tp_count)
    if assist:

        @pl.when(ends)
        def _():
            for copy in lend_out():
                copy.wait_send()

        @pl.when(helps)
        def _():
            for copies in relays() + (relays_across() if pair == 2 else []):
                for copy in copies:
                    copy.wait_send()

            def sent(block):
                @pl.when(block != tp + 1 - 2 * outward)
                def _():
                    query_copy(block, toward(outward)).wait_send()
                    kv_copy(block, toward(outward)).wait_send()

            each_part(sent, tp_count)

    each_part(lambda part: out_copy(part).wait())
    each_part(lambda block: mixed_copy(block).wait(), tp_count)

    @pl.when(ep < ep_count - 1)
    def _():
        halo(0).wait_send()

    @pl.when(ep > 0)
    def _():
        halo(1).wait_send()


def layer(
    second, first, gain_second, gain_first, router, routes, inverse, sink,
    gate, up, down, sgate, sup, sdown, wq, wk, wv, grp_count, ep_count, tp_count, slots,
):
    rows, width = second.shape
    experts = router.shape[0]
    vmem = pl.BlockSpec(memory_space=pltpu.VMEM)
    smem = pl.BlockSpec(memory_space=pltpu.SMEM)
    hbm = pl.BlockSpec(memory_space=pl.ANY)
    dma = pltpu.SemaphoreType.DMA
    bf16, f32 = jnp.bfloat16, jnp.float32
    total = ep_count * slots
    parts = width // CHUNK
    span = tp_count * rows
    kv_cols = wk.shape[1] + wv.shape[1]
    return pl.pallas_call(
        functools.partial(layer_kernel, grp_count, ep_count, tp_count, slots),
        out_shape=(
            jax.ShapeDtypeStruct((rows, width), bf16),
            jax.ShapeDtypeStruct((span, wq.shape[1]), bf16),
        ),
        in_specs=[vmem] * 6 + [smem] + [hbm] * 10,
        out_specs=(hbm, hbm),
        scratch_shapes=[
            pltpu.VMEM((span, wq.shape[1]), bf16),
            pltpu.VMEM((tp_count, rows, width), bf16),
            pltpu.VMEM((tp_count, rows, width), bf16),
            pltpu.VMEM((rows, width), bf16),
            pltpu.VMEM((tp_count, 2 * experts, rows), f32),
            pltpu.VMEM((tp_count, total, width), bf16),
            pltpu.VMEM((tp_count, total, width), bf16),
            pltpu.VMEM((tp_count, total, width), bf16),
            pltpu.VMEM((2, tp_count, rows, width), bf16),
            pltpu.VMEM((tp_count, rows, width), bf16),
            pltpu.VMEM(gate.shape[1:], bf16),
            pltpu.VMEM(up.shape[1:], bf16),
            pltpu.VMEM(down.shape[1:], bf16),
            pltpu.VMEM(sgate.shape, bf16),
            pltpu.VMEM(sup.shape, bf16),
            pltpu.VMEM(sdown.shape, bf16),
            pltpu.VMEM(wq.shape, bf16),
            pltpu.VMEM(wk.shape, bf16),
            pltpu.VMEM(wv.shape, bf16),
            pltpu.VMEM(wq.shape, bf16),
            pltpu.VMEM(wk.shape, bf16),
            pltpu.VMEM(wv.shape, bf16),
            pltpu.VMEM((tp_count, rows, wq.shape[1]), bf16),
            pltpu.VMEM((tp_count, rows, kv_cols), bf16),
            pltpu.VMEM((tp_count, rows, sgate.shape[1]), bf16),
            pltpu.VMEM((total, gate.shape[2]), bf16),
            pltpu.VMEM((span, LANES), f32),
            pltpu.VMEM((span, LANES), f32),
            pltpu.VMEM((span, wq.shape[1]), bf16),
            pltpu.VMEM((span + 2 * rows, kv_cols), bf16),
            dma((10,)),
            dma((2, tp_count)),
            dma((tp_count, parts)),
            dma((2, tp_count)),
            dma((tp_count,)),
            dma((2, tp_count)),
            dma((tp_count,)),
            dma((tp_count,)),
            dma((tp_count,)),
            dma((tp_count,)),
            dma((tp_count, parts)),
            dma((tp_count, parts)),
            dma((2, tp_count, parts)),
            dma((2,)),
            dma((2,)),
            dma((parts,)),
            dma((tp_count,)),
            dma((2 * grp_count, grp_count, 3)),
            dma((2 * grp_count, 3)),
            dma((2, tp_count)),
            dma((2, tp_count)),
        ],
        compiler_params=pltpu.CompilerParams(
            collective_id=0, has_side_effects=True, vmem_limit_bytes=VMEM_LIMIT
        ),
        name="layer",
    )(
        second, gain_second, gain_first, router, routes, inverse, sink,
        first, gate, up, down, sgate, sup, sdown, wq, wk, wv,
    )


def settle_kernel(first, second, first_out, second_out, first_buf, second_buf, sems):
    arrays = [(first, first_buf, first_out), (second, second_buf, second_out)]
    pieces = []
    for i, (source, buffer, target) in enumerate(arrays):
        half = source.shape[0] // 2
        for j in range(2):
            rows = pl.ds(j * half, half)
            pieces.append(
                (
                    pltpu.make_async_copy(source.at[rows], buffer.at[rows], sems.at[0, i, j]),
                    pltpu.make_async_copy(buffer.at[rows], target.at[rows], sems.at[1, i, j]),
                )
            )
    for load, _ in pieces:
        load.start()
    for load, store in pieces:
        load.wait()
        store.start()
    for _, store in pieces:
        store.wait()


def settle(first, second):
    hbm = pl.BlockSpec(memory_space=pl.ANY)
    return pl.pallas_call(
        settle_kernel,
        out_shape=(jax.ShapeDtypeStruct(first.shape, first.dtype), jax.ShapeDtypeStruct(second.shape, second.dtype)),
        in_specs=[hbm, hbm],
        out_specs=(hbm, hbm),
        scratch_shapes=[
            pltpu.VMEM(first.shape, first.dtype),
            pltpu.VMEM(second.shape, second.dtype),
            pltpu.SemaphoreType.DMA((2, 2, 2)),
        ],
        compiler_params=pltpu.CompilerParams(vmem_limit_bytes=VMEM_LIMIT),
        name="settle",
    )(first, second)


def body(
    mixer_in,
    mixer_gain,
    w_query,
    w_key,
    w_value,
    sink_logit,
    moe_in,
    moe_gain,
    router,
    routes,
    expert_gate,
    expert_up,
    expert_down,
    shared_gate,
    shared_up,
    shared_down,
):
    tokens = mixer_in.shape[0]
    ep_count, tp_count = lax.axis_size("ep"), lax.axis_size("tp")
    top_count = routes.shape[1]
    experts = router.shape[1]
    capacity = 3 * top_count * tokens // (2 * experts)
    slots = -(-capacity // 16) * 16
    half = HEAD_DIM // 2
    inverse = np.float32(THETA) ** (-(np.arange(half, dtype=np.float32) * np.float32(2.0)) / np.float32(HEAD_DIM))
    moe_out, mixed = layer(
        moe_in, mixer_in, moe_gain[None, :], mixer_gain[None, :], router.T, routes.T,
        jnp.asarray(np.tile(inverse, LANES // half)[None, :]), sink_logit[None, :],
        expert_gate, expert_up, expert_down, shared_gate, shared_up, shared_down,
        w_query, w_key, w_value, lax.axis_size("grp"), ep_count, tp_count, slots,
    )
    moe_out, mixed = settle(moe_out, mixed)
    return (mixed, moe_out)


def solution(mesh):
    return jax.shard_map(
        body,
        mesh=mesh,
        in_specs=(
            P(("grp", "ep", "tp"), None),
            P(),
            P(None, "tp"),
            P(None, "tp"),
            P(None, "tp"),
            P("tp"),
            P(("grp", "ep", "tp"), None),
            P(),
            P(),
            P(("grp", "ep", "tp"), None),
            P(("ep", "tp"), None, None),
            P(("ep", "tp"), None, None),
            P(("ep", "tp"), None, None),
            P(None, "tp"),
            P(None, "tp"),
            P("tp", None),
        ),
        out_specs=(P(("grp", "ep"), "tp"), P(("grp", "ep", "tp"), None)),
        check_vma=False,
    )
```

```python
import functools

import jax
import jax.numpy as jnp
import numpy as np
from jax import lax
from jax.experimental import pallas as pl
from jax.experimental.pallas import tpu as pltpu
from jax.sharding import PartitionSpec as P

HEAD_DIM = 64
WINDOW = 128
EPS = 1e-06
THETA = 10000.0
ROUTED_SCALE = 2.5
LANES = 128
CHUNK = 512
PASS = 256
LAG = 2
AHEAD = 1
MESH = pl.DeviceIdType.MESH
VMEM_LIMIT = 63 * 2**20


def remote(src, dst, send_sem, recv_sem, device):
    return pltpu.make_async_remote_copy(
        src_ref=src,
        dst_ref=dst,
        send_sem=send_sem,
        recv_sem=recv_sem,
        device_id=device,
        device_id_type=MESH,
    )


def greet(grp, ep, tp, grp_count, ep_count, tp_count):
    barrier = pltpu.get_barrier_semaphore()

    @pl.when(tp > 0)
    def _():
        pl.semaphore_signal(barrier, inc=1, device_id=(grp, ep, tp - 1), device_id_type=MESH)

    @pl.when(tp < tp_count - 1)
    def _():
        pl.semaphore_signal(barrier, inc=1, device_id=(grp, ep, tp + 1), device_id_type=MESH)

    for d in range(1, ep_count):
        pl.semaphore_signal(
            barrier, inc=1, device_id=(grp, lax.rem(ep + d, ep_count), tp), device_id_type=MESH
        )
    for d in range(1, grp_count):
        pl.semaphore_signal(
            barrier, inc=1, device_id=(lax.rem(grp + d, grp_count), ep, tp), device_id_type=MESH
        )
    return barrier


def layer_kernel(
    grp_count, ep_count, tp_count, slots,
    second_hbm, gain_second_hbm, router_hbm, routes_hbm, gain_first_hbm, inverse_hbm, sink_hbm,
    first_hbm, gate_hbm, up_hbm, down_hbm, sgate_hbm, sup_hbm, sdown_hbm, wq_hbm, wk_hbm, wv_hbm,
    out, mixed_out,
    mixed, second_in, gain_second, router, routes, gain_first, inverse, sink,
    gath2, gath1, first_in, metag, sbuf, disp, back, sides, psend,
    gate, up, down, sgate, sup, sdown, wq, wk, wv, far_q, far_k, far_v, lent_q, lent_kv,
    hidden, hexp, cosine, sine, qbuf, kvbuf,
    l_sem, s2, r2, sm, rm, s1, r1, sd, rd, sb, rb, sp, rs, hs, hr, out_sem, mixed_sem, ws, wr, qs, qr,
):
    grp, ep, tp = lax.axis_index("grp"), lax.axis_index("ep"), lax.axis_index("tp")
    rows, width = second_in.shape
    experts = metag.shape[1] // 2
    total = ep_count * slots
    parts = width // CHUNK
    f32, bf16 = jnp.float32, jnp.bfloat16
    away = pl.ds(slots, total - slots)

    barrier = greet(grp, ep, tp, grp_count, ep_count, tp_count)
    early_pairs = [
        (second_hbm, second_in),
        (gain_second_hbm, gain_second),
        (routes_hbm, routes),
        (router_hbm, router),
    ]
    pairs = early_pairs + [
        (gain_first_hbm, gain_first),
        (first_hbm, first_in),
        (sgate_hbm, sgate),
        (sup_hbm, sup),
        (wq_hbm, wq),
        (wk_hbm, wk),
        (wv_hbm, wv),
        (inverse_hbm, inverse),
        (sink_hbm, sink),
        (gate_hbm.at[0], gate),
        (up_hbm.at[0], up),
        (down_hbm.at[0], down),
        (sdown_hbm, sdown),
    ]
    local = [pltpu.make_async_copy(src, dst, l_sem.at[i]) for i, (src, dst) in enumerate(pairs)]
    for copy in local:
        copy.start()

    def toward(side):
        return (grp, ep, tp + 1 - 2 * side)

    def exists(side):
        return (tp + 1 - 2 * side >= 0) & (tp + 1 - 2 * side < tp_count)

    def peer(d):
        return (grp, lax.rem(ep + d, ep_count), tp)

    def part_span(part, size=CHUNK):
        return pl.ds(pl.multiple_of(part * size, size), size)

    def each_part(body, count=parts):
        def step(part, carry):
            body(part)
            return carry

        lax.fori_loop(0, count, step, 0)

    def near(side, distance):
        block = tp + (2 * side - 1) * distance
        return block, (block >= 0) & (block < tp_count)

    swaps = tp_count > 2

    def swapped(side, block, allowed):
        far, second = (tp_count - 1) * side, 1 + (tp_count - 3) * side
        other = jnp.where(block == second, far, jnp.where(block == far, second, block))
        return jnp.where(allowed, other, block)

    def at(side, order):
        block, inside = near(side, order)
        if swaps:
            block = swapped(side, block, jnp.where(side == 0, tp, tp_count - 1 - tp) >= 2)
        return block, inside

    def late(side):
        return (tp == 1 + side * (tp_count - 3)) & swaps

    def send_second(side, block, part):
        ref = gath2.at[block, :, part_span(part)]
        return remote(ref, ref, s2.at[side, block], r2.at[block, part], toward(side))

    def send_meta(side, block):
        return remote(metag.at[block], metag.at[block], sm.at[side, block], rm.at[block], toward(side))

    assist = tp_count >= 4
    ends = (tp == 0) | (tp == tp_count - 1)
    slim = tp_count == 4
    plain = jnp.logical_not(ends) | (not assist)
    helps = ((tp == 1) | (tp == tp_count - 2)) & assist
    outward = jnp.where(tp == 1, 1, 0)
    pair = 2 if ep_count % 2 == 0 else 1
    core = lax.rem(ep, pair)
    piece_rows = width // (grp_count * pair)
    lent = [(wq, far_q), (wk, far_k), (wv, far_v)]

    def carries(side):
        target = tp + 1 - 2 * side
        return exists(side) & (((target > 0) & (target < tp_count - 1)) | (not assist))

    def share_of(group, half):
        return group * pair + half

    def lend(share, to, device, own):
        span = pl.ds(pl.multiple_of(share * piece_rows, piece_rows), piece_rows)
        return [
            remote(
                (near_ref if own else far_ref).at[span], far_ref.at[span],
                ws.at[share, to, i], wr.at[share, i], device,
            )
            for i, (near_ref, far_ref) in enumerate(lent)
        ]

    def lend_out():
        return lend(share_of(grp, core), 0, (grp, ep, jnp.where(tp == 0, 1, tp_count - 2)), True)

    def partner():
        return (grp, ep + 1 - 2 * core, tp)

    def relays():
        mine = share_of(grp, core)
        copies = []
        for d in range(1, grp_count):
            copies.append(lend(mine, d, (lax.rem(grp + d, grp_count), ep, tp), False))
        if pair == 2:
            copies.append(lend(mine, 0, partner(), False))
        return copies

    def relays_across():
        copies = []
        for d in range(1, grp_count):
            copies.append(lend(share_of(lax.rem(grp + d, grp_count), core), 0, partner(), False))
        return copies

    def relay_first():
        for copy in lend(share_of(grp, core), 0, toward(outward), False):
            copy.wait_recv()
        for copies in relays():
            for copy in copies:
                copy.start()

    def relay_second():
        for copies in relays_across():
            for copy in copies:
                copy.wait_recv()
            if pair == 2:
                for copy in copies:
                    copy.start()

    def relay_last():
        if pair == 2:
            for group in range(grp_count):
                for copy in lend(share_of(group, 1 - core), 0, partner(), False):
                    copy.wait_recv()

    def query_copy(block, device):
        return remote(
            lent_q.at[block], qbuf.at[part_span(block, rows)], qs.at[0, block], qr.at[0, block], device
        )

    def kv_copy(block, device):
        return remote(
            lent_kv.at[block], kvbuf.at[part_span(block + 1, rows)], qs.at[1, block], qr.at[1, block], device
        )

    def send_first(side, block):
        return remote(gath1.at[block], gath1.at[block], s1.at[side, block], r1.at[block], toward(side))

    def dispatch_copy(block, d, span):
        mine = pl.ds(d * slots, slots)
        return remote(sbuf.at[block, mine, span], disp.at[block, mine, span], sd.at[block], rd.at[block], peer(d))

    def dispatch_all(block):
        return remote(sbuf.at[block, away], disp.at[block, away], sd.at[block], rd.at[block], peer(1))

    def return_copy(block, d, part):
        mine, span = pl.ds(d * slots, slots), part_span(part)
        return remote(
            sbuf.at[block, mine, span], back.at[block, mine, span],
            sb.at[block], rb.at[block, part], peer(ep_count - d),
        )

    def return_part(block, part):
        span = part_span(part)
        return remote(
            sbuf.at[block, away, span], back.at[block, away, span], sb.at[block], rb.at[block, part], peer(1)
        )

    def return_all(block):
        return remote(sbuf.at[block, away], back.at[block, away], sb.at[block], rb.at[block, 0], peer(1))

    def pass_on(side, block, part):
        span = part_span(part, PASS)
        return remote(
            psend.at[block, :, span], sides.at[side, block, :, span],
            sp.at[block, part], rs.at[side, block, part], toward(side),
        )

    def halo(side):
        source = tp_count * rows if side == 0 else rows
        target = 0 if side == 0 else (tp_count + 1) * rows
        return remote(
            kvbuf.at[pl.ds(source, rows)], kvbuf.at[pl.ds(target, rows)],
            hs.at[side], hr.at[side], (grp, ep + (1 if side == 0 else -1), tp),
        )

    def out_copy(part):
        span = part_span(part)
        return pltpu.make_async_copy(psend.at[tp, :, span], out.at[:, span], out_sem.at[part])

    def mixed_copy(block):
        span = part_span(block, rows)
        return pltpu.make_async_copy(mixed.at[span], mixed_out.at[span], mixed_sem.at[block])

    def normalize(source, gain, target):
        def squares(part, carry):
            values = source[:, part_span(part)].astype(f32)
            return carry + jnp.sum(values * values, axis=1, keepdims=True)

        summed = lax.fori_loop(0, parts, squares, jnp.zeros((rows, 1), f32))
        factor = lax.rsqrt(summed / width + EPS)

        def scale(part):
            span = part_span(part)
            target[:, span] = (source[:, span].astype(f32) * factor * gain[:, span]).astype(bf16)

        each_part(scale)

    def places_of(block, d):
        expert = lax.rem(ep + d, ep_count) * tp_count + tp
        slot_ids = lax.broadcasted_iota(jnp.int32, (slots, rows), 0).astype(f32)
        return slot_ids == metag[block, pl.ds(expert, 1), :], expert

    def pick_part(block, part):
        span = part_span(part)
        picks = [jnp.where(places_of(block, d)[0], 1.0, 0.0) for d in range(ep_count)]
        pick = jnp.concatenate(picks, axis=0).astype(bf16)
        picked = jnp.dot(pick, gath2[block, :, span], preferred_element_type=f32).astype(bf16)
        disp[block, 0:slots, span] = picked[0:slots]
        sbuf[block, slots:total, span] = picked[slots:total]
        for d in range(1, ep_count):
            dispatch_copy(block, d, span).start()

    def shared_hidden(block):
        values = gath2[block]
        gated = jnp.dot(values, sgate[...], preferred_element_type=f32)
        lifted = jnp.dot(values, sup[...], preferred_element_type=f32)
        hidden[block] = (jax.nn.silu(gated) * lifted).astype(bf16)

    def expert(block):
        dispatch_all(block).wait()

        def units(part):
            span = part_span(part, 256)
            values = disp[block]
            gated = jnp.dot(values, gate[:, span], preferred_element_type=f32)
            lifted = jnp.dot(values, up[:, span], preferred_element_type=f32)
            hexp[:, span] = (jax.nn.silu(gated) * lifted).astype(bf16)

        each_part(units, gate.shape[1] // 256)

        def columns(part):
            span = part_span(part)
            result = jnp.dot(hexp[...], down[:, span], preferred_element_type=f32).astype(bf16)
            back[block, 0:slots, span] = result[0:slots]
            sbuf[block, slots:total, span] = result[slots:total]

            @pl.when(block != tp)
            def _():
                for d in range(1, ep_count):
                    return_copy(block, d, part).start()

        each_part(columns)

    def experts_at(order):
        def one(side, carry):
            block, inside = at(side, order)

            @pl.when(inside & ((order > 0) | (side == 0)))
            def _():
                expert(block)

            return carry

        lax.fori_loop(0, 2, one, 0)

    def start_own_first(side, step):
        last = tp if side == 0 else tp_count - 1 - tp

        @pl.when(carries(side) & (step == last))
        def _():
            send_first(side, tp).start()

    def rotated(values, cos_rows, sin_rows):
        pieces = []
        half = HEAD_DIM // 2
        size = LANES if values.shape[1] % LANES == 0 else HEAD_DIM
        for start in range(0, values.shape[1], size):
            piece = values[:, start : start + size]
            if size == LANES:
                lane = lax.broadcasted_iota(jnp.int32, piece.shape, 1)
                crossed = jnp.where(
                    lax.rem(lane, HEAD_DIM) < half,
                    pltpu.roll(piece, LANES - half, 1),
                    pltpu.roll(piece, half, 1),
                )
            else:
                crossed = jnp.concatenate([piece[:, half:], piece[:, :half]], axis=1)
            pieces.append(piece * cos_rows[:, :size] + crossed * sin_rows[:, :size])
        return pieces[0] if len(pieces) == 1 else jnp.concatenate(pieces, axis=1)

    def projected(block, query_w, key_w, value_w):
        span = part_span(block, rows)
        values = gath1[block]
        cos_rows, sin_rows = cosine[span, :], sine[span, :]
        query = jnp.dot(values, query_w[...], preferred_element_type=f32)
        key = jnp.dot(values, key_w[...], preferred_element_type=f32)
        value = jnp.dot(values, value_w[...], preferred_element_type=f32)
        joined = jnp.concatenate([rotated(key, cos_rows, sin_rows), value], axis=1).astype(bf16)
        return rotated(query, cos_rows, sin_rows).astype(bf16), joined

    def project(block):
        qbuf[part_span(block, rows), :], kvbuf[part_span(block + 1, rows), :] = projected(block, wq, wk, wv)

    def project_far(block):
        lent_q[block], lent_kv[block] = projected(block, far_q, far_k, far_v)
        query_copy(block, toward(outward)).start()
        kv_copy(block, toward(outward)).start()

    def start_halo(block):
        @pl.when((block == tp_count - 1) & (ep < ep_count - 1))
        def _():
            halo(0).start()

        @pl.when((block == 0) & (ep > 0))
        def _():
            halo(1).start()

    def tables():
        def one(block):
            start = pl.multiple_of(block * rows, rows)
            shape = (rows, LANES)
            place = ep * (tp_count * rows) + start + lax.broadcasted_iota(jnp.int32, shape, 0)
            angle = place.astype(f32) * inverse[...]
            lane = lax.broadcasted_iota(jnp.int32, shape, 1)
            turn = jnp.sin(angle)
            cosine[pl.ds(start, rows), :] = jnp.cos(angle)
            sine[pl.ds(start, rows), :] = jnp.where(lax.rem(lane, HEAD_DIM) < HEAD_DIM // 2, -turn, turn)

        each_part(one, tp_count)

    kv_heads = wk.shape[1] // HEAD_DIM
    group = wq.shape[1] // wk.shape[1]

    def attend(block):
        base = pl.multiple_of(block * rows, rows)
        window = kvbuf[pl.ds(base, 3 * rows), :]
        query = qbuf[pl.ds(base, rows), :]
        shape = (rows, 3 * rows)
        row = lax.broadcasted_iota(jnp.int32, shape, 0)
        col = lax.broadcasted_iota(jnp.int32, shape, 1)
        gap = col - row - rows
        low = jnp.where((ep == 0) & (block == 0), rows, 0)
        high = jnp.where((ep == ep_count - 1) & (block == tp_count - 1), 2 * rows, 3 * rows)
        near = (gap <= WINDOW) & (gap >= -WINDOW) & (col >= low) & (col < high)
        pieces = []
        for g in range(kv_heads):
            keys = window[:, g * HEAD_DIM : (g + 1) * HEAD_DIM]
            start = (kv_heads + g) * HEAD_DIM
            values = window[:, start : start + HEAD_DIM]
            for h in range(g * group, (g + 1) * group):
                scores = lax.dot_general(
                    query[:, h * HEAD_DIM : (h + 1) * HEAD_DIM], keys, (((1,), (1,)), ((), ())),
                    preferred_element_type=f32,
                ) * HEAD_DIM ** (-0.5)
                scores = jnp.where(near, scores, -jnp.inf)
                bound = sink[0, h]
                top = jnp.maximum(jnp.max(scores, axis=1, keepdims=True), bound)
                weights = jnp.exp(scores - top)
                summed = jnp.sum(weights, axis=1, keepdims=True) + jnp.exp(bound - top)
                share = (weights * (1.0 / summed)).astype(bf16)
                pieces.append(jnp.dot(share, values, preferred_element_type=f32))
        mixed[pl.ds(base, rows), :] = jnp.concatenate(pieces, axis=1).astype(bf16)
        mixed_copy(block).start()

    for copy in local[: len(early_pairs)]:
        copy.wait()
    normalize(second_in, gain_second, gath2.at[tp])
    ids = lax.broadcasted_iota(jnp.int32, (experts, rows), 0)
    hit = ids == routes[0:1, :]
    for j in range(1, routes.shape[0]):
        hit = hit | (ids == routes[j : j + 1, :])
    earlier = (
        lax.broadcasted_iota(jnp.int32, (rows, rows), 0) < lax.broadcasted_iota(jnp.int32, (rows, rows), 1)
    )
    before = jnp.dot(
        jnp.where(hit, 1.0, 0.0).astype(bf16), jnp.where(earlier, 1.0, 0.0).astype(bf16),
        preferred_element_type=f32,
    )
    metag[tp, 0:experts, :] = jnp.where(hit, before, -1.0)
    pl.semaphore_wait(barrier, ep_count + grp_count - 1 + jnp.where((tp > 0) & (tp < tp_count - 1), 1, 0))

    def send_own(part):
        for side in range(2):

            @pl.when(exists(side) & (jnp.logical_not(late(side)) | (part < AHEAD)))
            def _():
                send_second(side, tp, part).start()

    send_own(0)
    affinity = lax.dot_general(
        router[...], gath2[tp], (((1,), (1,)), ((), ())), preferred_element_type=f32
    )
    chosen = jnp.where(hit, jax.nn.sigmoid(affinity), 0.0)
    metag[tp, experts : 2 * experts, :] = ROUTED_SCALE * chosen / jnp.sum(chosen, axis=0, keepdims=True)
    pick_part(tp, 0)
    for side in range(2):

        @pl.when(exists(side))
        def _():
            send_meta(side, tp).start()

    for part in range(1, parts):
        send_own(part)

    def pick_rest(part, carry):
        pick_part(tp, part)
        return carry

    lax.fori_loop(1, parts, pick_rest, 0)
    for copy in local[len(early_pairs) : len(early_pairs) + 2]:
        copy.wait()
    normalize(first_in, gain_first, gath1.at[tp])

    @pl.when(tp == 0)
    def _():
        sides[0] = jnp.zeros(sides.shape[1:], sides.dtype)

    @pl.when(tp == tp_count - 1)
    def _():
        sides[1] = jnp.zeros(sides.shape[1:], sides.dtype)

    @pl.when(ep == 0)
    def _():
        kvbuf[0:rows, :] = jnp.zeros((rows, kvbuf.shape[1]), bf16)

    @pl.when(ep == ep_count - 1)
    def _():
        kvbuf[(tp_count + 1) * rows : (tp_count + 2) * rows, :] = jnp.zeros((rows, kvbuf.shape[1]), bf16)

    for copy in local[len(early_pairs) + 2 :]:
        copy.wait()
    if assist:

        @pl.when(ends)
        def _():
            for copy in lend_out():
                copy.start()

    for side in range(2):
        start_own_first(side, 0)
    shared_hidden(tp)

    def weights_of(block):
        pieces = []
        for d in range(ep_count):
            hit_rows, number = places_of(block, d)
            pieces.append(jnp.where(hit_rows, metag[block, pl.ds(experts + number, 1), :], 0.0))
        weights = jnp.concatenate(pieces, axis=0)
        top = weights.astype(bf16)
        return top, (weights - top.astype(f32)).astype(bf16)

    def value_of(block, weights, span):
        turned = (((0,), (0,)), ((), ()))
        picked = back[block, :, span]
        return (
            lax.dot_general(weights[0], picked, turned, preferred_element_type=f32)
            + lax.dot_general(weights[1], picked, turned, preferred_element_type=f32)
            + jnp.dot(hidden[block], sdown[:, span], preferred_element_type=f32)
        )

    def reduce_piece(side, block, part, weights):
        span = part_span(part)
        return_part(block, part).wait_recv()
        own = value_of(block, weights, span)

        for i in range(CHUNK // PASS):
            number = part * (CHUNK // PASS) + i
            piece = part_span(number, PASS)

            @pl.when(exists(1 - side))
            def _():
                pass_on(side, block, number).wait_recv()

            part_sum = own[:, i * PASS : (i + 1) * PASS] + sides[side, block, :, piece].astype(f32)
            psend[block, :, piece] = part_sum.astype(bf16)
            pass_on(side, block, number).start()

    def edge(last):
        @pl.when((last == 1) & (ep < ep_count - 1))
        def _():
            halo(1).wait_recv()

        @pl.when((last == 0) & (ep > 0))
        def _():
            halo(0).wait_recv()

        attend((tp_count - 1) * last)

    def give_back(low, high):
        for part in range(low, high):
            for d in range(1, ep_count):
                return_copy(tp, d, part).start()

    def reduce_merged():
        end = (tp_count - 1) * (1 - outward)
        second = 1 + (tp_count - 3) * outward

        def slot(i):
            def stream(j, carry):
                part = i - LAG * j
                side = jnp.where(j == 1, outward, 1 - outward)
                block = jnp.where(j == 0, tp_count - 1 - end, jnp.where(j == 1, end, second))

                @pl.when((part >= 0) & (part < parts))
                def _():
                    reduce_piece(side, block, part, weights_of(block))

                return carry

            lax.fori_loop(0, 3, stream, 0)

            @pl.when(i == 1)
            def _():
                block, _ = near(outward, 2)
                send_first(outward, block).wait_recv()
                project_far(block)
                project(block)
                start_halo(block)
                give_back(0, parts)

            @pl.when(i == 2)
            def _():
                attend(second)

            @pl.when((i == 3) | (i == 5))
            def _():
                edge(jnp.where(i == 3, outward, 1 - outward))

        each_part(slot, parts + 2 * LAG)

    def reduce_step(step):
        def one(turn, carry):
            side = jnp.where(2 * tp < tp_count, 1 - turn, turn)
            block = jnp.where(side == 0, step - tp, 2 * (tp_count - 1) - step - tp)
            active = (block >= 0) & (block < tp_count)
            if swaps:
                block = swapped(1 - side, block, True)
            active = active & ((block - tp) * (1 - 2 * side) > 0)

            @pl.when(active)
            def _():
                weights = weights_of(block)
                each_part(lambda part: reduce_piece(side, block, part, weights))

            return carry

        lax.fori_loop(0, 2, one, 0)

    early = tp_count > 2

    def hop(k, carry):
        def one_turn(turn):
            def receive(second, carry):
                part = turn - second * LAG
                side = jnp.where(2 * tp < tp_count, second, 1 - second)
                block, inside = at(side, k)

                @pl.when(inside & (part >= 0) & (part < parts))
                def _():
                    send_second(side, block, part).wait_recv()

                    @pl.when(exists(side))
                    def _():
                        send_second(side, block, part).start()

                    @pl.when(part == 0)
                    def _():
                        send_meta(side, block).wait_recv()

                        @pl.when(exists(side))
                        def _():
                            send_meta(side, block).start()

                    @pl.when(late(side) & (k == 1) & (part == parts - 1))
                    def _():
                        for own in range(AHEAD, parts):
                            send_second(side, tp, own).start()

                    pick_part(block, part)

                return carry

            lax.fori_loop(0, 2, receive, 0)

            @pl.when(k == 1)
            def _():
                @pl.when(turn == 1)
                def _():
                    tables()

                @pl.when(turn == 2)
                def _():
                    project(tp)
                    start_halo(tp)

            if early:

                @pl.when(ends & (k == tp_count - 1) & (turn == LAG + 1))
                def _():
                    reduce_step(1)


            middle = ends & (k > 1) & (k == tp_count - 1) & (turn == LAG)

            @pl.when(middle | ((k == 1) & (turn == LAG + 2)))
            def _():
                experts_at(k - 1)

        each_part(one_turn, parts + LAG)
        for side in range(2):
            start_own_first(side, k)
        for side in range(2):
            block, inside = at(side, k)

            @pl.when(inside)
            def _():
                shared_hidden(block)

        if assist:

            @pl.when(helps & (k == 2))
            def _():
                relay_first()

        if slim:

            @pl.when(helps & (k == tp_count - 1))
            def _():
                side = 1 - outward
                block, _ = near(side, 1)
                send_first(side, block).wait_recv()
                send_first(side, block).start()
                project(block)
                start_halo(block)

        @pl.when((k > 1) & (jnp.logical_not(ends) | (k < tp_count - 1)))
        def _():
            experts_at(k - 1)

        return carry

    lax.fori_loop(1, tp_count, hop, 0)
    if early:
        reduce_step(2)

    experts_at(tp_count - 1)

    @pl.when(ends | (not slim))
    def _():
        give_back(0, parts // 2)

    if assist:

        @pl.when(helps)
        def _():
            relay_second()


    def first_hop(k, carry):
        def open_at(side):
            block, inside = near(side, k)
            if slim:
                inside = inside & (k == 1) & (side == outward)
            return block, inside

        for side in range(2):
            block, inside = open_at(side)

            @pl.when(inside & plain)
            def _():
                send_first(side, block).wait_recv()

                @pl.when(carries(side))
                def _():
                    send_first(side, block).start()

        if assist:

            @pl.when(helps)
            def _():
                @pl.when(k == 1)
                def _():
                    relay_last()

                def one(turn, carry):
                    block, inside = near(outward, k * turn)

                    if slim:
                        inside = inside & (k == 1)

                    @pl.when(inside & ((turn == 1) | (k == 1)))
                    def _():
                        project_far(block)

                    return carry

                lax.fori_loop(0, 2, one, 0)

        def use(side, carry):
            block, inside = open_at(side)

            @pl.when(inside & plain)
            def _():
                project(block)
                start_halo(block)

            return carry

        lax.fori_loop(0, 2, use, 0)
        if not slim:

            @pl.when((k == jnp.maximum(tp, tp_count - 1 - tp)) & plain)
            def _():
                give_back(parts // 2, parts)

        if slim:

            @pl.when((k == 2) & ends)
            def _():
                reduce_step(3)

            @pl.when((k == 2) & helps)
            def _():
                reduce_merged()

        elif early:

            @pl.when(k > 1)
            def _():
                reduce_step(2 * k - 1)
                reduce_step(2 * k)

        else:
            reduce_step(2 * k - 1)

        def settle(side, carry):
            block, _ = near(side, k - 1)

            inner = (block > 0) & (block < tp_count - 1) & ((k > 1) | (side == 0))
            if slim:
                inner = inner & (k == 1)

            @pl.when(inner & plain)
            def _():
                attend(block)

            return carry

        lax.fori_loop(0, 2, settle, 0)
        return carry

    lax.fori_loop(1, tp_count, first_hop, 0)
    if assist:

        @pl.when(ends)
        def _():
            def arrive(block):
                @pl.when(block != tp)
                def _():
                    query_copy(block, toward(jnp.where(tp == 0, 0, 1))).wait_recv()
                    kv_copy(block, toward(jnp.where(tp == 0, 0, 1))).wait_recv()
                    start_halo(block)

            each_part(arrive, tp_count)
            give_back(parts // 2, parts)
            each_part(lambda block: attend(block + 1), tp_count - 2)

    @pl.when(jnp.logical_not(helps) | (not slim))
    def _():
        each_part(lambda turn: edge(jnp.where(2 * tp < tp_count, 1 - turn, turn)), 2)

    own_weights = weights_of(tp)

    def last_part(part):
        span = part_span(part)
        return_part(tp, part).wait_recv()
        own = value_of(tp, own_weights, span)

        for i in range(CHUNK // PASS):

            @pl.when(tp > 0)
            def _():
                pass_on(0, tp, part * (CHUNK // PASS) + i).wait_recv()

            @pl.when(tp < tp_count - 1)
            def _():
                pass_on(1, tp, part * (CHUNK // PASS) + i).wait_recv()

        psend[tp, :, span] = (
            own + sides[0, tp, :, span].astype(f32) + sides[1, tp, :, span].astype(f32)
        ).astype(bf16)
        out_copy(part).start()

    each_part(last_part)

    def finish(block):
        return_all(block).wait_send()
        for side in range(2):
            passed = block <= tp if side == 0 else block >= tp
            summed = block > tp if side == 0 else block < tp

            @pl.when(exists(side) & passed)
            def _():
                ref = gath2.at[block]
                remote(ref, ref, s2.at[side, block], r2.at[block, 0], toward(side)).wait_send()
                send_meta(side, block).wait_send()

            @pl.when(carries(side) & passed)
            def _():
                send_first(side, block).wait_send()

            @pl.when(summed)
            def _():
                for number in range(width // PASS):
                    pass_on(side, block, number).wait_send()

    each_part(finish, tp_count)
    if assist:

        @pl.when(ends)
        def _():
            for copy in lend_out():
                copy.wait_send()

        @pl.when(helps)
        def _():
            for copies in relays() + (relays_across() if pair == 2 else []):
                for copy in copies:
                    copy.wait_send()

            def sent(block):
                @pl.when(block != tp + 1 - 2 * outward)
                def _():
                    query_copy(block, toward(outward)).wait_send()
                    kv_copy(block, toward(outward)).wait_send()

            each_part(sent, tp_count)

    each_part(lambda part: out_copy(part).wait())
    each_part(lambda block: mixed_copy(block).wait(), tp_count)

    @pl.when(ep < ep_count - 1)
    def _():
        halo(0).wait_send()

    @pl.when(ep > 0)
    def _():
        halo(1).wait_send()


def layer(
    second, first, gain_second, gain_first, router, routes, inverse, sink,
    gate, up, down, sgate, sup, sdown, wq, wk, wv, grp_count, ep_count, tp_count, slots,
):
    rows, width = second.shape
    experts = router.shape[0]
    hbm = pl.BlockSpec(memory_space=pl.ANY)
    dma = pltpu.SemaphoreType.DMA
    bf16, f32 = jnp.bfloat16, jnp.float32
    total = ep_count * slots
    parts = width // CHUNK
    span = tp_count * rows
    kv_cols = wk.shape[1] + wv.shape[1]
    return pl.pallas_call(
        functools.partial(layer_kernel, grp_count, ep_count, tp_count, slots),
        out_shape=(
            jax.ShapeDtypeStruct((rows, width), bf16),
            jax.ShapeDtypeStruct((span, wq.shape[1]), bf16),
        ),
        in_specs=[hbm] * 17,
        out_specs=(hbm, hbm),
        scratch_shapes=[
            pltpu.VMEM((span, wq.shape[1]), bf16),
            pltpu.VMEM((rows, width), bf16),
            pltpu.VMEM(gain_second.shape, f32),
            pltpu.VMEM(router.shape, bf16),
            pltpu.VMEM(routes.shape, jnp.int32),
            pltpu.VMEM(gain_first.shape, f32),
            pltpu.VMEM(inverse.shape, f32),
            pltpu.SMEM(sink.shape, f32),
            pltpu.VMEM((tp_count, rows, width), bf16),
            pltpu.VMEM((tp_count, rows, width), bf16),
            pltpu.VMEM((rows, width), bf16),
            pltpu.VMEM((tp_count, 2 * experts, rows), f32),
            pltpu.VMEM((tp_count, total, width), bf16),
            pltpu.VMEM((tp_count, total, width), bf16),
            pltpu.VMEM((tp_count, total, width), bf16),
            pltpu.VMEM((2, tp_count, rows, width), bf16),
            pltpu.VMEM((tp_count, rows, width), bf16),
            pltpu.VMEM(gate.shape[1:], bf16),
            pltpu.VMEM(up.shape[1:], bf16),
            pltpu.VMEM(down.shape[1:], bf16),
            pltpu.VMEM(sgate.shape, bf16),
            pltpu.VMEM(sup.shape, bf16),
            pltpu.VMEM(sdown.shape, bf16),
            pltpu.VMEM(wq.shape, bf16),
            pltpu.VMEM(wk.shape, bf16),
            pltpu.VMEM(wv.shape, bf16),
            pltpu.VMEM(wq.shape, bf16),
            pltpu.VMEM(wk.shape, bf16),
            pltpu.VMEM(wv.shape, bf16),
            pltpu.VMEM((tp_count, rows, wq.shape[1]), bf16),
            pltpu.VMEM((tp_count, rows, kv_cols), bf16),
            pltpu.VMEM((tp_count, rows, sgate.shape[1]), bf16),
            pltpu.VMEM((total, gate.shape[2]), bf16),
            pltpu.VMEM((span, LANES), f32),
            pltpu.VMEM((span, LANES), f32),
            pltpu.VMEM((span, wq.shape[1]), bf16),
            pltpu.VMEM((span + 2 * rows, kv_cols), bf16),
            dma((17,)),
            dma((2, tp_count)),
            dma((tp_count, parts)),
            dma((2, tp_count)),
            dma((tp_count,)),
            dma((2, tp_count)),
            dma((tp_count,)),
            dma((tp_count,)),
            dma((tp_count,)),
            dma((tp_count,)),
            dma((tp_count, parts)),
            dma((tp_count, width // PASS)),
            dma((2, tp_count, width // PASS)),
            dma((2,)),
            dma((2,)),
            dma((parts,)),
            dma((tp_count,)),
            dma((2 * grp_count, grp_count, 3)),
            dma((2 * grp_count, 3)),
            dma((2, tp_count)),
            dma((2, tp_count)),
        ],
        compiler_params=pltpu.CompilerParams(
            collective_id=0, has_side_effects=True, vmem_limit_bytes=VMEM_LIMIT
        ),
        name="layer",
    )(
        second, gain_second, router, routes, gain_first, inverse, sink,
        first, gate, up, down, sgate, sup, sdown, wq, wk, wv,
    )


def settle_kernel(first, second, first_out, second_out, first_buf, second_buf, sems):
    arrays = [(first, first_buf, first_out), (second, second_buf, second_out)]
    pieces = []
    for i, (source, buffer, target) in enumerate(arrays):
        half = source.shape[0] // 2
        for j in range(2):
            rows = pl.ds(j * half, half)
            pieces.append(
                (
                    pltpu.make_async_copy(source.at[rows], buffer.at[rows], sems.at[0, i, j]),
                    pltpu.make_async_copy(buffer.at[rows], target.at[rows], sems.at[1, i, j]),
                )
            )
    for load, _ in pieces:
        load.start()
    for load, store in pieces:
        load.wait()
        store.start()
    for _, store in pieces:
        store.wait()


def settle(first, second):
    hbm = pl.BlockSpec(memory_space=pl.ANY)
    return pl.pallas_call(
        settle_kernel,
        out_shape=(jax.ShapeDtypeStruct(first.shape, first.dtype), jax.ShapeDtypeStruct(second.shape, second.dtype)),
        in_specs=[hbm, hbm],
        out_specs=(hbm, hbm),
        scratch_shapes=[
            pltpu.VMEM(first.shape, first.dtype),
            pltpu.VMEM(second.shape, second.dtype),
            pltpu.SemaphoreType.DMA((2, 2, 2)),
        ],
        compiler_params=pltpu.CompilerParams(vmem_limit_bytes=VMEM_LIMIT),
        name="settle",
    )(first, second)


def body(
    mixer_in,
    mixer_gain,
    w_query,
    w_key,
    w_value,
    sink_logit,
    moe_in,
    moe_gain,
    router,
    routes,
    expert_gate,
    expert_up,
    expert_down,
    shared_gate,
    shared_up,
    shared_down,
):
    tokens = mixer_in.shape[0]
    ep_count, tp_count = lax.axis_size("ep"), lax.axis_size("tp")
    top_count = routes.shape[1]
    experts = router.shape[1]
    capacity = 3 * top_count * tokens // (2 * experts)
    slots = -(-capacity // 16) * 16
    half = HEAD_DIM // 2
    inverse = np.float32(THETA) ** (-(np.arange(half, dtype=np.float32) * np.float32(2.0)) / np.float32(HEAD_DIM))
    moe_out, mixed = layer(
        moe_in, mixer_in, moe_gain[None, :], mixer_gain[None, :], router.T, routes.T,
        jnp.asarray(np.tile(inverse, LANES // half)[None, :]), sink_logit[None, :],
        expert_gate, expert_up, expert_down, shared_gate, shared_up, shared_down,
        w_query, w_key, w_value, lax.axis_size("grp"), ep_count, tp_count, slots,
    )
    moe_out, mixed = settle(moe_out, mixed)
    return (mixed, moe_out)


def solution(mesh):
    return jax.shard_map(
        body,
        mesh=mesh,
        in_specs=(
            P(("grp", "ep", "tp"), None),
            P(),
            P(None, "tp"),
            P(None, "tp"),
            P(None, "tp"),
            P("tp"),
            P(("grp", "ep", "tp"), None),
            P(),
            P(),
            P(("grp", "ep", "tp"), None),
            P(("ep", "tp"), None, None),
            P(("ep", "tp"), None, None),
            P(("ep", "tp"), None, None),
            P(None, "tp"),
            P(None, "tp"),
            P("tp", None),
        ),
        out_specs=(P(("grp", "ep"), "tp"), P(("grp", "ep", "tp"), None)),
        check_vma=False,
    )
```

```python
import functools

import jax
import jax.numpy as jnp
import numpy as np
from jax import lax
from jax.experimental import pallas as pl
from jax.experimental.pallas import tpu as pltpu
from jax.sharding import PartitionSpec as P

HEAD_DIM = 64
WINDOW = 128
EPS = 1e-06
THETA = 10000.0
ROUTED_SCALE = 2.5
LANES = 128
CHUNK = 512
PASS = 256
LAG = 2
AHEAD = 1
MESH = pl.DeviceIdType.MESH
VMEM_LIMIT = 63 * 2**20


def remote(src, dst, send_sem, recv_sem, device):
    return pltpu.make_async_remote_copy(
        src_ref=src,
        dst_ref=dst,
        send_sem=send_sem,
        recv_sem=recv_sem,
        device_id=device,
        device_id_type=MESH,
    )


def greet(grp, ep, tp, grp_count, ep_count, tp_count):
    barrier = pltpu.get_barrier_semaphore()

    @pl.when(tp > 0)
    def _():
        pl.semaphore_signal(barrier, inc=1, device_id=(grp, ep, tp - 1), device_id_type=MESH)

    @pl.when(tp < tp_count - 1)
    def _():
        pl.semaphore_signal(barrier, inc=1, device_id=(grp, ep, tp + 1), device_id_type=MESH)

    for d in range(1, ep_count):
        pl.semaphore_signal(
            barrier, inc=1, device_id=(grp, lax.rem(ep + d, ep_count), tp), device_id_type=MESH
        )
    for d in range(1, grp_count):
        pl.semaphore_signal(
            barrier, inc=1, device_id=(lax.rem(grp + d, grp_count), ep, tp), device_id_type=MESH
        )
    return barrier


def layer_kernel(
    grp_count, ep_count, tp_count, slots,
    second_hbm, gain_second_hbm, router_hbm, routes_hbm, gain_first_hbm, inverse_hbm, sink_hbm,
    first_hbm, gate_hbm, up_hbm, down_hbm, sgate_hbm, sup_hbm, sdown_hbm, wq_hbm, wk_hbm, wv_hbm,
    out, mixed_out,
    mixed, second_in, gain_second, router, routes, gain_first, inverse, sink,
    gath2, gath1, first_in, metag, sbuf, disp, back, sides, psend,
    gate, up, down, sgate, sup, sdown, wq, wk, wv, far_q, far_k, far_v, lent_q, lent_kv,
    hidden, hexp, cosine, sine, qbuf, kvbuf,
    l_sem, s2, r2, sm, rm, s1, r1, sd, rd, sb, rb, sp, rs, hs, hr, out_sem, mixed_sem, ws, wr, qs, qr,
):
    grp, ep, tp = lax.axis_index("grp"), lax.axis_index("ep"), lax.axis_index("tp")
    rows, width = second_in.shape
    experts = metag.shape[1] // 2
    total = ep_count * slots
    parts = width // CHUNK
    f32, bf16 = jnp.float32, jnp.bfloat16
    away = pl.ds(slots, total - slots)

    barrier = greet(grp, ep, tp, grp_count, ep_count, tp_count)
    early_pairs = [
        (second_hbm, second_in),
        (gain_second_hbm, gain_second),
        (routes_hbm, routes),
        (router_hbm, router),
    ]
    pairs = early_pairs + [
        (gain_first_hbm, gain_first),
        (first_hbm, first_in),
        (sgate_hbm, sgate),
        (sup_hbm, sup),
        (wq_hbm, wq),
        (wk_hbm, wk),
        (wv_hbm, wv),
        (inverse_hbm, inverse),
        (sink_hbm, sink),
        (gate_hbm.at[0], gate),
        (up_hbm.at[0], up),
        (down_hbm.at[0], down),
        (sdown_hbm, sdown),
    ]
    local = [pltpu.make_async_copy(src, dst, l_sem.at[i]) for i, (src, dst) in enumerate(pairs)]
    for copy in local:
        copy.start()

    def toward(side):
        return (grp, ep, tp + 1 - 2 * side)

    def exists(side):
        return (tp + 1 - 2 * side >= 0) & (tp + 1 - 2 * side < tp_count)

    def peer(d):
        return (grp, lax.rem(ep + d, ep_count), tp)

    def part_span(part, size=CHUNK):
        return pl.ds(pl.multiple_of(part * size, size), size)

    def each_part(body, count=parts):
        def step(part, carry):
            body(part)
            return carry

        lax.fori_loop(0, count, step, 0)

    def near(side, distance):
        block = tp + (2 * side - 1) * distance
        return block, (block >= 0) & (block < tp_count)

    swaps = tp_count > 2

    def swapped(side, block, allowed):
        far, second = (tp_count - 1) * side, 1 + (tp_count - 3) * side
        other = jnp.where(block == second, far, jnp.where(block == far, second, block))
        return jnp.where(allowed, other, block)

    def at(side, order):
        block, inside = near(side, order)
        if swaps:
            block = swapped(side, block, jnp.where(side == 0, tp, tp_count - 1 - tp) >= 2)
        return block, inside

    def late(side):
        return (tp == 1 + side * (tp_count - 3)) & swaps

    def lane(side, block, owner):
        return jnp.where((block == owner) & (side == 1), tp_count, block)

    def send_second(side, block, part):
        ref = gath2.at[block, :, part_span(part)]
        return remote(ref, ref, s2.at[lane(side, block, tp)], r2.at[block, part], toward(side))

    def send_meta(side, block):
        return remote(metag.at[block], metag.at[block], sm.at[lane(side, block, tp)], rm.at[block], toward(side))

    assist = tp_count >= 4
    ends = (tp == 0) | (tp == tp_count - 1)
    slim = tp_count == 4
    plain = jnp.logical_not(ends) | (not assist)
    helps = ((tp == 1) | (tp == tp_count - 2)) & assist
    outward = jnp.where(tp == 1, 1, 0)
    pair = 2 if ep_count % 2 == 0 else 1
    core = lax.rem(ep, pair)
    piece_rows = width // (grp_count * pair)
    lent = [(wq, far_q), (wk, far_k), (wv, far_v)]

    def carries(side):
        target = tp + 1 - 2 * side
        return exists(side) & (((target > 0) & (target < tp_count - 1)) | (not assist))

    def share_of(group, half):
        return group * pair + half

    def lend(share, to, device, own):
        span = pl.ds(pl.multiple_of(share * piece_rows, piece_rows), piece_rows)
        return [
            remote(
                (near_ref if own else far_ref).at[span], far_ref.at[span],
                ws.at[to, i], wr.at[share, i], device,
            )
            for i, (near_ref, far_ref) in enumerate(lent)
        ]

    def lend_out():
        return lend(share_of(grp, core), 0, (grp, ep, jnp.where(tp == 0, 1, tp_count - 2)), True)

    def partner():
        return (grp, ep + 1 - 2 * core, tp)

    def relays():
        mine = share_of(grp, core)
        copies = []
        for d in range(1, grp_count):
            copies.append(lend(mine, d, (lax.rem(grp + d, grp_count), ep, tp), False))
        if pair == 2:
            copies.append(lend(mine, 0, partner(), False))
        return copies

    def relays_across():
        copies = []
        for d in range(1, grp_count):
            copies.append(lend(share_of(lax.rem(grp + d, grp_count), core), grp_count - 1 + d, partner(), False))
        return copies

    def relay_first():
        for copy in lend(share_of(grp, core), 0, toward(outward), False):
            copy.wait_recv()
        for copies in relays():
            for copy in copies:
                copy.start()

    def relay_second():
        for copies in relays_across():
            for copy in copies:
                copy.wait_recv()
            if pair == 2:
                for copy in copies:
                    copy.start()

    def relay_last():
        if pair == 2:
            for group in range(grp_count):
                for copy in lend(share_of(group, 1 - core), 0, partner(), False):
                    copy.wait_recv()

    def query_copy(block, device):
        return remote(
            lent_q.at[block], qbuf.at[part_span(block, rows)], qs.at[0], qr.at[0], device
        )

    def kv_copy(block, device):
        return remote(
            lent_kv.at[block], kvbuf.at[part_span(block + 1, rows)], qs.at[1], qr.at[1], device
        )

    def lent_all(device):
        span = pl.ds(0, (tp_count - 1) * rows)
        return [
            remote(ref.at[span], ref.at[span], qs.at[i], qr.at[i], device) for i, ref in enumerate((qbuf, kvbuf))
        ]

    def send_first(side, block):
        return remote(gath1.at[block], gath1.at[block], s1.at[lane(side, block, tp)], r1.at[block], toward(side))

    def dispatch_copy(block, d, span):
        mine = pl.ds(d * slots, slots)
        return remote(sbuf.at[block, mine, span], disp.at[block, mine, span], sd.at[block], rd.at[block], peer(d))

    def dispatch_all(block):
        return remote(sbuf.at[block, away], disp.at[block, away], sd.at[block], rd.at[block], peer(1))

    def return_copy(block, d, part):
        mine, span = pl.ds(d * slots, slots), part_span(part)
        return remote(
            sbuf.at[block, mine, span], back.at[block, mine, span],
            sb.at[block], rb.at[block, part], peer(ep_count - d),
        )

    def return_part(block, part):
        span = part_span(part)
        return remote(
            sbuf.at[block, away, span], back.at[block, away, span], sb.at[block], rb.at[block, part], peer(1)
        )

    def return_all(block):
        return remote(sbuf.at[block, away], back.at[block, away], sb.at[block], rb.at[block, 0], peer(1))

    def pass_on(side, block, part, owner):
        span = part_span(part, PASS)
        return remote(
            psend.at[block, :, span], sides.at[side, block, :, span],
            sp.at[block], rs.at[lane(side, block, owner), part], toward(side),
        )

    def halo(side):
        source = tp_count * rows if side == 0 else rows
        target = 0 if side == 0 else (tp_count + 1) * rows
        return remote(
            kvbuf.at[pl.ds(source, rows)], kvbuf.at[pl.ds(target, rows)],
            hs.at[side], hr.at[side], (grp, ep + (1 if side == 0 else -1), tp),
        )

    def out_copy(part):
        span = part_span(part)
        return pltpu.make_async_copy(psend.at[tp, :, span], out.at[:, span], out_sem.at[0])

    def mixed_copy(block):
        span = part_span(block, rows)
        return pltpu.make_async_copy(mixed.at[span], mixed_out.at[span], mixed_sem.at[0])

    def normalize(source, gain, target):
        def squares(part, carry):
            values = source[:, part_span(part)].astype(f32)
            return carry + jnp.sum(values * values, axis=1, keepdims=True)

        summed = lax.fori_loop(0, parts, squares, jnp.zeros((rows, 1), f32))
        factor = lax.rsqrt(summed / width + EPS)

        def scale(part):
            span = part_span(part)
            target[:, span] = (source[:, span].astype(f32) * factor * gain[:, span]).astype(bf16)

        each_part(scale)

    def places_of(block, d):
        expert = lax.rem(ep + d, ep_count) * tp_count + tp
        slot_ids = lax.broadcasted_iota(jnp.int32, (slots, rows), 0).astype(f32)
        return slot_ids == metag[block, pl.ds(expert, 1), :], expert

    def pick_part(block, part):
        span = part_span(part)
        picks = [jnp.where(places_of(block, d)[0], 1.0, 0.0) for d in range(ep_count)]
        pick = jnp.concatenate(picks, axis=0).astype(bf16)
        picked = jnp.dot(pick, gath2[block, :, span], preferred_element_type=f32).astype(bf16)
        disp[block, 0:slots, span] = picked[0:slots]
        sbuf[block, slots:total, span] = picked[slots:total]
        for d in range(1, ep_count):
            dispatch_copy(block, d, span).start()

    def shared_hidden(block):
        values = gath2[block]
        gated = jnp.dot(values, sgate[...], preferred_element_type=f32)
        lifted = jnp.dot(values, sup[...], preferred_element_type=f32)
        hidden[block] = (jax.nn.silu(gated) * lifted).astype(bf16)

    def expert(block):
        dispatch_all(block).wait()

        def units(part):
            span = part_span(part, 256)
            values = disp[block]
            gated = jnp.dot(values, gate[:, span], preferred_element_type=f32)
            lifted = jnp.dot(values, up[:, span], preferred_element_type=f32)
            hexp[:, span] = (jax.nn.silu(gated) * lifted).astype(bf16)

        each_part(units, gate.shape[1] // 256)

        def columns(part):
            span = part_span(part)
            result = jnp.dot(hexp[...], down[:, span], preferred_element_type=f32).astype(bf16)
            back[block, 0:slots, span] = result[0:slots]
            sbuf[block, slots:total, span] = result[slots:total]

            @pl.when(block != tp)
            def _():
                for d in range(1, ep_count):
                    return_copy(block, d, part).start()

        each_part(columns)

    def experts_at(order):
        def one(side, carry):
            block, inside = at(side, order)

            @pl.when(inside & ((order > 0) | (side == 0)))
            def _():
                expert(block)

            return carry

        lax.fori_loop(0, 2, one, 0)

    def start_own_first(side, step):
        last = tp if side == 0 else tp_count - 1 - tp

        @pl.when(carries(side) & (step == last))
        def _():
            send_first(side, tp).start()

    def rotated(values, cos_rows, sin_rows):
        pieces = []
        half = HEAD_DIM // 2
        size = LANES if values.shape[1] % LANES == 0 else HEAD_DIM
        for start in range(0, values.shape[1], size):
            piece = values[:, start : start + size]
            if size == LANES:
                lane = lax.broadcasted_iota(jnp.int32, piece.shape, 1)
                crossed = jnp.where(
                    lax.rem(lane, HEAD_DIM) < half,
                    pltpu.roll(piece, LANES - half, 1),
                    pltpu.roll(piece, half, 1),
                )
            else:
                crossed = jnp.concatenate([piece[:, half:], piece[:, :half]], axis=1)
            pieces.append(piece * cos_rows[:, :size] + crossed * sin_rows[:, :size])
        return pieces[0] if len(pieces) == 1 else jnp.concatenate(pieces, axis=1)

    def projected(block, query_w, key_w, value_w):
        span = part_span(block, rows)
        values = gath1[block]
        cos_rows, sin_rows = cosine[span, :], sine[span, :]
        query = jnp.dot(values, query_w[...], preferred_element_type=f32)
        key = jnp.dot(values, key_w[...], preferred_element_type=f32)
        value = jnp.dot(values, value_w[...], preferred_element_type=f32)
        joined = jnp.concatenate([rotated(key, cos_rows, sin_rows), value], axis=1).astype(bf16)
        return rotated(query, cos_rows, sin_rows).astype(bf16), joined

    def project(block):
        qbuf[part_span(block, rows), :], kvbuf[part_span(block + 1, rows), :] = projected(block, wq, wk, wv)

    def project_far(block):
        lent_q[block], lent_kv[block] = projected(block, far_q, far_k, far_v)
        query_copy(block, toward(outward)).start()
        kv_copy(block, toward(outward)).start()

    def start_halo(block):
        @pl.when((block == tp_count - 1) & (ep < ep_count - 1))
        def _():
            halo(0).start()

        @pl.when((block == 0) & (ep > 0))
        def _():
            halo(1).start()

    def tables():
        def one(block):
            start = pl.multiple_of(block * rows, rows)
            shape = (rows, LANES)
            place = ep * (tp_count * rows) + start + lax.broadcasted_iota(jnp.int32, shape, 0)
            angle = place.astype(f32) * inverse[...]
            lane = lax.broadcasted_iota(jnp.int32, shape, 1)
            turn = jnp.sin(angle)
            cosine[pl.ds(start, rows), :] = jnp.cos(angle)
            sine[pl.ds(start, rows), :] = jnp.where(lax.rem(lane, HEAD_DIM) < HEAD_DIM // 2, -turn, turn)

        each_part(one, tp_count)

    kv_heads = wk.shape[1] // HEAD_DIM
    group = wq.shape[1] // wk.shape[1]

    def attend(block):
        base = pl.multiple_of(block * rows, rows)
        window = kvbuf[pl.ds(base, 3 * rows), :]
        query = qbuf[pl.ds(base, rows), :]
        shape = (rows, 3 * rows)
        row = lax.broadcasted_iota(jnp.int32, shape, 0)
        col = lax.broadcasted_iota(jnp.int32, shape, 1)
        gap = col - row - rows
        low = jnp.where((ep == 0) & (block == 0), rows, 0)
        high = jnp.where((ep == ep_count - 1) & (block == tp_count - 1), 2 * rows, 3 * rows)
        near = (gap <= WINDOW) & (gap >= -WINDOW) & (col >= low) & (col < high)
        pieces = []
        for g in range(kv_heads):
            keys = window[:, g * HEAD_DIM : (g + 1) * HEAD_DIM]
            start = (kv_heads + g) * HEAD_DIM
            values = window[:, start : start + HEAD_DIM]
            for h in range(g * group, (g + 1) * group):
                scores = lax.dot_general(
                    query[:, h * HEAD_DIM : (h + 1) * HEAD_DIM], keys, (((1,), (1,)), ((), ())),
                    preferred_element_type=f32,
                ) * HEAD_DIM ** (-0.5)
                scores = jnp.where(near, scores, -jnp.inf)
                bound = sink[0, h]
                top = jnp.maximum(jnp.max(scores, axis=1, keepdims=True), bound)
                weights = jnp.exp(scores - top)
                summed = jnp.sum(weights, axis=1, keepdims=True) + jnp.exp(bound - top)
                share = (weights * (1.0 / summed)).astype(bf16)
                pieces.append(jnp.dot(share, values, preferred_element_type=f32))
        mixed[pl.ds(base, rows), :] = jnp.concatenate(pieces, axis=1).astype(bf16)
        mixed_copy(block).start()

    for copy in local[: len(early_pairs)]:
        copy.wait()
    normalize(second_in, gain_second, gath2.at[tp])
    ids = lax.broadcasted_iota(jnp.int32, (experts, rows), 0)
    hit = ids == routes[0:1, :]
    for j in range(1, routes.shape[0]):
        hit = hit | (ids == routes[j : j + 1, :])
    earlier = (
        lax.broadcasted_iota(jnp.int32, (rows, rows), 0) < lax.broadcasted_iota(jnp.int32, (rows, rows), 1)
    )
    before = jnp.dot(
        jnp.where(hit, 1.0, 0.0).astype(bf16), jnp.where(earlier, 1.0, 0.0).astype(bf16),
        preferred_element_type=f32,
    )
    metag[tp, 0:experts, :] = jnp.where(hit, before, -1.0)
    pl.semaphore_wait(barrier, ep_count + grp_count - 1 + jnp.where((tp > 0) & (tp < tp_count - 1), 1, 0))

    def send_own(part):
        for side in range(2):

            @pl.when(exists(side) & (jnp.logical_not(late(side)) | (part < AHEAD)))
            def _():
                send_second(side, tp, part).start()

    send_own(0)
    affinity = lax.dot_general(
        router[...], gath2[tp], (((1,), (1,)), ((), ())), preferred_element_type=f32
    )
    chosen = jnp.where(hit, jax.nn.sigmoid(affinity), 0.0)
    metag[tp, experts : 2 * experts, :] = ROUTED_SCALE * chosen / jnp.sum(chosen, axis=0, keepdims=True)
    pick_part(tp, 0)
    for side in range(2):

        @pl.when(exists(side))
        def _():
            send_meta(side, tp).start()

    for part in range(1, parts):
        send_own(part)

    def pick_rest(part, carry):
        pick_part(tp, part)
        return carry

    lax.fori_loop(1, parts, pick_rest, 0)
    for copy in local[len(early_pairs) : len(early_pairs) + 2]:
        copy.wait()
    normalize(first_in, gain_first, gath1.at[tp])

    @pl.when(tp == 0)
    def _():
        sides[0] = jnp.zeros(sides.shape[1:], sides.dtype)

    @pl.when(tp == tp_count - 1)
    def _():
        sides[1] = jnp.zeros(sides.shape[1:], sides.dtype)

    @pl.when(ep == 0)
    def _():
        kvbuf[0:rows, :] = jnp.zeros((rows, kvbuf.shape[1]), bf16)

    @pl.when(ep == ep_count - 1)
    def _():
        kvbuf[(tp_count + 1) * rows : (tp_count + 2) * rows, :] = jnp.zeros((rows, kvbuf.shape[1]), bf16)

    for copy in local[len(early_pairs) + 2 :]:
        copy.wait()
    if assist:

        @pl.when(ends)
        def _():
            for copy in lend_out():
                copy.start()

    for side in range(2):
        start_own_first(side, 0)
    shared_hidden(tp)

    def weights_of(block):
        pieces = []
        for d in range(ep_count):
            hit_rows, number = places_of(block, d)
            pieces.append(jnp.where(hit_rows, metag[block, pl.ds(experts + number, 1), :], 0.0))
        weights = jnp.concatenate(pieces, axis=0)
        top = weights.astype(bf16)
        return top, (weights - top.astype(f32)).astype(bf16)

    def value_of(block, weights, span):
        turned = (((0,), (0,)), ((), ()))
        picked = back[block, :, span]
        return (
            lax.dot_general(weights[0], picked, turned, preferred_element_type=f32)
            + lax.dot_general(weights[1], picked, turned, preferred_element_type=f32)
            + jnp.dot(hidden[block], sdown[:, span], preferred_element_type=f32)
        )

    def reduce_piece(side, block, part, weights):
        span = part_span(part)
        return_part(block, part).wait_recv()
        own = value_of(block, weights, span)

        for i in range(CHUNK // PASS):
            number = part * (CHUNK // PASS) + i
            piece = part_span(number, PASS)

            @pl.when(exists(1 - side))
            def _():
                pass_on(side, block, number, tp).wait_recv()

            part_sum = own[:, i * PASS : (i + 1) * PASS] + sides[side, block, :, piece].astype(f32)
            psend[block, :, piece] = part_sum.astype(bf16)
            pass_on(side, block, number, tp + 1 - 2 * side).start()

    def edge(last):
        @pl.when((last == 1) & (ep < ep_count - 1))
        def _():
            halo(1).wait_recv()

        @pl.when((last == 0) & (ep > 0))
        def _():
            halo(0).wait_recv()

        attend((tp_count - 1) * last)

    def give_back(low, high):
        for part in range(low, high):
            for d in range(1, ep_count):
                return_copy(tp, d, part).start()

    def reduce_merged():
        end = (tp_count - 1) * (1 - outward)
        second = 1 + (tp_count - 3) * outward

        def slot(i):
            def stream(j, carry):
                part = i - LAG * j
                side = jnp.where(j == 1, outward, 1 - outward)
                block = jnp.where(j == 0, tp_count - 1 - end, jnp.where(j == 1, end, second))

                @pl.when((part >= 0) & (part < parts))
                def _():
                    reduce_piece(side, block, part, weights_of(block))

                return carry

            lax.fori_loop(0, 3, stream, 0)

            @pl.when(i == 1)
            def _():
                block, _ = near(outward, 2)
                send_first(outward, block).wait_recv()
                project_far(block)
                project(block)
                start_halo(block)
                give_back(0, parts)

            @pl.when(i == 2)
            def _():
                attend(second)

            @pl.when((i == 3) | (i == 5))
            def _():
                edge(jnp.where(i == 3, outward, 1 - outward))

        each_part(slot, parts + 2 * LAG)

    def reduce_step(step):
        def one(turn, carry):
            side = jnp.where(2 * tp < tp_count, 1 - turn, turn)
            block = jnp.where(side == 0, step - tp, 2 * (tp_count - 1) - step - tp)
            active = (block >= 0) & (block < tp_count)
            if swaps:
                block = swapped(1 - side, block, True)
            active = active & ((block - tp) * (1 - 2 * side) > 0)

            @pl.when(active)
            def _():
                weights = weights_of(block)
                each_part(lambda part: reduce_piece(side, block, part, weights))

            return carry

        lax.fori_loop(0, 2, one, 0)

    early = tp_count > 2

    def hop(k, carry):
        def one_turn(turn):
            def receive(second, carry):
                part = turn - second * LAG
                side = jnp.where(2 * tp < tp_count, second, 1 - second)
                block, inside = at(side, k)

                @pl.when(inside & (part >= 0) & (part < parts))
                def _():
                    send_second(side, block, part).wait_recv()

                    @pl.when(exists(side))
                    def _():
                        send_second(side, block, part).start()

                    @pl.when(part == 0)
                    def _():
                        send_meta(side, block).wait_recv()

                        @pl.when(exists(side))
                        def _():
                            send_meta(side, block).start()

                    @pl.when(late(side) & (k == 1) & (part == parts - 1))
                    def _():
                        for own in range(AHEAD, parts):
                            send_second(side, tp, own).start()

                    pick_part(block, part)

                return carry

            lax.fori_loop(0, 2, receive, 0)

            @pl.when(k == 1)
            def _():
                @pl.when(turn == 1)
                def _():
                    tables()

                @pl.when(turn == 2)
                def _():
                    project(tp)
                    start_halo(tp)

            if early:

                @pl.when(ends & (k == tp_count - 1) & (turn == LAG + 1))
                def _():
                    reduce_step(1)


            middle = ends & (k > 1) & (k == tp_count - 1) & (turn == LAG)

            @pl.when(middle | ((k == 1) & (turn == LAG + 2)))
            def _():
                experts_at(k - 1)

        each_part(one_turn, parts + LAG)
        for side in range(2):
            start_own_first(side, k)
        for side in range(2):
            block, inside = at(side, k)

            @pl.when(inside)
            def _():
                shared_hidden(block)

        if assist:

            @pl.when(helps & (k == 2))
            def _():
                relay_first()

        if slim:

            @pl.when(helps & (k == tp_count - 1))
            def _():
                side = 1 - outward
                block, _ = near(side, 1)
                send_first(side, block).wait_recv()
                send_first(side, block).start()
                project(block)
                start_halo(block)

        @pl.when((k > 1) & (jnp.logical_not(ends) | (k < tp_count - 1)))
        def _():
            experts_at(k - 1)

        return carry

    lax.fori_loop(1, tp_count, hop, 0)
    if early:
        reduce_step(2)

    experts_at(tp_count - 1)

    @pl.when(ends | (not slim))
    def _():
        give_back(0, parts // 2)

    if assist:

        @pl.when(helps)
        def _():
            relay_second()


    def first_hop(k, carry):
        def open_at(side):
            block, inside = near(side, k)
            if slim:
                inside = inside & (k == 1) & (side == outward)
            return block, inside

        for side in range(2):
            block, inside = open_at(side)

            @pl.when(inside & plain)
            def _():
                send_first(side, block).wait_recv()

                @pl.when(carries(side))
                def _():
                    send_first(side, block).start()

        if assist:

            @pl.when(helps)
            def _():
                @pl.when(k == 1)
                def _():
                    relay_last()

                def one(turn, carry):
                    block, inside = near(outward, k * turn)

                    if slim:
                        inside = inside & (k == 1)

                    @pl.when(inside & ((turn == 1) | (k == 1)))
                    def _():
                        project_far(block)

                    return carry

                lax.fori_loop(0, 2, one, 0)

        def use(side, carry):
            block, inside = open_at(side)

            @pl.when(inside & plain)
            def _():
                project(block)
                start_halo(block)

            return carry

        lax.fori_loop(0, 2, use, 0)
        if not slim:

            @pl.when((k == jnp.maximum(tp, tp_count - 1 - tp)) & plain)
            def _():
                give_back(parts // 2, parts)

        if slim:

            @pl.when((k == 2) & ends)
            def _():
                reduce_step(3)

            @pl.when((k == 2) & helps)
            def _():
                reduce_merged()

        elif early:

            @pl.when(k > 1)
            def _():
                reduce_step(2 * k - 1)
                reduce_step(2 * k)

        else:
            reduce_step(2 * k - 1)

        def settle(side, carry):
            block, _ = near(side, k - 1)

            inner = (block > 0) & (block < tp_count - 1) & ((k > 1) | (side == 0))
            if slim:
                inner = inner & (k == 1)

            @pl.when(inner & plain)
            def _():
                attend(block)

            return carry

        lax.fori_loop(0, 2, settle, 0)
        return carry

    lax.fori_loop(1, tp_count, first_hop, 0)
    if assist:

        @pl.when(ends)
        def _():
            for copy in lent_all(toward(jnp.where(tp == 0, 0, 1))):
                copy.wait_recv()
            start_halo(tp_count - 1 - tp)
            give_back(parts // 2, parts)
            each_part(lambda block: attend(block + 1), tp_count - 2)

    @pl.when(jnp.logical_not(helps) | (not slim))
    def _():
        each_part(lambda turn: edge(jnp.where(2 * tp < tp_count, 1 - turn, turn)), 2)

    own_weights = weights_of(tp)

    def last_part(part):
        span = part_span(part)
        return_part(tp, part).wait_recv()
        own = value_of(tp, own_weights, span)

        for i in range(CHUNK // PASS):

            @pl.when(tp > 0)
            def _():
                pass_on(0, tp, part * (CHUNK // PASS) + i, tp).wait_recv()

            @pl.when(tp < tp_count - 1)
            def _():
                pass_on(1, tp, part * (CHUNK // PASS) + i, tp).wait_recv()

        psend[tp, :, span] = (
            own + sides[0, tp, :, span].astype(f32) + sides[1, tp, :, span].astype(f32)
        ).astype(bf16)
        out_copy(part).start()

    each_part(last_part)

    def finish(block):
        return_all(block).wait_send()
        for side in range(2):
            passed = block <= tp if side == 0 else block >= tp
            summed = block > tp if side == 0 else block < tp

            @pl.when(exists(side) & passed)
            def _():
                ref = gath2.at[block]
                remote(ref, ref, s2.at[lane(side, block, tp)], r2.at[block, 0], toward(side)).wait_send()
                send_meta(side, block).wait_send()

            @pl.when(carries(side) & passed)
            def _():
                send_first(side, block).wait_send()

            @pl.when(summed)
            def _():
                remote(
                    psend.at[block], sides.at[side, block], sp.at[block], rs.at[block, 0], toward(side)
                ).wait_send()

    each_part(finish, tp_count)
    if assist:

        @pl.when(ends)
        def _():
            for copy in lend_out():
                copy.wait_send()

        @pl.when(helps)
        def _():
            for copies in relays() + (relays_across() if pair == 2 else []):
                for copy in copies:
                    copy.wait_send()

            for copy in lent_all(toward(outward)):
                copy.wait_send()


    pltpu.make_async_copy(mixed, mixed_out, mixed_sem.at[0]).wait()
    pltpu.make_async_copy(psend.at[tp], out, out_sem.at[0]).wait()

    @pl.when(ep < ep_count - 1)
    def _():
        halo(0).wait_send()

    @pl.when(ep > 0)
    def _():
        halo(1).wait_send()


def layer(
    second, first, gain_second, gain_first, router, routes, inverse, sink,
    gate, up, down, sgate, sup, sdown, wq, wk, wv, grp_count, ep_count, tp_count, slots,
):
    rows, width = second.shape
    experts = router.shape[0]
    hbm = pl.BlockSpec(memory_space=pl.ANY)
    dma = pltpu.SemaphoreType.DMA
    bf16, f32 = jnp.bfloat16, jnp.float32
    total = ep_count * slots
    parts = width // CHUNK
    span = tp_count * rows
    kv_cols = wk.shape[1] + wv.shape[1]
    return pl.pallas_call(
        functools.partial(layer_kernel, grp_count, ep_count, tp_count, slots),
        out_shape=(
            jax.ShapeDtypeStruct((rows, width), bf16),
            jax.ShapeDtypeStruct((span, wq.shape[1]), bf16),
        ),
        in_specs=[hbm] * 17,
        out_specs=(hbm, hbm),
        scratch_shapes=[
            pltpu.VMEM((span, wq.shape[1]), bf16),
            pltpu.VMEM((rows, width), bf16),
            pltpu.VMEM(gain_second.shape, f32),
            pltpu.VMEM(router.shape, bf16),
            pltpu.VMEM(routes.shape, jnp.int32),
            pltpu.VMEM(gain_first.shape, f32),
            pltpu.VMEM(inverse.shape, f32),
            pltpu.SMEM(sink.shape, f32),
            pltpu.VMEM((tp_count, rows, width), bf16),
            pltpu.VMEM((tp_count, rows, width), bf16),
            pltpu.VMEM((rows, width), bf16),
            pltpu.VMEM((tp_count, 2 * experts, rows), f32),
            pltpu.VMEM((tp_count, total, width), bf16),
            pltpu.VMEM((tp_count, total, width), bf16),
            pltpu.VMEM((tp_count, total, width), bf16),
            pltpu.VMEM((2, tp_count, rows, width), bf16),
            pltpu.VMEM((tp_count, rows, width), bf16),
            pltpu.VMEM(gate.shape[1:], bf16),
            pltpu.VMEM(up.shape[1:], bf16),
            pltpu.VMEM(down.shape[1:], bf16),
            pltpu.VMEM(sgate.shape, bf16),
            pltpu.VMEM(sup.shape, bf16),
            pltpu.VMEM(sdown.shape, bf16),
            pltpu.VMEM(wq.shape, bf16),
            pltpu.VMEM(wk.shape, bf16),
            pltpu.VMEM(wv.shape, bf16),
            pltpu.VMEM(wq.shape, bf16),
            pltpu.VMEM(wk.shape, bf16),
            pltpu.VMEM(wv.shape, bf16),
            pltpu.VMEM((tp_count, rows, wq.shape[1]), bf16),
            pltpu.VMEM((tp_count, rows, kv_cols), bf16),
            pltpu.VMEM((tp_count, rows, sgate.shape[1]), bf16),
            pltpu.VMEM((total, gate.shape[2]), bf16),
            pltpu.VMEM((span, LANES), f32),
            pltpu.VMEM((span, LANES), f32),
            pltpu.VMEM((span, wq.shape[1]), bf16),
            pltpu.VMEM((span + 2 * rows, kv_cols), bf16),
            dma((17,)),
            dma((tp_count + 1,)),
            dma((tp_count, parts)),
            dma((tp_count + 1,)),
            dma((tp_count,)),
            dma((tp_count + 1,)),
            dma((tp_count,)),
            dma((tp_count,)),
            dma((tp_count,)),
            dma((tp_count,)),
            dma((tp_count, parts)),
            dma((tp_count,)),
            dma((tp_count + 1, width // PASS)),
            dma((2,)),
            dma((2,)),
            dma((1,)),
            dma((1,)),
            dma((2 * grp_count - 1, 3)),
            dma((2 * grp_count, 3)),
            dma((2,)),
            dma((2,)),
        ],
        compiler_params=pltpu.CompilerParams(
            collective_id=0, has_side_effects=True, vmem_limit_bytes=VMEM_LIMIT
        ),
        name="layer",
    )(
        second, gain_second, router, routes, gain_first, inverse, sink,
        first, gate, up, down, sgate, sup, sdown, wq, wk, wv,
    )


def settle_kernel(first, second, first_out, second_out, first_buf, second_buf, sems):
    arrays = [(first, first_buf, first_out), (second, second_buf, second_out)]
    pieces = []
    for i, (source, buffer, target) in enumerate(arrays):
        half = source.shape[0] // 2
        for j in range(2):
            rows = pl.ds(j * half, half)
            pieces.append(
                (
                    pltpu.make_async_copy(source.at[rows], buffer.at[rows], sems.at[0, i, j]),
                    pltpu.make_async_copy(buffer.at[rows], target.at[rows], sems.at[1, i, j]),
                )
            )
    for load, _ in pieces:
        load.start()
    for load, store in pieces:
        load.wait()
        store.start()
    for _, store in pieces:
        store.wait()


def settle(first, second):
    hbm = pl.BlockSpec(memory_space=pl.ANY)
    return pl.pallas_call(
        settle_kernel,
        out_shape=(jax.ShapeDtypeStruct(first.shape, first.dtype), jax.ShapeDtypeStruct(second.shape, second.dtype)),
        in_specs=[hbm, hbm],
        out_specs=(hbm, hbm),
        scratch_shapes=[
            pltpu.VMEM(first.shape, first.dtype),
            pltpu.VMEM(second.shape, second.dtype),
            pltpu.SemaphoreType.DMA((2, 2, 2)),
        ],
        compiler_params=pltpu.CompilerParams(vmem_limit_bytes=VMEM_LIMIT),
        name="settle",
    )(first, second)


def body(
    mixer_in,
    mixer_gain,
    w_query,
    w_key,
    w_value,
    sink_logit,
    moe_in,
    moe_gain,
    router,
    routes,
    expert_gate,
    expert_up,
    expert_down,
    shared_gate,
    shared_up,
    shared_down,
):
    tokens = mixer_in.shape[0]
    ep_count, tp_count = lax.axis_size("ep"), lax.axis_size("tp")
    top_count = routes.shape[1]
    experts = router.shape[1]
    capacity = 3 * top_count * tokens // (2 * experts)
    slots = -(-capacity // 16) * 16
    half = HEAD_DIM // 2
    inverse = np.float32(THETA) ** (-(np.arange(half, dtype=np.float32) * np.float32(2.0)) / np.float32(HEAD_DIM))
    moe_out, mixed = layer(
        moe_in, mixer_in, moe_gain[None, :], mixer_gain[None, :], router.T, routes.T,
        jnp.asarray(np.tile(inverse, LANES // half)[None, :]), sink_logit[None, :],
        expert_gate, expert_up, expert_down, shared_gate, shared_up, shared_down,
        w_query, w_key, w_value, lax.axis_size("grp"), ep_count, tp_count, slots,
    )
    moe_out, mixed = settle(moe_out, mixed)
    return (mixed, moe_out)


def solution(mesh):
    return jax.shard_map(
        body,
        mesh=mesh,
        in_specs=(
            P(("grp", "ep", "tp"), None),
            P(),
            P(None, "tp"),
            P(None, "tp"),
            P(None, "tp"),
            P("tp"),
            P(("grp", "ep", "tp"), None),
            P(),
            P(),
            P(("grp", "ep", "tp"), None),
            P(("ep", "tp"), None, None),
            P(("ep", "tp"), None, None),
            P(("ep", "tp"), None, None),
            P(None, "tp"),
            P(None, "tp"),
            P("tp", None),
        ),
        out_specs=(P(("grp", "ep"), "tp"), P(("grp", "ep", "tp"), None)),
        check_vma=False,
    )
```

```python
import functools

import jax
import jax.numpy as jnp
import numpy as np
from jax import lax
from jax.experimental import pallas as pl
from jax.experimental.pallas import tpu as pltpu
from jax.sharding import PartitionSpec as P

HEAD_DIM = 64
WINDOW = 128
EPS = 1e-06
THETA = 10000.0
ROUTED_SCALE = 2.5
LANES = 128
CHUNK = 512
PASS = 256
LAG = 2
AHEAD = 2
MESH = pl.DeviceIdType.MESH
VMEM_LIMIT = 63 * 2**20


def remote(src, dst, send_sem, recv_sem, device):
    return pltpu.make_async_remote_copy(
        src_ref=src,
        dst_ref=dst,
        send_sem=send_sem,
        recv_sem=recv_sem,
        device_id=device,
        device_id_type=MESH,
    )


def greet(grp, ep, tp, grp_count, ep_count, tp_count):
    barrier = pltpu.get_barrier_semaphore()

    @pl.when(tp > 0)
    def _():
        pl.semaphore_signal(barrier, inc=1, device_id=(grp, ep, tp - 1), device_id_type=MESH)

    @pl.when(tp < tp_count - 1)
    def _():
        pl.semaphore_signal(barrier, inc=1, device_id=(grp, ep, tp + 1), device_id_type=MESH)

    for d in range(1, ep_count):
        pl.semaphore_signal(
            barrier, inc=1, device_id=(grp, lax.rem(ep + d, ep_count), tp), device_id_type=MESH
        )
    for d in range(1, grp_count):
        pl.semaphore_signal(
            barrier, inc=1, device_id=(lax.rem(grp + d, grp_count), ep, tp), device_id_type=MESH
        )
    return barrier


def layer_kernel(
    grp_count, ep_count, tp_count, slots,
    second_hbm, gain_second_hbm, router_hbm, routes_hbm, gain_first_hbm, inverse_hbm, sink_hbm,
    first_hbm, gate_hbm, up_hbm, down_hbm, sgate_hbm, sup_hbm, sdown_hbm, wq_hbm, wk_hbm, wv_hbm,
    out, mixed_out,
    mixed, second_in, gain_second, router, routes, gain_first, inverse, sink,
    gath2, gath1, first_in, metag, sbuf, disp, back, sides, psend,
    gate, up, down, sgate, sup, sdown, wq, wk, wv, far_q, far_k, far_v, lent_q, lent_kv,
    hidden, hexp, cosine, sine, qbuf, kvbuf,
    l_sem, s2, r2, sm, rm, s1, r1, sd, rd, sb, rb, sp, rs, hs, hr, out_sem, mixed_sem, ws, wr, qs, qr,
):
    grp, ep, tp = lax.axis_index("grp"), lax.axis_index("ep"), lax.axis_index("tp")
    rows, width = second_in.shape
    experts = metag.shape[1] // 2
    total = ep_count * slots
    parts = width // CHUNK
    f32, bf16 = jnp.float32, jnp.bfloat16
    away = pl.ds(slots, total - slots)

    barrier = greet(grp, ep, tp, grp_count, ep_count, tp_count)
    early_pairs = [
        (second_hbm, second_in),
        (gain_second_hbm, gain_second),
        (routes_hbm, routes),
        (router_hbm, router),
    ]
    pairs = early_pairs + [
        (gain_first_hbm, gain_first),
        (first_hbm, first_in),
        (sgate_hbm, sgate),
        (sup_hbm, sup),
        (wq_hbm, wq),
        (wk_hbm, wk),
        (wv_hbm, wv),
        (inverse_hbm, inverse),
        (sink_hbm, sink),
        (gate_hbm.at[0], gate),
        (up_hbm.at[0], up),
        (down_hbm.at[0], down),
        (sdown_hbm, sdown),
    ]
    local = [pltpu.make_async_copy(src, dst, l_sem.at[i]) for i, (src, dst) in enumerate(pairs)]
    for copy in local:
        copy.start()

    def toward(side):
        return (grp, ep, tp + 1 - 2 * side)

    def exists(side):
        return (tp + 1 - 2 * side >= 0) & (tp + 1 - 2 * side < tp_count)

    def peer(d):
        return (grp, lax.rem(ep + d, ep_count), tp)

    def part_span(part, size=CHUNK):
        return pl.ds(pl.multiple_of(part * size, size), size)

    def each_part(body, count=parts):
        def step(part, carry):
            body(part)
            return carry

        lax.fori_loop(0, count, step, 0)

    def near(side, distance):
        block = tp + (2 * side - 1) * distance
        return block, (block >= 0) & (block < tp_count)

    swaps = tp_count > 2

    def swapped(side, block, allowed):
        far, second = (tp_count - 1) * side, 1 + (tp_count - 3) * side
        other = jnp.where(block == second, far, jnp.where(block == far, second, block))
        return jnp.where(allowed, other, block)

    def at(side, order):
        block, inside = near(side, order)
        if swaps:
            block = swapped(side, block, jnp.where(side == 0, tp, tp_count - 1 - tp) >= 2)
        return block, inside

    def late(side):
        return (tp == 1 + side * (tp_count - 3)) & swaps

    def lane(side, block, owner):
        return jnp.where((block == owner) & (side == 1), tp_count, block)

    def send_second(side, block, part):
        ref = gath2.at[block, :, part_span(part)]
        return remote(ref, ref, s2.at[lane(side, block, tp)], r2.at[block, part], toward(side))

    def send_meta(side, block):
        return remote(metag.at[block], metag.at[block], sm.at[lane(side, block, tp)], rm.at[block], toward(side))

    assist = tp_count >= 4
    ends = (tp == 0) | (tp == tp_count - 1)
    slim = tp_count == 4
    plain = jnp.logical_not(ends) | (not assist)
    helps = ((tp == 1) | (tp == tp_count - 2)) & assist
    outward = jnp.where(tp == 1, 1, 0)
    pair = 2 if ep_count % 2 == 0 else 1
    core = lax.rem(ep, pair)
    piece_rows = width // (grp_count * pair)
    lent = [(wq, far_q), (wk, far_k), (wv, far_v)]

    def carries(side):
        target = tp + 1 - 2 * side
        return exists(side) & (((target > 0) & (target < tp_count - 1)) | (not assist))

    def share_of(group, half):
        return group * pair + half

    def lend(share, to, device, own):
        span = pl.ds(pl.multiple_of(share * piece_rows, piece_rows), piece_rows)
        return [
            remote(
                (near_ref if own else far_ref).at[span], far_ref.at[span],
                ws.at[to, i], wr.at[share, i], device,
            )
            for i, (near_ref, far_ref) in enumerate(lent)
        ]

    def lend_out():
        return lend(share_of(grp, core), 0, (grp, ep, jnp.where(tp == 0, 1, tp_count - 2)), True)

    def partner():
        return (grp, ep + 1 - 2 * core, tp)

    def relays():
        mine = share_of(grp, core)
        copies = []
        for d in range(1, grp_count):
            copies.append(lend(mine, d, (lax.rem(grp + d, grp_count), ep, tp), False))
        if pair == 2:
            copies.append(lend(mine, 0, partner(), False))
        return copies

    def relays_across():
        copies = []
        for d in range(1, grp_count):
            copies.append(lend(share_of(lax.rem(grp + d, grp_count), core), grp_count - 1 + d, partner(), False))
        return copies

    def relay_first():
        for copy in lend(share_of(grp, core), 0, toward(outward), False):
            copy.wait_recv()
        for copies in relays():
            for copy in copies:
                copy.start()

    def relay_second():
        for copies in relays_across():
            for copy in copies:
                copy.wait_recv()
            if pair == 2:
                for copy in copies:
                    copy.start()

    def relay_last():
        if pair == 2:
            for group in range(grp_count):
                for copy in lend(share_of(group, 1 - core), 0, partner(), False):
                    copy.wait_recv()

    def query_copy(block, device):
        return remote(
            lent_q.at[block], qbuf.at[part_span(block, rows)], qs.at[0], qr.at[0], device
        )

    def kv_copy(block, device):
        return remote(
            lent_kv.at[block], kvbuf.at[part_span(block + 1, rows)], qs.at[1], qr.at[1], device
        )

    def lent_all(device):
        span = pl.ds(0, (tp_count - 1) * rows)
        return [
            remote(ref.at[span], ref.at[span], qs.at[i], qr.at[i], device) for i, ref in enumerate((qbuf, kvbuf))
        ]

    def send_first(side, block):
        return remote(gath1.at[block], gath1.at[block], s1.at[lane(side, block, tp)], r1.at[block], toward(side))

    def dispatch_copy(block, d, span):
        mine = pl.ds(d * slots, slots)
        return remote(sbuf.at[block, mine, span], disp.at[block, mine, span], sd.at[block], rd.at[block], peer(d))

    def dispatch_all(block):
        return remote(sbuf.at[block, away], disp.at[block, away], sd.at[block], rd.at[block], peer(1))

    def return_copy(block, d, part):
        mine, span = pl.ds(d * slots, slots), part_span(part)
        return remote(
            sbuf.at[block, mine, span], back.at[block, mine, span],
            sb.at[block], rb.at[block, part], peer(ep_count - d),
        )

    def return_part(block, part):
        span = part_span(part)
        return remote(
            sbuf.at[block, away, span], back.at[block, away, span], sb.at[block], rb.at[block, part], peer(1)
        )

    def return_all(block):
        return remote(sbuf.at[block, away], back.at[block, away], sb.at[block], rb.at[block, 0], peer(1))

    def pass_on(side, block, part, owner):
        span = part_span(part, PASS)
        return remote(
            psend.at[block, :, span], sides.at[side, block, :, span],
            sp.at[block], rs.at[lane(side, block, owner), part], toward(side),
        )

    def halo(side):
        source = tp_count * rows if side == 0 else rows
        target = 0 if side == 0 else (tp_count + 1) * rows
        return remote(
            kvbuf.at[pl.ds(source, rows)], kvbuf.at[pl.ds(target, rows)],
            hs.at[side], hr.at[side], (grp, ep + (1 if side == 0 else -1), tp),
        )

    def out_copy(part):
        span = part_span(part)
        return pltpu.make_async_copy(psend.at[tp, :, span], out.at[:, span], out_sem.at[0])

    def mixed_copy(block):
        span = part_span(block, rows)
        return pltpu.make_async_copy(mixed.at[span], mixed_out.at[span], mixed_sem.at[0])

    def normalize(source, gain, target):
        def squares(part, carry):
            values = source[:, part_span(part)].astype(f32)
            return carry + jnp.sum(values * values, axis=1, keepdims=True)

        summed = lax.fori_loop(0, parts, squares, jnp.zeros((rows, 1), f32))
        factor = lax.rsqrt(summed / width + EPS)

        def scale(part):
            span = part_span(part)
            target[:, span] = (source[:, span].astype(f32) * factor * gain[:, span]).astype(bf16)

        each_part(scale)

    def places_of(block, d):
        expert = lax.rem(ep + d, ep_count) * tp_count + tp
        slot_ids = lax.broadcasted_iota(jnp.int32, (slots, rows), 0).astype(f32)
        return slot_ids == metag[block, pl.ds(expert, 1), :], expert

    def pick_part(block, part):
        span = part_span(part)
        picks = [jnp.where(places_of(block, d)[0], 1.0, 0.0) for d in range(ep_count)]
        pick = jnp.concatenate(picks, axis=0).astype(bf16)
        picked = jnp.dot(pick, gath2[block, :, span], preferred_element_type=f32).astype(bf16)
        disp[block, 0:slots, span] = picked[0:slots]
        sbuf[block, slots:total, span] = picked[slots:total]
        for d in range(1, ep_count):
            dispatch_copy(block, d, span).start()

    def shared_hidden(block):
        values = gath2[block]
        gated = jnp.dot(values, sgate[...], preferred_element_type=f32)
        lifted = jnp.dot(values, sup[...], preferred_element_type=f32)
        hidden[block] = (jax.nn.silu(gated) * lifted).astype(bf16)

    def expert(block):
        dispatch_all(block).wait()

        def units(part):
            span = part_span(part, 256)
            values = disp[block]
            gated = jnp.dot(values, gate[:, span], preferred_element_type=f32)
            lifted = jnp.dot(values, up[:, span], preferred_element_type=f32)
            hexp[:, span] = (jax.nn.silu(gated) * lifted).astype(bf16)

        each_part(units, gate.shape[1] // 256)

        def columns(part):
            span = part_span(part)
            result = jnp.dot(hexp[...], down[:, span], preferred_element_type=f32).astype(bf16)
            back[block, 0:slots, span] = result[0:slots]
            sbuf[block, slots:total, span] = result[slots:total]

            @pl.when(block != tp)
            def _():
                for d in range(1, ep_count):
                    return_copy(block, d, part).start()

        each_part(columns)

    def experts_at(order):
        def one(side, carry):
            block, inside = at(side, order)

            @pl.when(inside & ((order > 0) | (side == 0)))
            def _():
                expert(block)

            return carry

        lax.fori_loop(0, 2, one, 0)

    def start_own_first(side, step):
        last = tp if side == 0 else tp_count - 1 - tp

        @pl.when(carries(side) & (step == last))
        def _():
            send_first(side, tp).start()

    def rotated(values, cos_rows, sin_rows):
        pieces = []
        half = HEAD_DIM // 2
        size = LANES if values.shape[1] % LANES == 0 else HEAD_DIM
        for start in range(0, values.shape[1], size):
            piece = values[:, start : start + size]
            if size == LANES:
                lane = lax.broadcasted_iota(jnp.int32, piece.shape, 1)
                crossed = jnp.where(
                    lax.rem(lane, HEAD_DIM) < half,
                    pltpu.roll(piece, LANES - half, 1),
                    pltpu.roll(piece, half, 1),
                )
            else:
                crossed = jnp.concatenate([piece[:, half:], piece[:, :half]], axis=1)
            pieces.append(piece * cos_rows[:, :size] + crossed * sin_rows[:, :size])
        return pieces[0] if len(pieces) == 1 else jnp.concatenate(pieces, axis=1)

    def projected(block, query_w, key_w, value_w):
        span = part_span(block, rows)
        values = gath1[block]
        cos_rows, sin_rows = cosine[span, :], sine[span, :]
        query = jnp.dot(values, query_w[...], preferred_element_type=f32)
        key = jnp.dot(values, key_w[...], preferred_element_type=f32)
        value = jnp.dot(values, value_w[...], preferred_element_type=f32)
        joined = jnp.concatenate([rotated(key, cos_rows, sin_rows), value], axis=1).astype(bf16)
        return rotated(query, cos_rows, sin_rows).astype(bf16), joined

    def project(block):
        qbuf[part_span(block, rows), :], kvbuf[part_span(block + 1, rows), :] = projected(block, wq, wk, wv)

    def project_far(block):
        lent_q[block], lent_kv[block] = projected(block, far_q, far_k, far_v)
        query_copy(block, toward(outward)).start()
        kv_copy(block, toward(outward)).start()

    def start_halo(block):
        @pl.when((block == tp_count - 1) & (ep < ep_count - 1))
        def _():
            halo(0).start()

        @pl.when((block == 0) & (ep > 0))
        def _():
            halo(1).start()

    def tables():
        def one(block):
            start = pl.multiple_of(block * rows, rows)
            shape = (rows, LANES)
            place = ep * (tp_count * rows) + start + lax.broadcasted_iota(jnp.int32, shape, 0)
            angle = place.astype(f32) * inverse[...]
            lane = lax.broadcasted_iota(jnp.int32, shape, 1)
            turn = jnp.sin(angle)
            cosine[pl.ds(start, rows), :] = jnp.cos(angle)
            sine[pl.ds(start, rows), :] = jnp.where(lax.rem(lane, HEAD_DIM) < HEAD_DIM // 2, -turn, turn)

        each_part(one, tp_count)

    kv_heads = wk.shape[1] // HEAD_DIM
    group = wq.shape[1] // wk.shape[1]

    def attend(block):
        base = pl.multiple_of(block * rows, rows)
        window = kvbuf[pl.ds(base, 3 * rows), :]
        query = qbuf[pl.ds(base, rows), :]
        shape = (rows, 3 * rows)
        row = lax.broadcasted_iota(jnp.int32, shape, 0)
        col = lax.broadcasted_iota(jnp.int32, shape, 1)
        gap = col - row - rows
        low = jnp.where((ep == 0) & (block == 0), rows, 0)
        high = jnp.where((ep == ep_count - 1) & (block == tp_count - 1), 2 * rows, 3 * rows)
        near = (gap <= WINDOW) & (gap >= -WINDOW) & (col >= low) & (col < high)
        pieces = []
        for g in range(kv_heads):
            keys = window[:, g * HEAD_DIM : (g + 1) * HEAD_DIM]
            start = (kv_heads + g) * HEAD_DIM
            values = window[:, start : start + HEAD_DIM]
            for h in range(g * group, (g + 1) * group):
                scores = lax.dot_general(
                    query[:, h * HEAD_DIM : (h + 1) * HEAD_DIM], keys, (((1,), (1,)), ((), ())),
                    preferred_element_type=f32,
                ) * HEAD_DIM ** (-0.5)
                scores = jnp.where(near, scores, -jnp.inf)
                bound = sink[0, h]
                top = jnp.maximum(jnp.max(scores, axis=1, keepdims=True), bound)
                weights = jnp.exp(scores - top)
                summed = jnp.sum(weights, axis=1, keepdims=True) + jnp.exp(bound - top)
                share = (weights * (1.0 / summed)).astype(bf16)
                pieces.append(jnp.dot(share, values, preferred_element_type=f32))
        mixed[pl.ds(base, rows), :] = jnp.concatenate(pieces, axis=1).astype(bf16)
        mixed_copy(block).start()

    for copy in local[: len(early_pairs)]:
        copy.wait()
    normalize(second_in, gain_second, gath2.at[tp])
    ids = lax.broadcasted_iota(jnp.int32, (experts, rows), 0)
    hit = ids == routes[0:1, :]
    for j in range(1, routes.shape[0]):
        hit = hit | (ids == routes[j : j + 1, :])
    earlier = (
        lax.broadcasted_iota(jnp.int32, (rows, rows), 0) < lax.broadcasted_iota(jnp.int32, (rows, rows), 1)
    )
    before = jnp.dot(
        jnp.where(hit, 1.0, 0.0).astype(bf16), jnp.where(earlier, 1.0, 0.0).astype(bf16),
        preferred_element_type=f32,
    )
    metag[tp, 0:experts, :] = jnp.where(hit, before, -1.0)
    pl.semaphore_wait(barrier, ep_count + grp_count - 1 + jnp.where((tp > 0) & (tp < tp_count - 1), 1, 0))

    def send_own(part):
        for side in range(2):

            @pl.when(exists(side) & (jnp.logical_not(late(side)) | (part < AHEAD)))
            def _():
                send_second(side, tp, part).start()

    send_own(0)
    affinity = lax.dot_general(
        router[...], gath2[tp], (((1,), (1,)), ((), ())), preferred_element_type=f32
    )
    chosen = jnp.where(hit, jax.nn.sigmoid(affinity), 0.0)
    metag[tp, experts : 2 * experts, :] = ROUTED_SCALE * chosen / jnp.sum(chosen, axis=0, keepdims=True)
    pick_part(tp, 0)
    for side in range(2):

        @pl.when(exists(side))
        def _():
            send_meta(side, tp).start()

    for part in range(1, parts):
        send_own(part)

    def pick_rest(part, carry):
        pick_part(tp, part)
        return carry

    lax.fori_loop(1, parts, pick_rest, 0)
    for copy in local[len(early_pairs) : len(early_pairs) + 2]:
        copy.wait()
    normalize(first_in, gain_first, gath1.at[tp])

    @pl.when(tp == 0)
    def _():
        sides[0] = jnp.zeros(sides.shape[1:], sides.dtype)

    @pl.when(tp == tp_count - 1)
    def _():
        sides[1] = jnp.zeros(sides.shape[1:], sides.dtype)

    @pl.when(ep == 0)
    def _():
        kvbuf[0:rows, :] = jnp.zeros((rows, kvbuf.shape[1]), bf16)

    @pl.when(ep == ep_count - 1)
    def _():
        kvbuf[(tp_count + 1) * rows : (tp_count + 2) * rows, :] = jnp.zeros((rows, kvbuf.shape[1]), bf16)

    for copy in local[len(early_pairs) + 2 :]:
        copy.wait()
    if assist:

        @pl.when(ends)
        def _():
            for copy in lend_out():
                copy.start()

    for side in range(2):
        start_own_first(side, 0)
    shared_hidden(tp)

    def weights_of(block):
        pieces = []
        for d in range(ep_count):
            hit_rows, number = places_of(block, d)
            pieces.append(jnp.where(hit_rows, metag[block, pl.ds(experts + number, 1), :], 0.0))
        weights = jnp.concatenate(pieces, axis=0)
        top = weights.astype(bf16)
        return top, (weights - top.astype(f32)).astype(bf16)

    def value_of(block, weights, span):
        turned = (((0,), (0,)), ((), ()))
        picked = back[block, :, span]
        return (
            lax.dot_general(weights[0], picked, turned, preferred_element_type=f32)
            + lax.dot_general(weights[1], picked, turned, preferred_element_type=f32)
            + jnp.dot(hidden[block], sdown[:, span], preferred_element_type=f32)
        )

    def reduce_piece(side, block, part, weights):
        span = part_span(part)
        return_part(block, part).wait_recv()
        own = value_of(block, weights, span)

        for i in range(CHUNK // PASS):
            number = part * (CHUNK // PASS) + i
            piece = part_span(number, PASS)

            @pl.when(exists(1 - side))
            def _():
                pass_on(side, block, number, tp).wait_recv()

            part_sum = own[:, i * PASS : (i + 1) * PASS] + sides[side, block, :, piece].astype(f32)
            psend[block, :, piece] = part_sum.astype(bf16)
            pass_on(side, block, number, tp + 1 - 2 * side).start()

    def edge(last):
        @pl.when((last == 1) & (ep < ep_count - 1))
        def _():
            halo(1).wait_recv()

        @pl.when((last == 0) & (ep > 0))
        def _():
            halo(0).wait_recv()

        attend((tp_count - 1) * last)

    def give_back(low, high):
        for part in range(low, high):
            for d in range(1, ep_count):
                return_copy(tp, d, part).start()

    def reduce_merged():
        end = (tp_count - 1) * (1 - outward)
        second = 1 + (tp_count - 3) * outward

        def slot(i):
            def stream(j, carry):
                part = i - LAG * j
                side = jnp.where(j == 1, outward, 1 - outward)
                block = jnp.where(j == 0, tp_count - 1 - end, jnp.where(j == 1, end, second))

                @pl.when((part >= 0) & (part < parts))
                def _():
                    reduce_piece(side, block, part, weights_of(block))

                return carry

            lax.fori_loop(0, 3, stream, 0)

            @pl.when(i == 1)
            def _():
                block, _ = near(outward, 2)
                send_first(outward, block).wait_recv()
                project_far(block)
                project(block)
                start_halo(block)
                give_back(0, parts)

            @pl.when(i == 2)
            def _():
                attend(second)

            @pl.when((i == 3) | (i == 5))
            def _():
                edge(jnp.where(i == 3, outward, 1 - outward))

        each_part(slot, parts + 2 * LAG)

    def arrive():
        for copy in lent_all(toward(jnp.where(tp == 0, 0, 1))):
            copy.wait_recv()
        start_halo(tp_count - 1 - tp)

    def reduce_ends():
        side = jnp.where(tp == 0, 0, 1)
        block = jnp.where(tp == 0, tp_count - 2, 1)
        weights = weights_of(block)

        def one(part):
            reduce_piece(side, block, part, weights)

            @pl.when(part == 0)
            def _():
                arrive()
                give_back(parts // 2, parts)

            @pl.when(part < tp_count - 2)
            def _():
                attend(part + 1)

        each_part(one)

    def reduce_step(step):
        def one(turn, carry):
            side = jnp.where(2 * tp < tp_count, 1 - turn, turn)
            block = jnp.where(side == 0, step - tp, 2 * (tp_count - 1) - step - tp)
            active = (block >= 0) & (block < tp_count)
            if swaps:
                block = swapped(1 - side, block, True)
            active = active & ((block - tp) * (1 - 2 * side) > 0)

            @pl.when(active)
            def _():
                weights = weights_of(block)
                each_part(lambda part: reduce_piece(side, block, part, weights))

            return carry

        lax.fori_loop(0, 2, one, 0)

    early = tp_count > 2

    def hop(k, carry):
        def one_turn(turn):
            def receive(second, carry):
                part = turn - second * LAG
                side = jnp.where(2 * tp < tp_count, second, 1 - second)
                block, inside = at(side, k)

                @pl.when(inside & (part >= 0) & (part < parts))
                def _():
                    send_second(side, block, part).wait_recv()

                    @pl.when(exists(side))
                    def _():
                        send_second(side, block, part).start()

                    @pl.when(part == 0)
                    def _():
                        send_meta(side, block).wait_recv()

                        @pl.when(exists(side))
                        def _():
                            send_meta(side, block).start()

                    @pl.when(late(side) & (k == 1) & (part == parts - 1))
                    def _():
                        for own in range(AHEAD, parts):
                            send_second(side, tp, own).start()

                    pick_part(block, part)

                return carry

            lax.fori_loop(0, 2, receive, 0)

            @pl.when(k == 1)
            def _():
                @pl.when(turn == 1)
                def _():
                    tables()

                @pl.when(turn == 2)
                def _():
                    project(tp)
                    start_halo(tp)

            if early:

                @pl.when(ends & (k == tp_count - 1) & (turn == LAG + 2))
                def _():
                    reduce_step(1)


            middle = ends & (k > 1) & (k == tp_count - 1) & (turn == LAG + 1)

            @pl.when(middle | ((k == 1) & (turn == LAG + 2)))
            def _():
                experts_at(k - 1)

        each_part(one_turn, parts + LAG)
        for side in range(2):
            start_own_first(side, k)
        for side in range(2):
            block, inside = at(side, k)

            @pl.when(inside)
            def _():
                shared_hidden(block)

        if assist:

            @pl.when(helps & (k == 2))
            def _():
                relay_first()

        if slim:

            @pl.when(helps & (k == tp_count - 1))
            def _():
                side = 1 - outward
                block, _ = near(side, 1)
                send_first(side, block).wait_recv()
                send_first(side, block).start()
                project(block)
                start_halo(block)

        @pl.when((k > 1) & (jnp.logical_not(ends) | (k < tp_count - 1)))
        def _():
            experts_at(k - 1)

        return carry

    lax.fori_loop(1, tp_count, hop, 0)
    if early:
        reduce_step(2)

    experts_at(tp_count - 1)

    @pl.when(ends | (not slim))
    def _():
        give_back(0, parts // 2)

    if assist:

        @pl.when(helps)
        def _():
            relay_second()


    def first_hop(k, carry):
        def open_at(side):
            block, inside = near(side, k)
            if slim:
                inside = inside & (k == 1) & (side == outward)
            return block, inside

        for side in range(2):
            block, inside = open_at(side)

            @pl.when(inside & plain)
            def _():
                send_first(side, block).wait_recv()

                @pl.when(carries(side))
                def _():
                    send_first(side, block).start()

        if assist:

            @pl.when(helps)
            def _():
                @pl.when(k == 1)
                def _():
                    relay_last()

                def one(turn, carry):
                    block, inside = near(outward, k * turn)

                    if slim:
                        inside = inside & (k == 1)

                    @pl.when(inside & ((turn == 1) | (k == 1)))
                    def _():
                        project_far(block)

                    return carry

                lax.fori_loop(0, 2, one, 0)

        def use(side, carry):
            block, inside = open_at(side)

            @pl.when(inside & plain)
            def _():
                project(block)
                start_halo(block)

            return carry

        lax.fori_loop(0, 2, use, 0)
        if not slim:

            @pl.when((k == jnp.maximum(tp, tp_count - 1 - tp)) & plain)
            def _():
                give_back(parts // 2, parts)

        if slim:

            @pl.when((k == 2) & ends)
            def _():
                reduce_ends()

            @pl.when((k == 2) & helps)
            def _():
                reduce_merged()

        elif early:

            @pl.when(k > 1)
            def _():
                reduce_step(2 * k - 1)
                reduce_step(2 * k)

        else:
            reduce_step(2 * k - 1)

        def settle(side, carry):
            block, _ = near(side, k - 1)

            inner = (block > 0) & (block < tp_count - 1) & ((k > 1) | (side == 0))
            if slim:
                inner = inner & (k == 1)

            @pl.when(inner & plain)
            def _():
                attend(block)

            return carry

        lax.fori_loop(0, 2, settle, 0)
        return carry

    lax.fori_loop(1, tp_count, first_hop, 0)
    if assist:

        @pl.when(ends)
        def _():
            if not slim:
                arrive()
                give_back(parts // 2, parts)
                each_part(lambda block: attend(block + 1), tp_count - 2)

    @pl.when(jnp.logical_not(helps) | (not slim))
    def _():
        each_part(lambda turn: edge(jnp.where(2 * tp < tp_count, 1 - turn, turn)), 2)

    own_weights = weights_of(tp)

    def last_part(part):
        span = part_span(part)
        return_part(tp, part).wait_recv()
        own = value_of(tp, own_weights, span)

        for i in range(CHUNK // PASS):

            @pl.when(tp > 0)
            def _():
                pass_on(0, tp, part * (CHUNK // PASS) + i, tp).wait_recv()

            @pl.when(tp < tp_count - 1)
            def _():
                pass_on(1, tp, part * (CHUNK // PASS) + i, tp).wait_recv()

        psend[tp, :, span] = (
            own + sides[0, tp, :, span].astype(f32) + sides[1, tp, :, span].astype(f32)
        ).astype(bf16)
        out_copy(part).start()

    each_part(last_part)

    def finish(block):
        return_all(block).wait_send()
        for side in range(2):
            passed = block <= tp if side == 0 else block >= tp
            summed = block > tp if side == 0 else block < tp

            @pl.when(exists(side) & passed)
            def _():
                ref = gath2.at[block]
                remote(ref, ref, s2.at[lane(side, block, tp)], r2.at[block, 0], toward(side)).wait_send()
                send_meta(side, block).wait_send()

            @pl.when(carries(side) & passed)
            def _():
                send_first(side, block).wait_send()

            @pl.when(summed)
            def _():
                remote(
                    psend.at[block], sides.at[side, block], sp.at[block], rs.at[block, 0], toward(side)
                ).wait_send()

    each_part(finish, tp_count)
    if assist:

        @pl.when(ends)
        def _():
            for copy in lend_out():
                copy.wait_send()

        @pl.when(helps)
        def _():
            for copies in relays() + (relays_across() if pair == 2 else []):
                for copy in copies:
                    copy.wait_send()

            for copy in lent_all(toward(outward)):
                copy.wait_send()


    pltpu.make_async_copy(mixed, mixed_out, mixed_sem.at[0]).wait()
    pltpu.make_async_copy(psend.at[tp], out, out_sem.at[0]).wait()

    @pl.when(ep < ep_count - 1)
    def _():
        halo(0).wait_send()

    @pl.when(ep > 0)
    def _():
        halo(1).wait_send()


def layer(
    second, first, gain_second, gain_first, router, routes, inverse, sink,
    gate, up, down, sgate, sup, sdown, wq, wk, wv, grp_count, ep_count, tp_count, slots,
):
    rows, width = second.shape
    experts = router.shape[0]
    hbm = pl.BlockSpec(memory_space=pl.ANY)
    dma = pltpu.SemaphoreType.DMA
    bf16, f32 = jnp.bfloat16, jnp.float32
    total = ep_count * slots
    parts = width // CHUNK
    span = tp_count * rows
    kv_cols = wk.shape[1] + wv.shape[1]
    return pl.pallas_call(
        functools.partial(layer_kernel, grp_count, ep_count, tp_count, slots),
        out_shape=(
            jax.ShapeDtypeStruct((rows, width), bf16),
            jax.ShapeDtypeStruct((span, wq.shape[1]), bf16),
        ),
        in_specs=[hbm] * 17,
        out_specs=(hbm, hbm),
        scratch_shapes=[
            pltpu.VMEM((span, wq.shape[1]), bf16),
            pltpu.VMEM((rows, width), bf16),
            pltpu.VMEM(gain_second.shape, f32),
            pltpu.VMEM(router.shape, bf16),
            pltpu.VMEM(routes.shape, jnp.int32),
            pltpu.VMEM(gain_first.shape, f32),
            pltpu.VMEM(inverse.shape, f32),
            pltpu.SMEM(sink.shape, f32),
            pltpu.VMEM((tp_count, rows, width), bf16),
            pltpu.VMEM((tp_count, rows, width), bf16),
            pltpu.VMEM((rows, width), bf16),
            pltpu.VMEM((tp_count, 2 * experts, rows), f32),
            pltpu.VMEM((tp_count, total, width), bf16),
            pltpu.VMEM((tp_count, total, width), bf16),
            pltpu.VMEM((tp_count, total, width), bf16),
            pltpu.VMEM((2, tp_count, rows, width), bf16),
            pltpu.VMEM((tp_count, rows, width), bf16),
            pltpu.VMEM(gate.shape[1:], bf16),
            pltpu.VMEM(up.shape[1:], bf16),
            pltpu.VMEM(down.shape[1:], bf16),
            pltpu.VMEM(sgate.shape, bf16),
            pltpu.VMEM(sup.shape, bf16),
            pltpu.VMEM(sdown.shape, bf16),
            pltpu.VMEM(wq.shape, bf16),
            pltpu.VMEM(wk.shape, bf16),
            pltpu.VMEM(wv.shape, bf16),
            pltpu.VMEM(wq.shape, bf16),
            pltpu.VMEM(wk.shape, bf16),
            pltpu.VMEM(wv.shape, bf16),
            pltpu.VMEM((tp_count, rows, wq.shape[1]), bf16),
            pltpu.VMEM((tp_count, rows, kv_cols), bf16),
            pltpu.VMEM((tp_count, rows, sgate.shape[1]), bf16),
            pltpu.VMEM((total, gate.shape[2]), bf16),
            pltpu.VMEM((span, LANES), f32),
            pltpu.VMEM((span, LANES), f32),
            pltpu.VMEM((span, wq.shape[1]), bf16),
            pltpu.VMEM((span + 2 * rows, kv_cols), bf16),
            dma((17,)),
            dma((tp_count + 1,)),
            dma((tp_count, parts)),
            dma((tp_count + 1,)),
            dma((tp_count,)),
            dma((tp_count + 1,)),
            dma((tp_count,)),
            dma((tp_count,)),
            dma((tp_count,)),
            dma((tp_count,)),
            dma((tp_count, parts)),
            dma((tp_count,)),
            dma((tp_count + 1, width // PASS)),
            dma((2,)),
            dma((2,)),
            dma((1,)),
            dma((1,)),
            dma((2 * grp_count - 1, 3)),
            dma((2 * grp_count, 3)),
            dma((2,)),
            dma((2,)),
        ],
        compiler_params=pltpu.CompilerParams(
            collective_id=0, has_side_effects=True, vmem_limit_bytes=VMEM_LIMIT
        ),
        name="layer",
    )(
        second, gain_second, router, routes, gain_first, inverse, sink,
        first, gate, up, down, sgate, sup, sdown, wq, wk, wv,
    )


def settle_kernel(first, second, first_out, second_out, first_buf, second_buf, sems):
    arrays = [(first, first_buf, first_out), (second, second_buf, second_out)]
    pieces = []
    for i, (source, buffer, target) in enumerate(arrays):
        half = source.shape[0] // 2
        for j in range(2):
            rows = pl.ds(j * half, half)
            pieces.append(
                (
                    pltpu.make_async_copy(source.at[rows], buffer.at[rows], sems.at[0, i, j]),
                    pltpu.make_async_copy(buffer.at[rows], target.at[rows], sems.at[1, i, j]),
                )
            )
    for load, _ in pieces:
        load.start()
    for load, store in pieces:
        load.wait()
        store.start()
    for _, store in pieces:
        store.wait()


def settle(first, second):
    hbm = pl.BlockSpec(memory_space=pl.ANY)
    return pl.pallas_call(
        settle_kernel,
        out_shape=(jax.ShapeDtypeStruct(first.shape, first.dtype), jax.ShapeDtypeStruct(second.shape, second.dtype)),
        in_specs=[hbm, hbm],
        out_specs=(hbm, hbm),
        scratch_shapes=[
            pltpu.VMEM(first.shape, first.dtype),
            pltpu.VMEM(second.shape, second.dtype),
            pltpu.SemaphoreType.DMA((2, 2, 2)),
        ],
        compiler_params=pltpu.CompilerParams(vmem_limit_bytes=VMEM_LIMIT),
        name="settle",
    )(first, second)


def body(
    mixer_in,
    mixer_gain,
    w_query,
    w_key,
    w_value,
    sink_logit,
    moe_in,
    moe_gain,
    router,
    routes,
    expert_gate,
    expert_up,
    expert_down,
    shared_gate,
    shared_up,
    shared_down,
):
    tokens = mixer_in.shape[0]
    ep_count, tp_count = lax.axis_size("ep"), lax.axis_size("tp")
    top_count = routes.shape[1]
    experts = router.shape[1]
    capacity = 3 * top_count * tokens // (2 * experts)
    slots = -(-capacity // 16) * 16
    half = HEAD_DIM // 2
    inverse = np.float32(THETA) ** (-(np.arange(half, dtype=np.float32) * np.float32(2.0)) / np.float32(HEAD_DIM))
    moe_out, mixed = layer(
        moe_in, mixer_in, moe_gain[None, :], mixer_gain[None, :], router.T, routes.T,
        jnp.asarray(np.tile(inverse, LANES // half)[None, :]), sink_logit[None, :],
        expert_gate, expert_up, expert_down, shared_gate, shared_up, shared_down,
        w_query, w_key, w_value, lax.axis_size("grp"), ep_count, tp_count, slots,
    )
    moe_out, mixed = settle(moe_out, mixed)
    return (mixed, moe_out)


def solution(mesh):
    return jax.shard_map(
        body,
        mesh=mesh,
        in_specs=(
            P(("grp", "ep", "tp"), None),
            P(),
            P(None, "tp"),
            P(None, "tp"),
            P(None, "tp"),
            P("tp"),
            P(("grp", "ep", "tp"), None),
            P(),
            P(),
            P(("grp", "ep", "tp"), None),
            P(("ep", "tp"), None, None),
            P(("ep", "tp"), None, None),
            P(("ep", "tp"), None, None),
            P(None, "tp"),
            P(None, "tp"),
            P("tp", None),
        ),
        out_specs=(P(("grp", "ep"), "tp"), P(("grp", "ep", "tp"), None)),
        check_vma=False,
    )
```
